512 devices in a mesh: sp: 64 (over z, y), dp: 8 (over x, core).
Axes of the slice: x: 4, y: 8, z: 8, core: 2. Of those that a mesh axis runs over, the one named last changes fastest.
Arguments:
- gated: bfloat16 [8, 8192, 3072], P('dp', 'sp'), may hold values from -6 to 6
- values_in: bfloat16 [8, 8192, 3072], P('dp', 'sp'), may hold values from -6 to 6
- upstream: bfloat16 [8, 8192, 3072], P('dp', 'sp'), may hold values from -6 to 6
- gain: float32 [3072], replicated, may hold values from 0.1 to 1.9
- shift: float32 [3072], replicated, may hold values from -3 to 3
- mix_w: bfloat16 [512, 4, 512], P('dp'), may hold values from -0.375 to 0.375
- mix_bias: float32 [4, 512], replicated, may hold values from 0.1 to 1.9
Outputs:
- grad_u: bfloat16 [8, 8192, 3072], P('dp', 'sp')
- grad_v: bfloat16 [8, 8192, 3072], P('dp', 'sp')
- grad_mix: float32 [512, 4, 512], P('dp')
- grad_bias: float32 [4, 512], replicated
- grad_gain: float32 [3072], replicated
- grad_shift: float32 [3072], replicated
The draws below stay inside these ranges and needn't reach their ends.
All inputs are finite; a program needn't handle non-finite values.
Results may differ from the reference program's by a relative error of at most 0.014.
Values may be sent and summed in bfloat16 or wider, within the bound.
A program may use at most 64 MiB of HBM per device.

```python
import jax
import jax.numpy as jnp
from jax import lax

GROUPS = 4
GROUP_DIM = 768
SPAN = 512
SEG = 64
HALF = 3072
LENGTH = 8192
BATCH = 8


def level_of(own_key, extent, shards, smallest, top_value):
    def one(dim, parts):
        steps = jax.random.uniform(jax.random.fold_in(jax.random.fold_in(own_key, 6), dim), (parts,), jnp.float32, smallest / len(shards), top_value / len(shards))
        return jnp.repeat(jnp.exp(steps), extent[dim] // parts).reshape((-1,) + (1,) * (len(extent) - dim - 1))

    loudness = one(*shards[0])
    for cut in shards[1:]:
        loudness = loudness * one(*cut)
    return loudness


def noise(rng, dims, deviation, most, split=(), kind=jnp.bfloat16):
    loudness = level_of(rng, dims, split, -0.22, 0.18) if split else 1.0
    drawn = jax.random.normal(rng, dims, jnp.float32) * deviation * loudness
    return jnp.minimum(jnp.maximum(drawn, -most), most).astype(kind)


def setup_inputs(seed: int = 0) -> dict:
    streams_of = jax.random.split(jax.random.key(seed), 8)
    gated = noise(streams_of[0], (BATCH, LENGTH, HALF), 1.0, 6.0, ((0, 8), (1, 64)))
    values_in = noise(streams_of[1], (BATCH, LENGTH, HALF), 1.0, 6.0, ((0, 8), (1, 64)))
    upstream = noise(streams_of[2], (BATCH, LENGTH, HALF), 1.0, 6.0, ((0, 8), (1, 64)))
    gain = jnp.clip(1.0 + 0.18 * jax.random.normal(streams_of[3], (HALF,), jnp.float32), 0.1, 1.9)
    shift = noise(streams_of[4], (HALF,), 0.5, 3.0, (), jnp.float32)
    mix_w = noise(streams_of[5], (SPAN, GROUPS, SPAN), (SPAN // 2) ** -0.5, 0.375, ((0, 8),))
    mix_bias = jnp.clip(1.0 + 0.18 * jax.random.normal(streams_of[6], (GROUPS, SPAN), jnp.float32), 0.1, 1.9)
    return {"gated": gated, "values_in": values_in, "upstream": upstream, "gain": gain, "shift": shift, "mix_w": mix_w, "mix_bias": mix_bias}


EPS = 1e-05

def span_mask():
    places = jnp.arange(SPAN)
    return (places[:, None] // SEG >= places[None, :] // SEG).astype(jnp.float32)

def reference(gated, values_in, upstream, gain, shift, mix_w, mix_bias):
    allowed = span_mask()
    masked_w = mix_w.astype(jnp.float32) * allowed[:, None, :]
    blocks = LENGTH // SPAN

    def one_sequence(carry, inputs):
        gated_row, values_row, upstream_row = inputs
        raw_values = values_row.astype(jnp.float32)
        centred = raw_values - lax.optimization_barrier(jnp.mean(raw_values, axis=-1, keepdims=True))
        inv_std = lax.rsqrt(lax.optimization_barrier(jnp.mean(centred * centred, axis=-1, keepdims=True)) + EPS)
        unit_v = centred * inv_std
        normed = (unit_v * gain + shift).astype(jnp.bfloat16)
        mix_grad = (upstream_row.astype(jnp.float32) * gated_row.astype(jnp.float32)).astype(jnp.bfloat16)
        norm_blocks = normed.reshape(blocks, SPAN, GROUPS, GROUP_DIM).astype(jnp.float32)
        grad_blocks = mix_grad.reshape(blocks, SPAN, GROUPS, GROUP_DIM).astype(jnp.float32)
        mixed_f = jnp.einsum('tgs,nsgc->ntgc', masked_w, norm_blocks) + mix_bias.T[None, :, :, None]
        mixed = lax.optimization_barrier(mixed_f.astype(jnp.bfloat16)).reshape(LENGTH, HALF)
        grad_u = (upstream_row.astype(jnp.float32) * mixed.astype(jnp.float32)).astype(jnp.bfloat16)
        back_f = jnp.einsum('tgs,ntgc->nsgc', masked_w, grad_blocks)
        grad_normed = lax.optimization_barrier(back_f.astype(jnp.bfloat16)).reshape(LENGTH, HALF).astype(jnp.float32)
        scaled = grad_normed * gain
        grad_v = inv_std * (scaled - lax.optimization_barrier(jnp.mean(scaled, axis=-1, keepdims=True)) - unit_v * lax.optimization_barrier(jnp.mean(scaled * unit_v, axis=-1, keepdims=True)))
        mix_term = jnp.einsum('ntgc,nsgc->tgs', grad_blocks, norm_blocks) * allowed[:, None, :]
        bias_term = lax.optimization_barrier(jnp.sum(grad_blocks, axis=(0, 3))).T
        carry = (carry[0] + mix_term, carry[1] + bias_term, carry[2] + lax.optimization_barrier(jnp.sum(grad_normed * unit_v, axis=0)), carry[3] + lax.optimization_barrier(jnp.sum(grad_normed, axis=0)))
        return (carry, (grad_u, grad_v.astype(jnp.bfloat16)))
    initial = (jnp.zeros((SPAN, GROUPS, SPAN), jnp.float32), jnp.zeros((GROUPS, SPAN), jnp.float32), jnp.zeros((HALF,), jnp.float32), jnp.zeros((HALF,), jnp.float32))
    totals, outputs = lax.scan(one_sequence, initial, (gated, values_in, upstream))
    return (outputs[0], outputs[1], totals[0], totals[1], totals[2], totals[3])
```

```python
import jax
import jax.numpy as jnp
from jax import lax
from jax.experimental import pallas as pl
from jax.experimental.pallas import tpu as pltpu
from jax.sharding import Mesh
from jax.sharding import PartitionSpec as P

AXES = ("z", "y", "x", "core")
DP = ("x", "core")
SP = ("z", "y")
MESH = pl.DeviceIdType.MESH
F32 = jnp.float32
BF16 = jnp.bfloat16
EPS = 1e-05

GROUPS = 4
ROWS = 128
WIDTH = 3072
CHUNKS = 8
CW = WIDTH // CHUNKS

TILES = {
    (0, 0): [(0, g) for g in range(4)],
    (1, 1): [(0, g) for g in range(4)] + [(1, g) for g in range(4)],
    (1, 2): [(0, 2), (0, 3), (1, 2), (1, 3)],
    (1, 3): [(0, 2), (0, 3), (1, 2), (1, 3)],
    (2, 2): [(2, g) for g in range(4)] + [(0, 0), (0, 1), (1, 0), (1, 1)],
    (2, 3): [(2, g) for g in range(4)] + [(0, 0), (0, 1), (1, 0), (1, 1)],
    (3, 3): [(3, g) for g in range(4)],
}
PIECES = {
    (0, 0): [(0, 4, 0, 128)],
    (1, 1): [(0, 4, 0, 256)],
    (1, 2): [(2, 4, 0, 256)],
    (1, 3): [(2, 4, 0, 256)],
    (2, 2): [(0, 4, 256, 384), (0, 2, 0, 256)],
    (2, 3): [(0, 4, 256, 384), (0, 2, 0, 256)],
    (3, 3): [(0, 4, 384, 512)],
}


def remote(src, dst, send, recv, device):
    return pltpu.make_async_remote_copy(
        src_ref=src, dst_ref=dst, send_sem=send, recv_sem=recv, device_id=device, device_id_type=MESH
    )


def dot(a, b):
    return jnp.dot(a, b, preferred_element_type=F32)


def dot_t(a, b):
    return lax.dot_general(a, b, (((1,), (1,)), ((), ())), preferred_element_type=F32)


def loop(lo, hi, body):
    lax.fori_loop(lo, hi, lambda i, _: (body(i), None)[1], None)


def kernel(
    gated, values, upstream, gain, shift, wt, bias,
    out_u, out_v, out_mix, out_vec,
    XC, YC, UN, INV, RES, YP, PS1, PS2, PSQ, PR, PQ, ACC,
    WBUF, WX, WXT, BIASC, GX, GS, GR, GZ, ZR, YS, YR, ZS, ZG,
    VS, VA, VT, VB, VU, VC, VW, VD,
    w_s, w_r, m_s, m_r, r1_s, r1_r, r2_s, r2_r, r3_s, r3_r, r4_s, r4_r,
    v1_s, v1_r, v2_s, v2_r, v3_s, v3_r, v4_s, v4_r,
):
    z, y = lax.axis_index("z"), lax.axis_index("y")
    x, core = lax.axis_index("x"), lax.axis_index("core")
    d = x * 2 + core
    half = y // 4
    j = y % 4
    up = j // 2
    inner = (j == 1) | (j == 2)
    lower = up == 0
    upper = up == 1
    base = half * 4
    own_outer = (z, base + 3 * up, x, core)
    own_inner = (z, base + 1 + up, x, core)
    opp_inner = (z, base + 2 - up, x, core)
    opp_outer = (z, base + 3 - 3 * up, x, core)
    kx, ky = up, 1 - up

    def dp_peer(o):
        e = (d + o) % 8
        return e, (z, y, e // 2, e % 2)

    def z_peer(o):
        e = (z + o) % 8
        return e, (e, y, x, core)

    def y_peer(o):
        e = (y + o) % 8
        return e, (z, e, x, core)

    def phys(q):
        return (q + 4 * up) % 8

    barrier = pltpu.get_barrier_semaphore()

    def greet(o):
        for peer in (dp_peer, z_peer, y_peer):
            pl.semaphore_signal(barrier, inc=1, device_id=peer(o)[1], device_id_type=MESH)

    loop(1, 8, greet)

    def norm(i):
        r = pl.multiple_of(i * 16, 16)
        v = values[0, pl.ds(r, 16), :].astype(F32)
        d0 = v - jnp.sum(v, axis=1, keepdims=True) * (1.0 / WIDTH)
        inv = lax.rsqrt(jnp.sum(d0 * d0, axis=1, keepdims=True) * (1.0 / WIDTH) + EPS)
        INV[pl.ds(r, 16), :] = jnp.broadcast_to(inv, (16, 128))
        u = d0 * inv
        n = (u * gain[...] + shift[...]).astype(BF16)
        m = (upstream[0, pl.ds(r, 16), :].astype(F32) * gated[0, pl.ds(r, 16), :].astype(F32)).astype(BF16)
        for c in range(CHUNKS):
            UN[c, pl.ds(r, 16), :] = u[:, c * CW : (c + 1) * CW]

        def put(a, b):
            for c in range(CHUNKS):
                XC[c, pl.ds(r + ROWS, 16), :] = a[:, c * CW : (c + 1) * CW]
                YC[c, pl.ds(r, 16), :] = b[:, c * CW : (c + 1) * CW]

        @pl.when(lower)
        def _():
            put(n, m)

        @pl.when(upper)
        def _():
            put(m, n)

    loop(0, 8, norm)

    pl.semaphore_wait(barrier, 21)

    for (jj, t), pieces in PIECES.items():

        @pl.when((j == jj) & (x == t))
        def _(t=t, pieces=pieces):
            def send(o):
                e, peer = dp_peer(o)
                for i, (g0, g1, c0, c1) in enumerate(pieces):
                    remote(
                        wt.at[g0:g1, :, c0:c1],
                        WBUF.at[t, g0:g1, pl.ds(core * 64, 64), c0:c1],
                        w_s.at[e, i],
                        w_r.at[d, i],
                        peer,
                    ).start()

            loop(1, 8, send)

    def x_near(c, to):
        return remote(XC.at[c, pl.ds(ROWS, ROWS), :], XC.at[c, pl.ds(0, ROWS), :], m_s.at[0, c], m_r.at[0, c], to)

    def x_far(c):
        return remote(
            XC.at[c, pl.ds(ROWS, ROWS), :], YC.at[c, pl.ds(2 * ROWS, ROWS), :], m_s.at[1, c], m_r.at[2, c], opp_inner
        )

    def x_opp(c):
        return remote(
            XC.at[c, pl.ds(ROWS, ROWS), :], YC.at[c, pl.ds(ROWS, ROWS), :], m_s.at[0, c], m_r.at[1, c], opp_inner
        )

    def p_inner(c):
        return remote(PS1.at[c], PR.at[c], m_s.at[1, c], m_r.at[3, c], opp_inner)

    def p_outer(c):
        return remote(PS2.at[c], PR.at[c], m_s.at[2, c], m_r.at[3, c], opp_outer)

    def q_outer(c):
        return remote(PSQ.at[c], PQ.at[c], m_s.at[3, c], m_r.at[4, c], own_outer)

    @pl.when(inner)
    def _():
        loop(0, 4, lambda q: x_opp(phys(q)).start())

    @pl.when(jnp.logical_not(inner))
    def _():
        def send(q):
            x_near(phys(q + 4), own_inner).start()
            x_far(phys(q)).start()

        loop(0, 4, send)
        loop(0, 4, lambda q: x_near(phys(q), own_inner).start())

    VS[...] = jnp.zeros_like(VS)
    GX[...] = jnp.zeros_like(GX)
    ones = jnp.ones((8, CW), BF16)
    for g in range(GROUPS):
        rows = jnp.broadcast_to(bias[pl.ds(g, 1), pl.ds(pl.multiple_of(j * 128, 128), 128)], (128, 128))
        BIASC[g] = rows.T

    def sum_bias(source, row0):
        for g in range(GROUPS):
            s = dot_t(ones, source[2 * g, pl.ds(row0, ROWS), :]) + dot_t(ones, source[2 * g + 1, pl.ds(row0, ROWS), :])
            VS[6 + g // 2, pl.ds((g % 2) * 4 + j, 1), :] = s[0:1]

    @pl.when(lower)
    def _():
        sum_bias(YC, 0)

    @pl.when(upper)
    def _():
        sum_bias(XC, ROWS)

    WBUF[x, :, pl.ds(pl.multiple_of(core * 64, 64), 64), :] = wt[...]
    for (jj, t), pieces in PIECES.items():
        for cc in range(2):

            @pl.when((j == jj) & (d != 2 * t + cc))
            def _(t=t, cc=cc, pieces=pieces):
                for i, (g0, g1, c0, c1) in enumerate(pieces):
                    there = WBUF.at[t, g0:g1, cc * 64 : cc * 64 + 64, c0:c1]
                    remote(there, there, w_s.at[0, i], w_r.at[2 * t + cc, i], own_inner).wait_recv()

    seg_t = lax.broadcasted_iota(jnp.int32, (128, 128), 0) // 64
    seg_s = lax.broadcasted_iota(jnp.int32, (128, 128), 1) // 64
    allowed = seg_t >= seg_s

    def tile(t, s, g):
        w = WBUF[t, g, :, s * 128 : (s + 1) * 128]
        return jnp.where(allowed, w, jnp.zeros_like(w)) if t == s else w

    def place(g, dst, src, a, b):
        WX[g, dst * 128 : (dst + 1) * 128, src * 128 : (src + 1) * 128] = a
        WXT[g, src * 128 : (src + 1) * 128, dst * 128 : (dst + 1) * 128] = b

    @pl.when(j == 0)
    def _():
        for g in range(GROUPS):
            w = tile(0, 0, g)
            place(g, 0, 0, w, w.T)

    @pl.when(j == 3)
    def _():
        for g in range(GROUPS):
            w = tile(3, 3, g)
            place(g, 0, 0, w.T, w)

    @pl.when(j == 1)
    def _():
        for g in range(GROUPS):
            for t in (1, 2, 3) if g >= 2 else (1,):
                for s in (0, 1):
                    w = tile(t, s, g)
                    place(g, t - 1, s, w, w.T)

    @pl.when(j == 2)
    def _():
        for g in range(GROUPS):
            for s in (0, 1, 2) if g < 2 else (2,):
                for t in (2, 3):
                    w = tile(t, s, g)
                    place(g, 2 - s, 3 - t, w.T, w)

    def bias_of(g, on):
        b = jnp.where(on, BIASC[g], 0.0)
        return jnp.concatenate([b] * (CW // 128), axis=1)

    def put_x(c, g, value):
        RES[kx, c] = (value + bias_of(g, lower)).astype(BF16)

    def put_y(c, g, value):
        RES[ky, c] = (value + bias_of(g, upper)).astype(BF16)

    @pl.when(inner)
    def _():
        def early(q):
            c = phys(q)
            s = dot(WXT[c // 2, :, 0:ROWS], YC[c, 0:ROWS, :])
            PSQ[c] = s[0:ROWS].astype(BF16)
            YP[c] = s[ROWS:]
            q_outer(c).start()

        loop(0, 4, early)

        def second(i):
            c = phys(i + 4)
            g = c // 2
            x_near(c, own_outer).wait_recv()
            r = dot(WX[g], XC[c])
            PS1[c] = r[ROWS : 2 * ROWS].astype(BF16)
            PS2[c] = r[2 * ROWS :].astype(BF16)
            put_x(c, g, r[0:ROWS])
            p_outer(c).start()
            p_inner(c).start()
            x_opp(c).wait_recv()
            x_far(c).wait_recv()
            s = dot(WXT[g], YC[c])
            PSQ[c] = s[0:ROWS].astype(BF16)
            put_y(c, g, s[ROWS:])
            q_outer(c).start()
            GX[g] += dot_t(YC[c], XC[c])

        loop(0, 4, second)

        def first(q):
            c = phys(q)
            g = c // 2
            x_near(c, own_outer).wait_recv()
            put_x(c, g, dot(WX[g, 0:ROWS, :], XC[c]))
            GX[g, 0:ROWS, :] += dot_t(YC[c, 0:ROWS, :], XC[c])

        loop(0, 4, first)

    @pl.when(jnp.logical_not(inner))
    def _():
        def local(c):
            g = c // 2
            own_x = XC[c, pl.ds(ROWS, ROWS), :]
            own_y = YC[c, pl.ds(0, ROWS), :]
            put_x(c, g, dot(WX[g, 0:ROWS, 0:ROWS], own_x))
            YP[c] = dot(WXT[g, 0:ROWS, 0:ROWS], own_y)
            GX[g, 0:ROWS, 0:ROWS] += dot_t(own_y, own_x)

        loop(0, 8, local)

    def stage(t, index, value):
        value = value.astype(BF16)
        GS[t, 0, index] = value[0:64]
        GS[t, 1, index] = value[64:128]

    for (jj, t), tiles in TILES.items():

        @pl.when(j == jj)
        def _(jj=jj, t=t, tiles=tiles):
            for index, (s, g) in enumerate(tiles):
                if jj == 0:
                    value = GX[g, 0:128, 0:128]
                elif jj == 3:
                    value = GX[g, 0:128, 0:128].T
                elif jj == 1:
                    value = GX[g, (t - 1) * 128 : t * 128, s * 128 : (s + 1) * 128]
                else:
                    value = GX[g, (2 - s) * 128 : (3 - s) * 128, (3 - t) * 128 : (4 - t) * 128].T
                stage(t, index, value)
            n = len(tiles)
            for h in range(2):
                e = 2 * t + h

                @pl.when(d != e)
                def _():
                    remote(
                        GS.at[t, h, 0:n], GR.at[d, 0:n], r1_s.at[e], r1_r.at[d], (z, y, t, h)
                    ).start()

                @pl.when(d == e)
                def _():
                    GR[e, 0:n] = GS[t, h, 0:n]

    @pl.when(inner)
    def _():
        def late(q):
            c = phys(q)
            p_inner(c).wait_recv()
            put_y(c, c // 2, YP[c] + PR[c].astype(F32))

        loop(0, 4, late)

    @pl.when(jnp.logical_not(inner))
    def _():
        def late(q):
            c = phys(q)
            p_outer(c).wait_recv()
            q_outer(c).wait_recv()
            put_y(c, c // 2, YP[c] + PR[c].astype(F32) + PQ[c].astype(F32))

        loop(0, 4, late)

        def later(q):
            c = phys(q)
            q_outer(c).wait_recv()
            put_y(c, c // 2, YP[c] + PQ[c].astype(F32))

        loop(4, 8, later)

    def each_owned(body):
        for (jj, t), tiles in TILES.items():

            @pl.when((j == jj) & (x == t))
            def _(jj=jj, t=t, tiles=tiles):
                body(jj, t, tiles)

    def sum_dp(jj, t, tiles):
        n = len(tiles)

        def wait(o):
            e, peer = dp_peer(o)
            remote(GR.at[e, 0:n], GR.at[e, 0:n], r1_s.at[0], r1_r.at[e], peer).wait_recv()

        loop(1, 8, wait)

        def add(i):
            total = GR[0, i].astype(F32)
            for e in range(1, 8):
                total = total + GR[e, i].astype(F32)
            total = total.astype(BF16)
            for rs in range(4):
                GZ[rs, i] = total[rs * 16 : (rs + 1) * 16]

        loop(0, n, add)
        m = n // 2

        def send(o):
            e, peer = z_peer(o)
            remote(
                GZ.at[e % 4, pl.ds((e // 4) * m, m)], ZR.at[z, 0:m], r2_s.at[e], r2_r.at[z], peer
            ).start()

        loop(1, 8, send)
        ZR[z, 0:m] = GZ[z % 4, pl.ds((z // 4) * m, m)]

    each_owned(sum_dp)

    ACC[...] = jnp.zeros_like(ACC)

    def sums(c):
        back = RES[1, c].astype(F32)
        u = UN[c]
        g = gain[:, pl.ds(pl.multiple_of(c * CW, 128), CW)]
        bu = back * u
        a, b = back * g, bu * g
        ACC[0] += a[:, 0:128] + a[:, 128:256] + a[:, 256:384]
        ACC[1] += b[:, 0:128] + b[:, 128:256] + b[:, 256:384]
        gt = jnp.sum(bu, axis=0, keepdims=True)
        st = jnp.sum(back, axis=0, keepdims=True)
        for i in range(3):
            row = c * 3 + i
            VS[row // 8, pl.ds(row % 8, 1), :] = gt[:, i * 128 : (i + 1) * 128]
            VS[row // 8 + 3, pl.ds(row % 8, 1), :] = st[:, i * 128 : (i + 1) * 128]

    loop(0, CHUNKS, sums)

    def vec_send(source, land, me, send, recv, peer):
        def one(o):
            e, to = peer(o)
            remote(source(e), land.at[me], send.at[e], recv.at[me], to).start()

        loop(1, 8, one)

    def vec_wait(land, send, recv, peer):
        def one(o):
            e, to = peer(o)
            remote(land.at[e], land.at[e], send.at[e], recv.at[e], to).wait_recv()

        loop(1, 8, one)

    def vec_sum(land):
        total = land[0]
        for e in range(1, 8):
            total = total + land[e]
        return total

    vec_send(lambda e: VS.at[e], VA, d, v1_s, v1_r, dp_peer)
    VA[d] = VS[d]

    def sum_z(jj, t, tiles):
        m = len(tiles) // 2

        def wait(o):
            e, peer = z_peer(o)
            remote(ZR.at[e, 0:m], ZR.at[e, 0:m], r2_s.at[0], r2_r.at[e], peer).wait_recv()

        loop(1, 8, wait)
        total = ZR[0, 0:m].astype(F32)
        for e in range(1, 8):
            total = total + ZR[e, 0:m].astype(F32)
        YS[0:m] = total.astype(BF16)

        def send(o):
            e, peer = y_peer(o)
            remote(YS.at[0:m], YR.at[y, 0:m], r3_s.at[e], r3_r.at[y], peer).start()

        loop(1, 8, send)
        YR[y, 0:m] = YS[0:m]

    each_owned(sum_z)

    vec_wait(VA, v1_s, v1_r, dp_peer)
    VT[...] = vec_sum(VA)
    vec_send(lambda e: VT, VB, z, v2_s, v2_r, z_peer)
    VB[z] = VT[...]

    mean_a = jnp.sum(ACC[0], axis=1, keepdims=True) * (1.0 / WIDTH)
    mean_b = jnp.sum(ACC[1], axis=1, keepdims=True) * (1.0 / WIDTH)
    ACC[0] = jnp.broadcast_to(mean_a, (ROWS, 128))
    ACC[1] = jnp.broadcast_to(mean_b, (ROWS, 128))

    def wide(v):
        return jnp.concatenate([v] * (CW // 128), axis=1)

    def outputs(c):
        cols = pl.ds(pl.multiple_of(c * CW, 128), CW)
        scaled = RES[1, c].astype(F32) * gain[:, cols]
        out_v[0, :, cols] = (wide(INV[...]) * (scaled - wide(ACC[0]) - UN[c] * wide(ACC[1]))).astype(BF16)
        out_u[0, :, cols] = (upstream[0, :, cols].astype(F32) * RES[0, c].astype(F32)).astype(BF16)

    loop(0, CHUNKS, outputs)

    vec_wait(VB, v2_s, v2_r, z_peer)
    VU[...] = vec_sum(VB)
    vec_send(lambda e: VU, VC, y, v3_s, v3_r, y_peer)
    VC[y] = VU[...]

    for t in range(4):
        places = [(jj, tiles) for (jj, tt), tiles in TILES.items() if tt == t]
        total_tiles = sum(len(tiles) // 2 for _, tiles in places)

        @pl.when(x == t)
        def _(t=t, places=places, total_tiles=total_tiles):
            off = 0
            for jj, tiles in places:
                m = len(tiles) // 2
                for yy in (jj, jj + 4):

                    @pl.when(y != yy)
                    def _():
                        there = YR.at[yy, 0:m]
                        remote(there, there, r3_s.at[0], r3_r.at[yy], own_inner).wait_recv()

                for i in range(m):
                    ZS[off + i] = (YR[jj, i].astype(F32) + YR[jj + 4, i].astype(F32)).astype(BF16)
                off += m

            def send(o):
                e, peer = z_peer(o)
                remote(ZS.at[0:total_tiles], ZG.at[z, 0:total_tiles], r4_s.at[e], r4_r.at[z], peer).start()

            loop(1, 8, send)
            ZG[z, 0:total_tiles] = ZS[0:total_tiles]

    vec_wait(VC, v3_s, v3_r, y_peer)
    VW[...] = vec_sum(VC)
    vec_send(lambda e: VW, VD, d, v4_s, v4_r, dp_peer)
    VD[d] = VW[...]

    out_mix[...] = jnp.zeros_like(out_mix)
    keep = lax.broadcasted_iota(jnp.int32, (16, 128), 1) // 64 <= core
    for t in range(4):
        places = [(jj, tiles) for (jj, tt), tiles in TILES.items() if tt == t]
        total_tiles = sum(len(tiles) // 2 for _, tiles in places)

        @pl.when(x == t)
        def _(t=t, places=places, total_tiles=total_tiles):
            def wait(o):
                e, peer = z_peer(o)
                there = ZG.at[e, 0:total_tiles]
                remote(there, there, r4_s.at[0], r4_r.at[e], peer).wait_recv()

            loop(1, 8, wait)
            for k in range(8):
                rows = slice(16 * (k % 4), 16 * (k % 4) + 16)
                off = 0
                for jj, tiles in places:
                    m = len(tiles) // 2
                    for i in range(m):
                        s, g = tiles[(k // 4) * m + i]
                        value = ZG[k, off + i].astype(F32)
                        if s == t:
                            value = jnp.where(keep, value, 0.0)
                        out_mix[g, rows, s * 128 : (s + 1) * 128] = value
                    off += m

    vec_wait(VD, v4_s, v4_r, dp_peer)
    out_vec[...] = VD[...]

    for (jj, t), pieces in PIECES.items():

        @pl.when((j == jj) & (x == t))
        def _(t=t, pieces=pieces):
            def wait(o):
                e, peer = dp_peer(o)
                for i, (g0, g1, c0, c1) in enumerate(pieces):
                    remote(
                        wt.at[g0:g1, :, c0:c1],
                        WBUF.at[t, g0:g1, pl.ds(core * 64, 64), c0:c1],
                        w_s.at[e, i],
                        w_r.at[d, i],
                        peer,
                    ).wait_send()

            loop(1, 8, wait)

    @pl.when(inner)
    def _():
        def wait(q):
            x_opp(phys(q)).wait_send()
            p_outer(phys(q + 4)).wait_send()
            p_inner(phys(q + 4)).wait_send()

        loop(0, 4, wait)
        loop(0, 8, lambda q: q_outer(phys(q)).wait_send())

    @pl.when(jnp.logical_not(inner))
    def _():
        loop(0, 4, lambda q: x_far(phys(q)).wait_send())
        loop(0, 8, lambda q: x_near(phys(q), own_inner).wait_send())

    for (jj, t), tiles in TILES.items():
        n = len(tiles)
        for h in range(2):

            @pl.when((j == jj) & (d != 2 * t + h))
            def _(t=t, h=h, n=n):
                remote(
                    GS.at[t, h, 0:n], GR.at[d, 0:n], r1_s.at[2 * t + h], r1_r.at[d], (z, y, t, h)
                ).wait_send()

    def sent(jj, t, tiles):
        m = len(tiles) // 2

        def one(o):
            e, peer = z_peer(o)
            remote(GZ.at[0, 0:m], ZR.at[z, 0:m], r2_s.at[e], r2_r.at[z], peer).wait_send()
            e, peer = y_peer(o)
            remote(YS.at[0:m], YR.at[y, 0:m], r3_s.at[e], r3_r.at[y], peer).wait_send()

        loop(1, 8, one)

    each_owned(sent)
    for t in range(4):
        total_tiles = sum(len(tiles) // 2 for (_, tt), tiles in TILES.items() if tt == t)

        @pl.when(x == t)
        def _(total_tiles=total_tiles):
            def one(o):
                e, peer = z_peer(o)
                remote(ZS.at[0:total_tiles], ZG.at[z, 0:total_tiles], r4_s.at[e], r4_r.at[z], peer).wait_send()

            loop(1, 8, one)

    def vec_sent(o):
        for source, land, me, send, recv, peer in (
            (VS.at[0], VA, d, v1_s, v1_r, dp_peer),
            (VT, VB, z, v2_s, v2_r, z_peer),
            (VU, VC, y, v3_s, v3_r, y_peer),
            (VW, VD, d, v4_s, v4_r, dp_peer),
        ):
            e, to = peer(o)
            remote(source, land.at[me], send.at[e], recv.at[me], to).wait_send()

    loop(1, 8, vec_sent)


def per_device(gated, values_in, upstream, gain, shift, mix_w, mix_bias):
    vmem = pl.BlockSpec(memory_space=pltpu.VMEM)
    chunks = (CHUNKS, ROWS, CW)
    dma = pltpu.SemaphoreType.DMA
    out_u, out_v, out_mix, out_vec = pl.pallas_call(
        kernel,
        out_shape=(
            jax.ShapeDtypeStruct((1, ROWS, WIDTH), BF16),
            jax.ShapeDtypeStruct((1, ROWS, WIDTH), BF16),
            jax.ShapeDtypeStruct((GROUPS, 64, 512), F32),
            jax.ShapeDtypeStruct((8, 8, 128), F32),
        ),
        in_specs=[vmem] * 7,
        out_specs=[vmem] * 4,
        scratch_shapes=[
            pltpu.VMEM((CHUNKS, 2 * ROWS, CW), BF16),
            pltpu.VMEM((CHUNKS, 3 * ROWS, CW), BF16),
            pltpu.VMEM(chunks, F32),
            pltpu.VMEM((ROWS, 128), F32),
            pltpu.VMEM((2, *chunks), BF16),
            pltpu.VMEM(chunks, F32),
            pltpu.VMEM(chunks, BF16),
            pltpu.VMEM(chunks, BF16),
            pltpu.VMEM(chunks, BF16),
            pltpu.VMEM(chunks, BF16),
            pltpu.VMEM(chunks, BF16),
            pltpu.VMEM((2, ROWS, 128), F32),
            pltpu.VMEM((4, GROUPS, 128, 512), BF16),
            pltpu.VMEM((GROUPS, 384, 256), BF16),
            pltpu.VMEM((GROUPS, 256, 384), BF16),
            pltpu.VMEM((GROUPS, 128, 128), F32),
            pltpu.VMEM((GROUPS, 384, 256), F32),
            pltpu.VMEM((4, 2, 8, 64, 128), BF16),
            pltpu.VMEM((8, 8, 64, 128), BF16),
            pltpu.VMEM((4, 8, 16, 128), BF16),
            pltpu.VMEM((8, 4, 16, 128), BF16),
            pltpu.VMEM((4, 16, 128), BF16),
            pltpu.VMEM((8, 4, 16, 128), BF16),
            pltpu.VMEM((8, 16, 128), BF16),
            pltpu.VMEM((8, 8, 16, 128), BF16),
            pltpu.VMEM((8, 8, 128), F32),
            pltpu.VMEM((8, 8, 128), F32),
            pltpu.VMEM((8, 128), F32),
            pltpu.VMEM((8, 8, 128), F32),
            pltpu.VMEM((8, 128), F32),
            pltpu.VMEM((8, 8, 128), F32),
            pltpu.VMEM((8, 128), F32),
            pltpu.VMEM((8, 8, 128), F32),
            dma((8, 2)), dma((8, 2)), dma((4, 8)), dma((5, 8)),
            *[dma((8,)) for _ in range(16)],
        ],
        compiler_params=pltpu.CompilerParams(
            collective_id=0, has_side_effects=True, vmem_limit_bytes=48 * 1024 * 1024
        ),
        name="span",
    )(
        gated,
        values_in,
        upstream,
        gain.reshape(1, WIDTH),
        shift.reshape(1, WIDTH),
        mix_w.transpose(1, 0, 2),
        mix_bias,
    )
    vec = out_vec.reshape(64 * 128)
    return (
        out_u,
        out_v,
        out_mix.transpose(1, 0, 2),
        vec[2 * WIDTH :].reshape(GROUPS, 512),
        vec[:WIDTH],
        vec[WIDTH : 2 * WIDTH],
    )


def solution(mesh):
    torus = Mesh(mesh.devices.reshape(8, 8, 4, 2), AXES)
    return jax.shard_map(
        per_device,
        mesh=torus,
        in_specs=(
            P(DP, SP, None),
            P(DP, SP, None),
            P(DP, SP, None),
            P(),
            P(),
            P(DP, None, None),
            P(),
        ),
        out_specs=(P(DP, SP, None), P(DP, SP, None), P(DP, None, None), P(), P(), P()),
        check_vma=False,
    )
```

```python
import jax
import jax.numpy as jnp
from jax import lax
from jax.experimental import pallas as pl
from jax.experimental.pallas import tpu as pltpu
from jax.sharding import Mesh
from jax.sharding import PartitionSpec as P

AXES = ("z", "y", "x", "core")
DP = ("x", "core")
SP = ("z", "y")
MESH = pl.DeviceIdType.MESH
F32 = jnp.float32
BF16 = jnp.bfloat16
EPS = 1e-05

GROUPS = 4
ROWS = 128
WIDTH = 3072
CHUNKS = 8
CW = WIDTH // CHUNKS

TILES = {
    (0, 0): [(0, g) for g in range(4)],
    (1, 1): [(0, 2), (0, 3), (1, 2), (1, 3), (0, 0), (0, 1), (1, 0), (1, 1)],
    (1, 2): [(0, 2), (0, 3), (1, 2), (1, 3)],
    (1, 3): [(0, 2), (0, 3), (1, 2), (1, 3)],
    (2, 2): [(2, 0), (2, 1), (0, 0), (0, 1), (1, 0), (1, 1), (2, 2), (2, 3)],
    (2, 3): [(2, 0), (2, 1), (0, 0), (0, 1), (1, 0), (1, 1), (2, 2), (2, 3)],
    (3, 3): [(3, g) for g in range(4)],
}
FIRST = {(0, 0): 4, (1, 1): 4, (1, 2): 4, (1, 3): 4, (2, 2): 6, (2, 3): 6, (3, 3): 4}
ORDER = {0: (0, 1, 2, 3), 1: (0, 1, 2, 3), 2: (2, 3, 0, 1), 3: (2, 3, 0, 1)}
COLUMNS = {
    (0, 0): {g: (0, 128) for g in range(4)},
    (1, 1): {g: (0, 256) for g in range(4)},
    (1, 2): {2: (0, 256), 3: (0, 256)},
    (1, 3): {2: (0, 256), 3: (0, 256)},
    (2, 2): {0: (0, 384), 1: (0, 384), 2: (256, 384), 3: (256, 384)},
    (2, 3): {0: (0, 384), 1: (0, 384), 2: (256, 384), 3: (256, 384)},
    (3, 3): {g: (384, 512) for g in range(4)},
}


def remote(src, dst, send, recv, device):
    return pltpu.make_async_remote_copy(
        src_ref=src, dst_ref=dst, send_sem=send, recv_sem=recv, device_id=device, device_id_type=MESH
    )


def dot(a, b):
    return jnp.dot(a, b, preferred_element_type=F32)


def dot_t(a, b):
    return lax.dot_general(a, b, (((1,), (1,)), ((), ())), preferred_element_type=F32)


def loop(lo, hi, body, name="loop"):
    with jax.named_scope(name):
        lax.fori_loop(lo, hi, lambda i, _: (body(i), None)[1], None)


def kernel(
    gated_hbm, values_hbm, upstream_hbm, gain, shift, WT, bias,
    out_u, out_v, out_mix, out_vec, out_bias,
    gated, values, upstream,
    XC, YC, UN, MEAN, INV, RES, YP, PS1, PS2, PSQ, PR, PQ, ACC,
    WBUF, WX, WXT, BIASC, GX, GS, GR, GZ, ZR, YS, YR, ZS, ZG,
    VS, VA, VT, VB, VU, VC, VW, VD,
    in_s, w_s, f_s, w_r, w_r2, m_s, m_r, y_r, p_r, r1_s, r1_r, r2_s, r2_r, r3_s, r3_r, r4_s, r4_r,
    v_s, v_r,
):
    z, y = lax.axis_index("z"), lax.axis_index("y")
    x, core = lax.axis_index("x"), lax.axis_index("core")
    d = x * 2 + core
    half = y // 4
    j = y % 4
    up = j // 2
    inner = (j == 1) | (j == 2)
    outer = jnp.logical_not(inner)
    lower = up == 0
    upper = up == 1
    base = half * 4
    own_outer = (z, base + 3 * up, x, core)
    own_inner = (z, base + 1 + up, x, core)
    opp_inner = (z, base + 2 - up, x, core)
    opp_outer = (z, base + 3 - 3 * up, x, core)
    partner = (z, y, x, 1 - core)
    kx, ky = up, 1 - up

    def dp_peer(o):
        e = (d + o) % 8
        return e, (z, y, e // 2, e % 2)

    def z_peer(o):
        e = (z + o) % 8
        return e, (e, y, x, core)

    def y_peer(o):
        e = (y + o) % 8
        return e, (z, e, x, core)

    def phys(q):
        return (q + 4 * up) % 8

    big = ((values_hbm, values), (upstream_hbm, upstream), (gated_hbm, gated))

    def fetch(k, part):
        rows = pl.ds(part * 32, 32)
        source, dest = big[k]
        return pltpu.make_async_copy(source.at[0, rows, :], dest.at[rows, :], in_s.at[part if k == 0 else 3 + k])

    barrier = pltpu.get_barrier_semaphore()

    def greet(o):
        for peer in (dp_peer, z_peer, y_peer):
            pl.semaphore_signal(barrier, inc=1, device_id=peer(o)[1], device_id_type=MESH)

    @pl.when(lower)
    def _():
        for part in range(4):
            fetch(0, part).start()

    @pl.when(upper)
    def _():
        for part in range(4):
            fetch(1, part).start()
            fetch(2, part).start()

    loop(1, 8, greet, "greet")

    @pl.when(lower)
    def _():
        for part in range(4):
            fetch(1, part).start()
            fetch(2, part).start()

    @pl.when(upper)
    def _():
        for part in range(4):
            fetch(0, part).start()

    def stats(i):
        r = pl.multiple_of(i * 32, 32)
        fetch(0, i).wait()
        v = values[pl.ds(r, 32), :].astype(F32)
        mean = jnp.sum(v, axis=1, keepdims=True) * (1.0 / WIDTH)
        d0 = v - mean
        inv = lax.rsqrt(jnp.sum(d0 * d0, axis=1, keepdims=True) * (1.0 / WIDTH) + EPS)
        MEAN[pl.ds(r, 32), :] = jnp.broadcast_to(mean, (32, 128))
        INV[pl.ds(r, 32), :] = jnp.broadcast_to(inv, (32, 128))

    def wide(v):
        return jnp.concatenate([v] * (CW // 128), axis=1)

    def columns(c):
        return pl.ds(pl.multiple_of(c * CW, 128), CW)

    def norm(c, dest, row0):
        cols = columns(c)
        u = (values[:, cols].astype(F32) - wide(MEAN[...])) * wide(INV[...])
        UN[c] = u
        dest[c, row0 : row0 + ROWS, :] = (u * gain[:, cols] + shift[:, cols]).astype(BF16)

    def mix_grad(c, dest, row0):
        cols = columns(c)
        dest[c, row0 : row0 + ROWS, :] = (upstream[:, cols].astype(F32) * gated[:, cols].astype(F32)).astype(BF16)

    def fetched_pair():
        for k in (1, 2):
            source, dest = big[k]
            pltpu.make_async_copy(source.at[0], dest, in_s.at[3 + k]).wait()

    @pl.when(lower)
    def _():
        loop(0, 4, stats, "stats")

    @pl.when(upper)
    def _():
        fetched_pair()

    with jax.named_scope("barrier"):
        pl.semaphore_wait(barrier, 21)

    def x_near(c, to):
        return remote(XC.at[c, pl.ds(ROWS, ROWS), :], XC.at[c, pl.ds(0, ROWS), :], m_s.at[1], m_r.at[c], to)

    def x_far(c):
        return remote(
            XC.at[c, pl.ds(ROWS, ROWS), :], YC.at[c, pl.ds(2 * ROWS, ROWS), :], m_s.at[0], y_r.at[c % 4], opp_inner
        )

    def x_opp(c):
        return remote(
            XC.at[c, pl.ds(ROWS, ROWS), :], YC.at[c, pl.ds(ROWS, ROWS), :], m_s.at[0], y_r.at[c % 4], opp_inner
        )

    def p_inner(c):
        return remote(PS1.at[c], PR.at[c], m_s.at[1], p_r.at[c % 4], opp_inner)

    def p_outer(c):
        return remote(PS2.at[c], PR.at[c], m_s.at[1], p_r.at[c % 4], opp_outer)

    def q_outer(c):
        return remote(PSQ.at[c], PQ.at[c], m_s.at[0], m_r.at[c], own_outer)

    def make_x(c):
        @pl.when(lower)
        def _():
            norm(c, XC, ROWS)

        @pl.when(upper)
        def _():
            mix_grad(c, XC, ROWS)

    @pl.when(inner)
    def _():
        def send(q):
            c = phys(q)
            make_x(c)
            x_opp(c).start()

        loop(0, 4, send, "make_x")

    @pl.when(outer)
    def _():
        def send(q):
            c = phys(q + 4)
            make_x(c)
            x_near(c, own_inner).start()
            c = phys(q)
            make_x(c)
            x_far(c).start()

        loop(0, 4, send, "make_x")
        loop(0, 4, lambda q: x_near(phys(q), own_inner).start())

    def w_rows(t, g, h):
        c0, c1 = COLUMNS[t][g]
        return WBUF.at[t[1], g, pl.ds(h * 64, 64), c0:c1]

    def w_send(key, g, o):
        c0, c1 = COLUMNS[key][g]
        to = partner if o == 0 else (z, y, (x + o) % 4, core)
        land = w_r2.at[g] if o == 0 else w_r.at[key[1], g]
        return remote(WT.at[g, :, c0:c1], w_rows(key, g, core), w_s.at[0], land, to)

    for key in COLUMNS:

        @pl.when((j == key[0]) & (x == key[1]))
        def _(key=key):
            for g in ORDER[key[0]]:
                if g in COLUMNS[key]:
                    for o in (2, 1, 3, 0):
                        w_send(key, g, o).start()

    WBUF[x, :, pl.ds(pl.multiple_of(core * 64, 64), 64), :] = WT[...]

    @pl.when(inner)
    def _():
        loop(4, 8, lambda q: make_x(phys(q)), "make_x")

    @pl.when(lower)
    def _():
        fetched_pair()
        loop(0, CHUNKS, lambda c: mix_grad(c, YC, 0), "mix_grad")

    @pl.when(upper)
    def _():
        loop(0, 4, stats, "stats")
        loop(0, CHUNKS, lambda c: norm(c, YC, 0), "norm")

    VS[...] = jnp.zeros_like(VS)
    GX[...] = jnp.zeros_like(GX)
    ACC[...] = jnp.zeros_like(ACC)
    ones = jnp.ones((8, CW), BF16)
    for g in range(GROUPS):
        rows = jnp.broadcast_to(bias[pl.ds(g, 1), pl.ds(pl.multiple_of(j * 128, 128), 128)], (128, 128))
        BIASC[g] = rows.T

    def sum_bias(source, row0):
        for g in range(GROUPS):
            s = dot_t(ones, source[2 * g, pl.ds(row0, ROWS), :]) + dot_t(ones, source[2 * g + 1, pl.ds(row0, ROWS), :])
            VS[6 + g // 2, pl.ds((g % 2) * 4 + j, 1), :] = s[0:1]

    @pl.when(lower)
    def _():
        sum_bias(YC, 0)

    @pl.when(upper)
    def _():
        sum_bias(XC, ROWS)

    seg_t = lax.broadcasted_iota(jnp.int32, (128, 128), 0) // 64
    seg_s = lax.broadcasted_iota(jnp.int32, (128, 128), 1) // 64
    allowed = seg_t >= seg_s

    def tile(t, s, g):
        w = WBUF[t, g, :, s * 128 : (s + 1) * 128]
        return jnp.where(allowed, w, jnp.zeros_like(w)) if t == s else w

    def place(g, dst, src, a, b):
        WX[g, dst * 128 : (dst + 1) * 128, src * 128 : (src + 1) * 128] = a
        WXT[g, src * 128 : (src + 1) * 128, dst * 128 : (dst + 1) * 128] = b

    def w_relay(key, g):
        rows = w_rows(key, g, core)
        return remote(rows, rows, f_s.at[key[1]], w_r2.at[g], partner)

    def w_ready(jj, g):
        keys = [key for key in COLUMNS if key[0] == jj and g in COLUMNS[key]]
        with jax.named_scope("w_wait"):
            for key in keys:

                @pl.when(x != key[1])
                def _(key=key):
                    rows = w_rows(key, g, core)
                    remote(rows, rows, w_s.at[0], w_r.at[key[1], g], partner).wait_recv()
                    w_relay(key, g).start()

            c0, c1 = COLUMNS[keys[0]][g]
            rows = WBUF.at[0 : len(keys), g, 0:64, c0:c1]
            remote(rows, rows, w_s.at[0], w_r2.at[g], partner).wait_recv()
        if jj == 0:
            w = tile(0, 0, g)
            place(g, 0, 0, w, w.T)
        elif jj == 3:
            w = tile(3, 3, g)
            place(g, 0, 0, w.T, w)
        elif jj == 1:
            for t in (1, 2, 3) if g >= 2 else (1,):
                for s in (0, 1):
                    w = tile(t, s, g)
                    place(g, t - 1, s, w, w.T)
        else:
            for s in (0, 1, 2) if g < 2 else (2,):
                for t in (2, 3):
                    w = tile(t, s, g)
                    place(g, 2 - s, 3 - t, w.T, w)

    def bias_of(g, on):
        b = jnp.where(on, BIASC[g], 0.0)
        return jnp.concatenate([b] * (CW // 128), axis=1)

    def sums(c, value):
        back = value.astype(F32)
        u = UN[c]
        g = gain[:, columns(c)]
        bu = back * u
        a, b = back * g, bu * g
        ACC[0] += a[:, 0:128] + a[:, 128:256] + a[:, 256:384]
        ACC[1] += b[:, 0:128] + b[:, 128:256] + b[:, 256:384]
        gt = jnp.sum(bu, axis=0, keepdims=True)
        st = jnp.sum(back, axis=0, keepdims=True)
        for i in range(3):
            row = c * 3 + i
            VS[row // 8, pl.ds(row % 8, 1), :] = gt[:, i * 128 : (i + 1) * 128]
            VS[row // 8 + 3, pl.ds(row % 8, 1), :] = st[:, i * 128 : (i + 1) * 128]

    def put_x(c, g, value):
        value = (value + bias_of(g, lower)).astype(BF16)
        RES[kx, c] = value

        @pl.when(upper)
        def _():
            sums(c, value)

    def put_y(c, g, value):
        value = (value + bias_of(g, upper)).astype(BF16)
        RES[ky, c] = value

        @pl.when(lower)
        def _():
            sums(c, value)

    def stage(part):
        for key, tiles in TILES.items():
            jj, t = key
            lo, hi = ((0, FIRST[key]), (FIRST[key], len(tiles)))[part]
            if lo == hi:
                continue

            @pl.when(j == jj)
            def _(jj=jj, t=t, tiles=tiles, lo=lo, hi=hi):
                for index in range(lo, hi):
                    s, g = tiles[index]
                    if jj == 0:
                        value = GX[g, 0:128, 0:128]
                    elif jj == 3:
                        value = GX[g, 0:128, 0:128].T
                    elif jj == 1:
                        value = GX[g, (t - 1) * 128 : t * 128, s * 128 : (s + 1) * 128]
                    else:
                        value = GX[g, (2 - s) * 128 : (3 - s) * 128, (3 - t) * 128 : (4 - t) * 128].T
                    value = value.astype(BF16)
                    GS[t, 0, index] = value[0:64]
                    GS[t, 1, index] = value[64:128]
                for h in range(2):
                    e = 2 * t + h

                    @pl.when(d != e)
                    def _():
                        remote(
                            GS.at[t, h, lo:hi], GR.at[d, lo:hi], r1_s.at[part, t], r1_r.at[part], (z, y, t, h)
                        ).start()

                    @pl.when(d == e)
                    def _():
                        GR[e, lo:hi] = GS[t, h, lo:hi]

    def sum_dp(key, tiles):
        n = len(tiles)
        lo = FIRST[key]

        with jax.named_scope("r1_wait"):
            for part, (a, b) in enumerate(((0, lo), (lo, n))):
                if a < b:
                    there = GR.at[0:7, a:b]
                    remote(there, there, r1_s.at[0, 0], r1_r.at[part], partner).wait_recv()

        def add(i):
            total = GR[0, i].astype(F32)
            for e in range(1, 8):
                total = total + GR[e, i].astype(F32)
            total = total.astype(BF16)
            for rs in range(4):
                GZ[rs, i] = total[rs * 16 : (rs + 1) * 16]

        loop(0, n, add, "dp_add")
        m = n // 2

        def send(o):
            e, peer = z_peer(o)
            remote(GZ.at[e % 4, pl.ds((e // 4) * m, m)], ZR.at[z, 0:m], r2_s.at[0], r2_r.at[0], peer).start()

        loop(1, 8, send, "r2_send")
        ZR[z, 0:m] = GZ[z % 4, pl.ds((z // 4) * m, m)]

    def sum_z(key, tiles):
        jj = key[0]
        m = len(tiles) // 2

        with jax.named_scope("r2_wait"):
            there = ZR.at[0:7, 0:m]
            remote(there, there, r2_s.at[0], r2_r.at[0], partner).wait_recv()
        total = ZR[0, 0:m].astype(F32)
        for e in range(1, 8):
            total = total + ZR[e, 0:m].astype(F32)
        YS[0:m] = total.astype(BF16)

        def send(o):
            e, peer = y_peer(o)
            remote(YS.at[0:m], YR.at[y, 0:m], r3_s.at[0], r3_r.at[jj], peer).start()

        loop(1, 8, send, "r3_send")
        YR[y, 0:m] = YS[0:m]

    @pl.when(inner)
    def _():
        def early(c):
            s = dot(WXT[c // 2, :, 0:ROWS], YC[c, 0:ROWS, :])
            PSQ[c] = s[0:ROWS].astype(BF16)
            YP[c] = s[ROWS:]
            q_outer(c).start()

        def second(c):
            g = c // 2
            with jax.named_scope("wait_x"):
                x_near(c, own_outer).wait_recv()
            r = dot(WX[g], XC[c])
            PS1[c] = r[ROWS : 2 * ROWS].astype(BF16)
            PS2[c] = r[2 * ROWS :].astype(BF16)
            put_x(c, g, r[0:ROWS])
            p_outer(c).start()
            p_inner(c).start()
            with jax.named_scope("wait_y"):
                both_y = YC.at[c, pl.ds(ROWS, 2 * ROWS), :]
                remote(both_y, both_y, m_s.at[0], y_r.at[c % 4], opp_inner).wait_recv()
            s = dot(WXT[g], YC[c])
            PSQ[c] = s[0:ROWS].astype(BF16)
            put_y(c, g, s[ROWS:])
            q_outer(c).start()
            GX[g] += dot_t(YC[c], XC[c])

        for i in range(4):
            for jj in (1, 2):

                @pl.when(j == jj)
                def _(jj=jj, i=i):
                    w_ready(jj, ORDER[jj][i])

            if i < 2:
                loop(2 * i, 2 * i + 2, lambda q: early(phys(q)), "early")
            else:
                loop(2 * i, 2 * i + 2, lambda q: second(phys(q)), "second")

    @pl.when(inner)
    def _():
        stage(0)

        def first(q):
            c = phys(q)
            g = c // 2
            x_near(c, own_outer).wait_recv()
            put_x(c, g, dot(WX[g, 0:ROWS, :], XC[c]))
            GX[g, 0:ROWS, :] += dot_t(YC[c, 0:ROWS, :], XC[c])

        loop(0, 4, first, "first")
        stage(1)

    @pl.when(outer)
    def _():
        for jj in (0, 3):

            @pl.when(j == jj)
            def _(jj=jj):
                for g in ORDER[jj]:
                    w_ready(jj, g)

        def local(c):
            g = c // 2
            own_x = XC[c, pl.ds(ROWS, ROWS), :]
            own_y = YC[c, pl.ds(0, ROWS), :]
            put_x(c, g, dot(WX[g, 0:ROWS, 0:ROWS], own_x))
            YP[c] = dot(WXT[g, 0:ROWS, 0:ROWS], own_y)
            GX[g, 0:ROWS, 0:ROWS] += dot_t(own_y, own_x)

        loop(0, 8, local, "local")
        stage(0)

    def late_inner(q):
        c = phys(q)
        p_inner(c).wait_recv()
        put_y(c, c // 2, YP[c] + PR[c].astype(F32))

    def late_outer(q):
        c = phys(q)
        q_outer(c).wait_recv()
        p_outer(c).wait_recv()
        put_y(c, c // 2, YP[c] + PR[c].astype(F32) + PQ[c].astype(F32))

    def later_outer(q):
        c = phys(q)
        q_outer(c).wait_recv()
        put_y(c, c // 2, YP[c] + PQ[c].astype(F32))

    def owned(places, body):
        for key, tiles in TILES.items():
            if key[0] in places:

                @pl.when((j == key[0]) & (x == key[1]))
                def _(key=key, tiles=tiles):
                    body(key, tiles)

    @pl.when(inner)
    def _():
        loop(0, 3, late_inner, "late_inner")
        owned((1, 2), sum_dp)
        loop(3, 4, late_inner, "late_inner")

    def both(q):
        later_outer(q + 4)
        late_outer(q)

    @pl.when(outer)
    def _():
        owned((0, 3), sum_dp)
        loop(0, 1, both, "late_outer")
        owned((0, 3), sum_z)
        loop(1, 4, both, "late_outer")

    def vec_send(source, land, me, k, peer):
        for o in range(1, 8):
            e, to = peer(o)
            remote(source(e), land.at[me], v_s.at[k], v_r.at[k], to).start()

    def vec_wait(land, k):
        with jax.named_scope("v_wait"):
            remote(land.at[0:7], land.at[0:7], v_s.at[k], v_r.at[k], partner).wait()

    def vec_sum(land):
        total = land[0]
        for e in range(1, 8):
            total = total + land[e]
        return total

    vec_send(lambda e: VS.at[e], VA, d, 0, dp_peer)
    VA[d] = VS[d]

    @pl.when(inner)
    def _():
        owned((1, 2), sum_z)

    vec_wait(VA, 0)
    VT[...] = vec_sum(VA)
    vec_send(lambda e: VT, VB, z, 1, z_peer)
    VB[z] = VT[...]

    mean_a = jnp.sum(ACC[0], axis=1, keepdims=True) * (1.0 / WIDTH)
    mean_b = jnp.sum(ACC[1], axis=1, keepdims=True) * (1.0 / WIDTH)
    ACC[0] = jnp.broadcast_to(mean_a, (ROWS, 128))
    ACC[1] = jnp.broadcast_to(mean_b, (ROWS, 128))

    def outputs(c):
        cols = columns(c)
        scaled = RES[1, c].astype(F32) * gain[:, cols]
        out_v[0, :, cols] = (wide(INV[...]) * (scaled - wide(ACC[0]) - UN[c] * wide(ACC[1]))).astype(BF16)
        out_u[0, :, cols] = (upstream[:, cols].astype(F32) * RES[0, c].astype(F32)).astype(BF16)

    loop(0, CHUNKS, outputs, "outputs")

    vec_wait(VB, 1)
    VU[...] = vec_sum(VB)
    vec_send(lambda e: VU, VC, y, 2, y_peer)
    VC[y] = VU[...]

    for t in range(4):
        places = [(jj, tiles) for (jj, tt), tiles in TILES.items() if tt == t]
        total_tiles = sum(len(tiles) // 2 for _, tiles in places)

        @pl.when(x == t)
        def _(t=t, places=places, total_tiles=total_tiles):
            off = 0
            for jj, tiles in places:
                m = len(tiles) // 2
                for count in (1, 2):

                    @pl.when((j == jj) if count == 1 else (j != jj))
                    @jax.named_scope("r3_wait")
                    def _():
                        there = YR.at[0:count, 0:m]
                        remote(there, there, r3_s.at[0], r3_r.at[jj], partner).wait_recv()

                for i in range(m):
                    ZS[off + i] = (YR[jj, i].astype(F32) + YR[jj + 4, i].astype(F32)).astype(BF16)
                off += m

            def send(o):
                e, peer = z_peer(o)
                remote(ZS.at[0:total_tiles], ZG.at[z, 0:total_tiles], r4_s.at[0], r4_r.at[0], peer).start()

            loop(1, 8, send, "r4_send")
            ZG[z, 0:total_tiles] = ZS[0:total_tiles]

    for key in COLUMNS:

        total = sum(c1 - c0 for c0, c1 in COLUMNS[key].values())
        groups = 2 if total % 512 == 0 and key != (1, 1) and key[0] != 0 and key[0] != 3 else 4
        cols = total // groups

        @pl.when((j == key[0]) & (x == key[1]))
        def _(groups=groups, cols=cols):
            rows = WBUF.at[0:4, 0:groups, 0:64, 0:cols]
            remote(rows, rows, w_s.at[0], w_r2.at[0], partner).wait_send()

        @pl.when((j == key[0]) & (x != key[1]))
        def _(key=key, groups=groups, cols=cols):
            rows = WBUF.at[0, 0:groups, 0:64, 0:cols]
            remote(rows, rows, f_s.at[key[1]], w_r2.at[0], partner).wait_send()

    def chunks_left(source, sem):
        remote(source, source, m_s.at[sem], m_r.at[0], own_inner).wait_send()

    @pl.when(inner)
    def _():
        chunks_left(YC.at[0:4], 0)
        chunks_left(PS1, 1)

    @pl.when(outer)
    def _():
        chunks_left(PS1.at[0:4], 0)
        chunks_left(PS1, 1)

    for key, tiles in TILES.items():
        jj, t = key
        for part, (lo, hi) in enumerate(((0, FIRST[key]), (FIRST[key], len(tiles)))):
            for count in (1, 2):
                if lo < hi:

                    @pl.when((j == jj) & ((x == t) if count == 1 else (x != t)))
                    def _(t=t, count=count, lo=lo, hi=hi, part=part):
                        there = GS.at[0, 0:count, lo:hi]
                        remote(there, there, r1_s.at[part, t], r1_r.at[part], partner).wait_send()

    def sent(key, tiles):
        m = len(tiles) // 2

        there = ZR.at[0:7, 0:m]
        remote(there, there, r2_s.at[0], r2_r.at[0], partner).wait_send()
        remote(there, there, r3_s.at[0], r3_r.at[0], partner).wait_send()

    owned((0, 1, 2, 3), sent)

    vec_wait(VC, 2)
    VW[...] = vec_sum(VC)
    vec_send(lambda e: VW, VD, d, 3, dp_peer)
    VD[d] = VW[...]

    out_mix[...] = jnp.zeros_like(out_mix)
    keep = lax.broadcasted_iota(jnp.int32, (16, 128), 1) // 64 <= core
    for t in range(4):
        places = [(jj, tiles) for (jj, tt), tiles in TILES.items() if tt == t]
        total_tiles = sum(len(tiles) // 2 for _, tiles in places)

        @pl.when(x == t)
        def _(t=t, places=places, total_tiles=total_tiles):
            with jax.named_scope("r4_wait"):
                there = ZG.at[0:7, 0:total_tiles]
                remote(there, there, r4_s.at[0], r4_r.at[0], partner).wait()
            for k in range(8):
                rows = slice(16 * (k % 4), 16 * (k % 4) + 16)
                off = 0
                for jj, tiles in places:
                    m = len(tiles) // 2
                    for i in range(m):
                        s, g = tiles[(k // 4) * m + i]
                        value = ZG[k, off + i].astype(F32)
                        if s == t:
                            value = jnp.where(keep, value, 0.0)
                        out_mix[rows, g, s * 128 : (s + 1) * 128] = value
                    off += m

    vec_wait(VD, 3)
    out_vec[...] = VD[0:6]
    for g in range(GROUPS):
        for k in range(4):
            out_bias[g : g + 1, k * 128 : (k + 1) * 128] = VD[6 + g // 2, (g % 2) * 4 + k : (g % 2) * 4 + k + 1]


def writer(u, v, mix, vec, bias, out_u, out_v, out_mix, out_bias, out_gain, out_shift, sems):
    copies = [
        pltpu.make_async_copy(source, dest, sems.at[i])
        for i, (source, dest) in enumerate(
            (
                (u, out_u),
                (v, out_v),
                (mix, out_mix),
                (bias, out_bias),
                (vec.at[0:3], out_gain),
                (vec.at[3:6], out_shift),
            )
        )
    ]
    for copy in copies:
        copy.start()
    for copy in copies:
        copy.wait()


def per_device(gated, values_in, upstream, gain, shift, mix_w, mix_bias):
    vmem = pl.BlockSpec(memory_space=pltpu.VMEM)
    hbm = pl.BlockSpec(memory_space=pltpu.HBM)
    chunks = (CHUNKS, ROWS, CW)
    dma = pltpu.SemaphoreType.DMA
    results = pl.pallas_call(
        kernel,
        out_shape=(
            jax.ShapeDtypeStruct((1, ROWS, WIDTH), BF16),
            jax.ShapeDtypeStruct((1, ROWS, WIDTH), BF16),
            jax.ShapeDtypeStruct((64, GROUPS, 512), F32),
            jax.ShapeDtypeStruct((6, 8, 128), F32),
            jax.ShapeDtypeStruct((GROUPS, 512), F32),
        ),
        in_specs=[hbm] * 3 + [vmem] * 4,
        out_specs=[vmem] * 5,
        scratch_shapes=[
            pltpu.VMEM((ROWS, WIDTH), BF16),
            pltpu.VMEM((ROWS, WIDTH), BF16),
            pltpu.VMEM((ROWS, WIDTH), BF16),
            pltpu.VMEM((CHUNKS, 2 * ROWS, CW), BF16),
            pltpu.VMEM((CHUNKS, 3 * ROWS, CW), BF16),
            pltpu.VMEM(chunks, F32),
            pltpu.VMEM((ROWS, 128), F32),
            pltpu.VMEM((ROWS, 128), F32),
            pltpu.VMEM((2, *chunks), BF16),
            pltpu.VMEM(chunks, F32),
            pltpu.VMEM(chunks, BF16),
            pltpu.VMEM(chunks, BF16),
            pltpu.VMEM(chunks, BF16),
            pltpu.VMEM(chunks, BF16),
            pltpu.VMEM(chunks, BF16),
            pltpu.VMEM((2, ROWS, 128), F32),
            pltpu.VMEM((4, GROUPS, 128, 512), BF16),
            pltpu.VMEM((GROUPS, 384, 256), BF16),
            pltpu.VMEM((GROUPS, 256, 384), BF16),
            pltpu.VMEM((GROUPS, 128, 128), F32),
            pltpu.VMEM((GROUPS, 384, 256), F32),
            pltpu.VMEM((4, 2, 8, 64, 128), BF16),
            pltpu.VMEM((8, 8, 64, 128), BF16),
            pltpu.VMEM((4, 8, 16, 128), BF16),
            pltpu.VMEM((8, 4, 16, 128), BF16),
            pltpu.VMEM((4, 16, 128), BF16),
            pltpu.VMEM((8, 4, 16, 128), BF16),
            pltpu.VMEM((8, 16, 128), BF16),
            pltpu.VMEM((8, 8, 16, 128), BF16),
            pltpu.VMEM((8, 8, 128), F32),
            pltpu.VMEM((8, 8, 128), F32),
            pltpu.VMEM((8, 128), F32),
            pltpu.VMEM((8, 8, 128), F32),
            pltpu.VMEM((8, 128), F32),
            pltpu.VMEM((8, 8, 128), F32),
            pltpu.VMEM((8, 128), F32),
            pltpu.VMEM((8, 8, 128), F32),
            dma((6,)), dma((1,)), dma((4,)), dma((4, 4)), dma((4,)), dma((2,)), dma((8,)), dma((4,)), dma((4,)),
            dma((2, 4)), dma((2,)), dma((1,)), dma((1,)), dma((1,)), dma((4,)), dma((1,)), dma((1,)),
            dma((4,)), dma((4,)),
        ],
        compiler_params=pltpu.CompilerParams(
            collective_id=0, has_side_effects=True, vmem_limit_bytes=67043328 - 13312 * 1024
        ),
        name="span",
    )(
        gated,
        values_in,
        upstream,
        gain.reshape(1, WIDTH),
        shift.reshape(1, WIDTH),
        mix_w.transpose(1, 0, 2),
        mix_bias,
    )
    out_u, out_v, out_mix, out_bias, out_gain, out_shift = pl.pallas_call(
        writer,
        out_shape=(
            jax.ShapeDtypeStruct((1, ROWS, WIDTH), BF16),
            jax.ShapeDtypeStruct((1, ROWS, WIDTH), BF16),
            jax.ShapeDtypeStruct((64, GROUPS, 512), F32),
            jax.ShapeDtypeStruct((GROUPS, 512), F32),
            jax.ShapeDtypeStruct((3, 8, 128), F32),
            jax.ShapeDtypeStruct((3, 8, 128), F32),
        ),
        in_specs=[vmem] * 5,
        out_specs=[hbm] * 6,
        scratch_shapes=[dma((6,))],
        compiler_params=pltpu.CompilerParams(vmem_limit_bytes=1024 * 1024),
        name="writer",
    )(*results)
    return (out_u, out_v, out_mix, out_bias, out_gain.reshape(WIDTH), out_shift.reshape(WIDTH))


def solution(mesh):
    torus = Mesh(mesh.devices.reshape(8, 8, 4, 2), AXES)
    return jax.shard_map(
        per_device,
        mesh=torus,
        in_specs=(
            P(DP, SP, None),
            P(DP, SP, None),
            P(DP, SP, None),
            P(),
            P(),
            P(DP, None, None),
            P(),
        ),
        out_specs=(P(DP, SP, None), P(DP, SP, None), P(DP, None, None), P(), P(), P()),
        check_vma=False,
    )
```

```python
import jax
import jax.numpy as jnp
from jax import lax
from jax.experimental import pallas as pl
from jax.experimental.pallas import tpu as pltpu
from jax.sharding import Mesh
from jax.sharding import PartitionSpec as P

AXES = ("z", "y", "x", "core")
DP = ("x", "core")
SP = ("z", "y")
MESH = pl.DeviceIdType.MESH
F32 = jnp.float32
BF16 = jnp.bfloat16
EPS = 1e-05

GROUPS = 4
ROWS = 128
WIDTH = 3072
CHUNKS = 8
CW = WIDTH // CHUNKS

TILES = {
    (0, 0): [(0, g) for g in range(4)],
    (1, 1): [(0, 2), (0, 3), (1, 2), (1, 3), (0, 0), (0, 1), (1, 0), (1, 1)],
    (1, 2): [(0, 2), (0, 3), (1, 2), (1, 3)],
    (1, 3): [(0, 2), (0, 3), (1, 2), (1, 3)],
    (2, 2): [(2, 0), (2, 1), (0, 0), (0, 1), (1, 0), (1, 1), (2, 2), (2, 3)],
    (2, 3): [(2, 0), (2, 1), (0, 0), (0, 1), (1, 0), (1, 1), (2, 2), (2, 3)],
    (3, 3): [(3, g) for g in range(4)],
}
FIRST = {(0, 0): 4, (1, 1): 4, (1, 2): 4, (1, 3): 4, (2, 2): 6, (2, 3): 6, (3, 3): 4}
ORDER = {0: (0, 1, 2, 3), 1: (0, 1, 2, 3), 2: (2, 3, 0, 1), 3: (2, 3, 0, 1)}
COLUMNS = {
    (0, 0): {g: (0, 128) for g in range(4)},
    (1, 1): {g: (0, 256) for g in range(4)},
    (1, 2): {2: (0, 256), 3: (0, 256)},
    (1, 3): {2: (0, 256), 3: (0, 256)},
    (2, 2): {0: (0, 384), 1: (0, 384), 2: (256, 384), 3: (256, 384)},
    (2, 3): {0: (0, 384), 1: (0, 384), 2: (256, 384), 3: (256, 384)},
    (3, 3): {g: (384, 512) for g in range(4)},
}


def remote(src, dst, send, recv, device):
    return pltpu.make_async_remote_copy(
        src_ref=src, dst_ref=dst, send_sem=send, recv_sem=recv, device_id=device, device_id_type=MESH
    )


def dot(a, b):
    return jnp.dot(a, b, preferred_element_type=F32)


def dot_t(a, b):
    return lax.dot_general(a, b, (((1,), (1,)), ((), ())), preferred_element_type=F32)


def loop(lo, hi, body, name="loop"):
    with jax.named_scope(name):
        lax.fori_loop(lo, hi, lambda i, _: (body(i), None)[1], None)


def kernel(
    gated_hbm, values_hbm, upstream_hbm, gain, shift, WT, bias,
    out_u, out_v, out_mix, out_vec, out_bias,
    gated, values, upstream,
    XC, XF, YC, UN, MEAN, INV, RES, YP, PS1, PS2, PSQ, PR, PQ, ACC,
    WBUF, WX, WXT, BIASC, GX, GS, GR, GZ, ZR, YS, YR, ZS, ZG,
    VS, VA, VT, VB, VU, VC, VW, VD,
    in_s, w_s, f_s, w_r, w_r2, m_s, m_r, y_r, p_r, r1_s, r1_r, r2_s, r2_r, r3_s, r3_r, r4_s, r4_r,
    v_s, v_r,
):
    z, y = lax.axis_index("z"), lax.axis_index("y")
    x, core = lax.axis_index("x"), lax.axis_index("core")
    d = x * 2 + core
    half = y // 4
    j = y % 4
    up = j // 2
    inner = (j == 1) | (j == 2)
    outer = jnp.logical_not(inner)
    lower = up == 0
    upper = up == 1
    base = half * 4
    own_outer = (z, base + 3 * up, x, core)
    own_inner = (z, base + 1 + up, x, core)
    opp_inner = (z, base + 2 - up, x, core)
    opp_outer = (z, base + 3 - 3 * up, x, core)
    partner = (z, y, x, 1 - core)
    kx, ky = up, 1 - up

    def dp_peer(o):
        e = (d + o) % 8
        return e, (z, y, e // 2, e % 2)

    def z_peer(o):
        e = (z + o) % 8
        return e, (e, y, x, core)

    def y_peer(o):
        e = (y + o) % 8
        return e, (z, e, x, core)

    def phys(q):
        return (q + 4 * up) % 8

    big = ((values_hbm, values), (upstream_hbm, upstream), (gated_hbm, gated))

    def fetch(k, part):
        rows = pl.ds(part * 32, 32)
        source, dest = big[k]
        return pltpu.make_async_copy(source.at[0, rows, :], dest.at[rows, :], in_s.at[part if k == 0 else 3 + k])

    barrier = pltpu.get_barrier_semaphore()

    def greet(o):
        for peer in (dp_peer, z_peer, y_peer):
            pl.semaphore_signal(barrier, inc=1, device_id=peer(o)[1], device_id_type=MESH)

    @pl.when(lower)
    def _():
        for part in range(4):
            fetch(0, part).start()

    @pl.when(upper)
    def _():
        for part in range(4):
            fetch(1, part).start()
            fetch(2, part).start()

    loop(1, 8, greet, "greet")

    @pl.when(lower)
    def _():
        for part in range(4):
            fetch(1, part).start()
            fetch(2, part).start()

    @pl.when(upper)
    def _():
        for part in range(4):
            fetch(0, part).start()

    def stats(i):
        r = pl.multiple_of(i * 32, 32)
        fetch(0, i).wait()
        v = values[pl.ds(r, 32), :].astype(F32)
        mean = jnp.sum(v, axis=1, keepdims=True) * (1.0 / WIDTH)
        d0 = v - mean
        inv = lax.rsqrt(jnp.sum(d0 * d0, axis=1, keepdims=True) * (1.0 / WIDTH) + EPS)
        MEAN[pl.ds(r, 32), :] = jnp.broadcast_to(mean, (32, 128))
        INV[pl.ds(r, 32), :] = jnp.broadcast_to(inv, (32, 128))

    def wide(v):
        return jnp.concatenate([v] * (CW // 128), axis=1)

    def columns(c):
        return pl.ds(pl.multiple_of(c * CW, 128), CW)

    def norm(c, dest, row0, far=False):
        cols = columns(c)
        u = (values[:, cols].astype(F32) - wide(MEAN[...])) * wide(INV[...])
        UN[c] = u
        if far:
            XF[c % 4] = u.astype(BF16)
        dest[c, row0 : row0 + ROWS, :] = (u * gain[:, cols] + shift[:, cols]).astype(BF16)

    def mix_grad(c, dest, row0, far=False):
        cols = columns(c)
        m = (upstream[:, cols].astype(F32) * gated[:, cols].astype(F32)).astype(BF16)
        if far:
            XF[c % 4] = m
        dest[c, row0 : row0 + ROWS, :] = m

    def fetched_pair():
        for k in (1, 2):
            source, dest = big[k]
            pltpu.make_async_copy(source.at[0], dest, in_s.at[3 + k]).wait()

    @pl.when(lower)
    def _():
        loop(0, 4, stats, "stats")

    @pl.when(upper)
    def _():
        fetched_pair()

    with jax.named_scope("barrier"):
        pl.semaphore_wait(barrier, 21)

    def x_near(c, to):
        return remote(XC.at[c, pl.ds(ROWS, ROWS), :], XC.at[c, pl.ds(0, ROWS), :], m_s.at[1], m_r.at[c], to)

    def x_far(c):
        return remote(
            XF.at[c % 4], YC.at[c, pl.ds(2 * ROWS, ROWS), :], m_s.at[0], y_r.at[c % 4], opp_inner
        )

    def x_opp(c):
        return remote(
            XF.at[c % 4], YC.at[c, pl.ds(ROWS, ROWS), :], m_s.at[0], y_r.at[c % 4], opp_inner
        )

    def p_inner(c):
        return remote(PS1.at[c], PR.at[c], m_s.at[1], p_r.at[c % 4], opp_inner)

    def p_outer(c):
        return remote(PS2.at[c], PR.at[c], m_s.at[1], p_r.at[c % 4], opp_outer)

    def q_outer(c):
        return remote(PSQ.at[c], PQ.at[c], m_s.at[0], m_r.at[c], own_outer)

    def make_x(c, far):
        @pl.when(lower)
        def _():
            norm(c, XC, ROWS, far)

        @pl.when(upper)
        def _():
            mix_grad(c, XC, ROWS, far)

    @pl.when(inner)
    def _():
        def send(q):
            c = phys(q)
            make_x(c, True)
            x_opp(c).start()

        loop(0, 4, send, "make_x")

    @pl.when(outer)
    def _():
        def send(q):
            c = phys(q + 4)
            make_x(c, False)
            x_near(c, own_inner).start()
            c = phys(q)
            make_x(c, True)
            x_far(c).start()

        loop(0, 4, send, "make_x")
        loop(0, 4, lambda q: x_near(phys(q), own_inner).start())

    def w_rows(t, g, h):
        c0, c1 = COLUMNS[t][g]
        return WBUF.at[t[1], g, pl.ds(h * 64, 64), c0:c1]

    def w_send(key, g, o):
        c0, c1 = COLUMNS[key][g]
        to = partner if o == 0 else (z, y, (x + o) % 4, core)
        land = w_r2.at[g] if o == 0 else w_r.at[key[1], g]
        return remote(WT.at[g, :, c0:c1], w_rows(key, g, core), w_s.at[0], land, to)

    for key in COLUMNS:

        @pl.when((j == key[0]) & (x == key[1]))
        def _(key=key):
            for g in ORDER[key[0]]:
                if g in COLUMNS[key]:
                    for o in (2, 1, 3, 0):
                        w_send(key, g, o).start()

    WBUF[x, :, pl.ds(pl.multiple_of(core * 64, 64), 64), :] = WT[...]

    @pl.when(inner)
    def _():
        loop(4, 8, lambda q: make_x(phys(q), False), "make_x")

    @pl.when(lower)
    def _():
        fetched_pair()
        loop(0, CHUNKS, lambda c: mix_grad(c, YC, 0), "mix_grad")

    @pl.when(upper)
    def _():
        loop(0, 4, stats, "stats")
        loop(0, CHUNKS, lambda c: norm(c, YC, 0), "norm")

    VS[...] = jnp.zeros_like(VS)
    GX[...] = jnp.zeros_like(GX)
    ACC[...] = jnp.zeros_like(ACC)
    ones = jnp.ones((8, CW), BF16)
    for g in range(GROUPS):
        rows = jnp.broadcast_to(bias[pl.ds(g, 1), pl.ds(pl.multiple_of(j * 128, 128), 128)], (128, 128))
        BIASC[g] = rows.T

    def sum_bias(source, row0):
        for g in range(GROUPS):
            s = dot_t(ones, source[2 * g, pl.ds(row0, ROWS), :]) + dot_t(ones, source[2 * g + 1, pl.ds(row0, ROWS), :])
            VS[6 + g // 2, pl.ds((g % 2) * 4 + j, 1), :] = s[0:1]

    @pl.when(lower)
    def _():
        sum_bias(YC, 0)

    @pl.when(upper)
    def _():
        sum_bias(XC, ROWS)

    seg_t = lax.broadcasted_iota(jnp.int32, (128, 128), 0) // 64
    seg_s = lax.broadcasted_iota(jnp.int32, (128, 128), 1) // 64
    allowed = seg_t >= seg_s

    def tile(t, s, g):
        w = WBUF[t, g, :, s * 128 : (s + 1) * 128]
        return jnp.where(allowed, w, jnp.zeros_like(w)) if t == s else w

    def place(g, dst, src, a, b):
        WX[g, dst * 128 : (dst + 1) * 128, src * 128 : (src + 1) * 128] = a
        WXT[g, src * 128 : (src + 1) * 128, dst * 128 : (dst + 1) * 128] = b

    def w_relay(key, g):
        rows = w_rows(key, g, core)
        return remote(rows, rows, f_s.at[key[1]], w_r2.at[g], partner)

    def w_ready(jj, g):
        keys = [key for key in COLUMNS if key[0] == jj and g in COLUMNS[key]]
        with jax.named_scope("w_wait"):
            for key in keys:

                @pl.when(x != key[1])
                def _(key=key):
                    rows = w_rows(key, g, core)
                    remote(rows, rows, w_s.at[0], w_r.at[key[1], g], partner).wait_recv()
                    w_relay(key, g).start()

            c0, c1 = COLUMNS[keys[0]][g]
            rows = WBUF.at[0 : len(keys), g, 0:64, c0:c1]
            remote(rows, rows, w_s.at[0], w_r2.at[g], partner).wait_recv()
        if jj == 0:
            w = tile(0, 0, g)
            place(g, 0, 0, w, w.T)
        elif jj == 3:
            w = tile(3, 3, g)
            place(g, 0, 0, w.T, w)
        elif jj == 1:
            for t in (1, 2, 3) if g >= 2 else (1,):
                for s in (0, 1):
                    w = tile(t, s, g)
                    place(g, t - 1, s, w, w.T)
        else:
            for s in (0, 1, 2) if g < 2 else (2,):
                for t in (2, 3):
                    w = tile(t, s, g)
                    place(g, 2 - s, 3 - t, w.T, w)

    def bias_of(g, on):
        b = jnp.where(on, BIASC[g], 0.0)
        return jnp.concatenate([b] * (CW // 128), axis=1)

    def row_sums(c, back):
        a = back * gain[:, columns(c)]
        b = a * UN[c]
        ACC[0] += a[:, 0:128] + a[:, 128:256] + a[:, 256:384]
        ACC[1] += b[:, 0:128] + b[:, 128:256] + b[:, 256:384]

    def column_sums(c, product, back):
        gt = jnp.sum(product, axis=0, keepdims=True)
        st = jnp.sum(back, axis=0, keepdims=True)
        for i in range(3):
            row = c * 3 + i
            VS[row // 8, pl.ds(row % 8, 1), :] += gt[:, i * 128 : (i + 1) * 128]
            VS[row // 8 + 3, pl.ds(row % 8, 1), :] += st[:, i * 128 : (i + 1) * 128]

    def put_x(c, g, value):
        value = (value + bias_of(g, lower)).astype(BF16)
        RES[kx, c] = value

        @pl.when(upper)
        def _():
            back = value.astype(F32)
            row_sums(c, back)
            column_sums(c, back * UN[c], back)

    def put_y(c, g, value, columns_too):
        value = (value + bias_of(g, upper)).astype(BF16)
        RES[ky, c] = value

        @pl.when(lower)
        def _():
            back = value.astype(F32)
            row_sums(c, back)
            if columns_too:
                column_sums(c, back * UN[c], back)

    def stage(part):
        for key, tiles in TILES.items():
            jj, t = key
            lo, hi = ((0, FIRST[key]), (FIRST[key], len(tiles)))[part]
            if lo == hi:
                continue

            @pl.when(j == jj)
            def _(jj=jj, t=t, tiles=tiles, lo=lo, hi=hi):
                for index in range(lo, hi):
                    s, g = tiles[index]
                    if jj == 0:
                        value = GX[g, 0:128, 0:128]
                    elif jj == 3:
                        value = GX[g, 0:128, 0:128].T
                    elif jj == 1:
                        value = GX[g, (t - 1) * 128 : t * 128, s * 128 : (s + 1) * 128]
                    else:
                        value = GX[g, (2 - s) * 128 : (3 - s) * 128, (3 - t) * 128 : (4 - t) * 128].T
                    value = value.astype(BF16)
                    GS[t, 0, index] = value[0:64]
                    GS[t, 1, index] = value[64:128]
                for h in range(2):
                    e = 2 * t + h

                    @pl.when(d != e)
                    def _():
                        remote(
                            GS.at[t, h, lo:hi], GR.at[d, lo:hi], r1_s.at[part, t], r1_r.at[part], (z, y, t, h)
                        ).start()

                    @pl.when(d == e)
                    def _():
                        GR[e, lo:hi] = GS[t, h, lo:hi]

    def sum_dp(key, tiles):
        n = len(tiles)
        lo = FIRST[key]

        with jax.named_scope("r1_wait"):
            for part, (a, b) in enumerate(((0, lo), (lo, n))):
                if a < b:
                    there = GR.at[0:7, a:b]
                    remote(there, there, r1_s.at[0, 0], r1_r.at[part], partner).wait_recv()

        def add(i):
            total = GR[0, i].astype(F32)
            for e in range(1, 8):
                total = total + GR[e, i].astype(F32)
            total = total.astype(BF16)
            for rs in range(4):
                GZ[rs, i] = total[rs * 16 : (rs + 1) * 16]

        loop(0, n, add, "dp_add")
        m = n // 2

        def send(o):
            e, peer = z_peer(o)
            remote(GZ.at[e % 4, pl.ds((e // 4) * m, m)], ZR.at[z, 0:m], r2_s.at[0], r2_r.at[0], peer).start()

        loop(1, 8, send, "r2_send")
        ZR[z, 0:m] = GZ[z % 4, pl.ds((z // 4) * m, m)]

    def sum_z(key, tiles):
        jj = key[0]
        m = len(tiles) // 2

        with jax.named_scope("r2_wait"):
            there = ZR.at[0:7, 0:m]
            remote(there, there, r2_s.at[0], r2_r.at[0], partner).wait_recv()
        total = ZR[0, 0:m].astype(F32)
        for e in range(1, 8):
            total = total + ZR[e, 0:m].astype(F32)
        YS[0:m] = total.astype(BF16)

        def send(o):
            e, peer = y_peer(o)
            remote(YS.at[0:m], YR.at[y, 0:m], r3_s.at[0], r3_r.at[jj], peer).start()

        loop(1, 8, send, "r3_send")
        YR[y, 0:m] = YS[0:m]

    @pl.when(inner)
    def _():
        def early(c):
            s = dot(WXT[c // 2, :, 0:ROWS], YC[c, 0:ROWS, :])
            PSQ[c] = s[0:ROWS].astype(BF16)
            YP[c] = s[ROWS:]
            q_outer(c).start()

            @pl.when(lower)
            def _():
                column_sums(c, s[ROWS:] * UN[c], s[ROWS:])

        def second(c):
            g = c // 2
            with jax.named_scope("wait_x"):
                x_near(c, own_outer).wait_recv()
            r = dot(WX[g], XC[c])
            PS1[c] = r[ROWS : 2 * ROWS].astype(BF16)
            PS2[c] = r[2 * ROWS :].astype(BF16)
            put_x(c, g, r[0:ROWS])
            p_outer(c).start()
            p_inner(c).start()
            with jax.named_scope("wait_y"):
                both_y = YC.at[c, pl.ds(ROWS, 2 * ROWS), :]
                remote(both_y, both_y, m_s.at[0], y_r.at[c % 4], opp_inner).wait_recv()

            @pl.when(upper)
            def _():
                u = YC[c, pl.ds(ROWS, 2 * ROWS), :].astype(F32)
                near, far = PS1[c].astype(F32), PS2[c].astype(F32)
                column_sums(c, near * u[0:ROWS] + far * u[ROWS:], near + far)
                YC[c, pl.ds(ROWS, 2 * ROWS), :] = (u * gain[:, columns(c)] + shift[:, columns(c)]).astype(BF16)

            s = dot(WXT[g], YC[c])
            PSQ[c] = s[0:ROWS].astype(BF16)
            q_outer(c).start()
            put_y(c, g, s[ROWS:], True)
            GX[g] += dot_t(YC[c], XC[c])

        for i in range(4):
            for jj in (1, 2):

                @pl.when(j == jj)
                def _(jj=jj, i=i):
                    w_ready(jj, ORDER[jj][i])

            if i < 2:
                loop(2 * i, 2 * i + 2, lambda q: early(phys(q)), "early")
            else:
                loop(2 * i, 2 * i + 2, lambda q: second(phys(q)), "second")

    @pl.when(inner)
    def _():
        stage(0)

        def first(q):
            c = phys(q)
            g = c // 2
            x_near(c, own_outer).wait_recv()
            put_x(c, g, dot(WX[g, 0:ROWS, :], XC[c]))
            GX[g, 0:ROWS, :] += dot_t(YC[c, 0:ROWS, :], XC[c])

        loop(0, 4, first, "first")

    @pl.when(outer)
    def _():
        for jj in (0, 3):

            @pl.when(j == jj)
            def _(jj=jj):
                for g in ORDER[jj]:
                    w_ready(jj, g)

        def local(c):
            g = c // 2
            own_x = XC[c, pl.ds(ROWS, ROWS), :]
            own_y = YC[c, pl.ds(0, ROWS), :]
            put_x(c, g, dot(WX[g, 0:ROWS, 0:ROWS], own_x))
            YP[c] = dot(WXT[g, 0:ROWS, 0:ROWS], own_y)
            GX[g, 0:ROWS, 0:ROWS] += dot_t(own_y, own_x)

        loop(0, 8, local, "local")
        stage(0)

    def late(q):
        c = phys(q)
        p_inner(c).wait_recv()
        put_y(c, c // 2, YP[c] + PR[c].astype(F32), False)

    def near_part(q):
        c = phys(q)
        q_outer(c).wait_recv()
        part = YP[c] + PQ[c].astype(F32)
        YP[c] = part

        @pl.when(lower)
        def _():
            column_sums(c, part * UN[c], part)

    def near_whole(q):
        c = phys(q)
        q_outer(c).wait_recv()
        put_y(c, c // 2, YP[c] + PQ[c].astype(F32), True)

    def owned(places, body):
        for key, tiles in TILES.items():
            if key[0] in places:

                @pl.when((j == key[0]) & (x == key[1]))
                def _(key=key, tiles=tiles):
                    body(key, tiles)

    @pl.when(outer)
    def _():
        loop(0, 4, near_part, "near_part")
        owned((0, 3), sum_dp)
        loop(4, 6, near_whole, "near_whole")
        owned((0, 3), sum_z)
        loop(6, 8, near_whole, "near_whole")

    def vec_send(source, land, me, k, peer):
        for o in range(1, 8):
            e, to = peer(o)
            remote(source(e), land.at[me], v_s.at[k], v_r.at[k], to).start()

    def vec_wait(land, k):
        with jax.named_scope("v_wait"):
            remote(land.at[0:7], land.at[0:7], v_s.at[k], v_r.at[k], partner).wait()

    def vec_sum(land):
        total = land[0]
        for e in range(1, 8):
            total = total + land[e]
        return total

    vec_send(lambda e: VS.at[e], VA, d, 0, dp_peer)
    VA[d] = VS[d]

    @pl.when(inner)
    def _():
        stage(1)

    late(0)
    vec_wait(VA, 0)
    VT[...] = vec_sum(VA)
    vec_send(lambda e: VT, VB, z, 1, z_peer)
    VB[z] = VT[...]
    late(1)

    @pl.when(inner)
    def _():
        owned((1, 2), sum_dp)

    late(2)
    vec_wait(VB, 1)
    VU[...] = vec_sum(VB)
    vec_send(lambda e: VU, VC, y, 2, y_peer)
    VC[y] = VU[...]
    late(3)

    @pl.when(inner)
    def _():
        owned((1, 2), sum_z)

    mean_a = jnp.sum(ACC[0], axis=1, keepdims=True) * (1.0 / WIDTH)
    mean_b = jnp.sum(ACC[1], axis=1, keepdims=True) * (1.0 / WIDTH)
    ACC[0] = jnp.broadcast_to(mean_a, (ROWS, 128))
    ACC[1] = jnp.broadcast_to(mean_b, (ROWS, 128))

    def outputs(c):
        cols = columns(c)
        scaled = RES[1, c].astype(F32) * gain[:, cols]
        out_v[0, :, cols] = (wide(INV[...]) * (scaled - wide(ACC[0]) - UN[c] * wide(ACC[1]))).astype(BF16)
        out_u[0, :, cols] = (upstream[:, cols].astype(F32) * RES[0, c].astype(F32)).astype(BF16)

    loop(0, CHUNKS, outputs, "outputs")

    vec_wait(VC, 2)
    VW[...] = vec_sum(VC)
    vec_send(lambda e: VW, VD, d, 3, dp_peer)
    VD[d] = VW[...]

    for t in range(4):
        places = [(jj, tiles) for (jj, tt), tiles in TILES.items() if tt == t]
        total_tiles = sum(len(tiles) // 2 for _, tiles in places)

        @pl.when(x == t)
        def _(t=t, places=places, total_tiles=total_tiles):
            off = 0
            for jj, tiles in places:
                m = len(tiles) // 2
                for count in (1, 2):

                    @pl.when((j == jj) if count == 1 else (j != jj))
                    @jax.named_scope("r3_wait")
                    def _():
                        there = YR.at[0:count, 0:m]
                        remote(there, there, r3_s.at[0], r3_r.at[jj], partner).wait_recv()

                for i in range(m):
                    ZS[off + i] = (YR[jj, i].astype(F32) + YR[jj + 4, i].astype(F32)).astype(BF16)
                off += m

            def send(o):
                e, peer = z_peer(o)
                remote(ZS.at[0:total_tiles], ZG.at[z, 0:total_tiles], r4_s.at[0], r4_r.at[0], peer).start()

            loop(1, 8, send, "r4_send")
            ZG[z, 0:total_tiles] = ZS[0:total_tiles]

    for key in COLUMNS:

        total = sum(c1 - c0 for c0, c1 in COLUMNS[key].values())
        groups = 2 if total % 512 == 0 and key != (1, 1) and key[0] != 0 and key[0] != 3 else 4
        cols = total // groups

        @pl.when((j == key[0]) & (x == key[1]))
        def _(groups=groups, cols=cols):
            rows = WBUF.at[0:4, 0:groups, 0:64, 0:cols]
            remote(rows, rows, w_s.at[0], w_r2.at[0], partner).wait_send()

        @pl.when((j == key[0]) & (x != key[1]))
        def _(key=key, groups=groups, cols=cols):
            rows = WBUF.at[0, 0:groups, 0:64, 0:cols]
            remote(rows, rows, f_s.at[key[1]], w_r2.at[0], partner).wait_send()

    def chunks_left(source, sem):
        remote(source, source, m_s.at[sem], m_r.at[0], own_inner).wait_send()

    @pl.when(inner)
    def _():
        chunks_left(YC.at[0:4], 0)
        chunks_left(PS1, 1)

    @pl.when(outer)
    def _():
        chunks_left(PS1.at[0:4], 0)
        chunks_left(PS1, 1)

    for key, tiles in TILES.items():
        jj, t = key
        for part, (lo, hi) in enumerate(((0, FIRST[key]), (FIRST[key], len(tiles)))):
            for count in (1, 2):
                if lo < hi:

                    @pl.when((j == jj) & ((x == t) if count == 1 else (x != t)))
                    def _(t=t, count=count, lo=lo, hi=hi, part=part):
                        there = GS.at[0, 0:count, lo:hi]
                        remote(there, there, r1_s.at[part, t], r1_r.at[part], partner).wait_send()

    def sent(key, tiles):
        m = len(tiles) // 2

        there = ZR.at[0:7, 0:m]
        remote(there, there, r2_s.at[0], r2_r.at[0], partner).wait_send()
        remote(there, there, r3_s.at[0], r3_r.at[0], partner).wait_send()

    owned((0, 1, 2, 3), sent)

    out_mix[...] = jnp.zeros_like(out_mix)
    keep = lax.broadcasted_iota(jnp.int32, (16, 128), 1) // 64 <= core
    for t in range(4):
        places = [(jj, tiles) for (jj, tt), tiles in TILES.items() if tt == t]
        total_tiles = sum(len(tiles) // 2 for _, tiles in places)

        @pl.when(x == t)
        def _(t=t, places=places, total_tiles=total_tiles):
            with jax.named_scope("r4_wait"):
                there = ZG.at[0:7, 0:total_tiles]
                remote(there, there, r4_s.at[0], r4_r.at[0], partner).wait()
            for k in range(8):
                rows = slice(16 * (k % 4), 16 * (k % 4) + 16)
                off = 0
                for jj, tiles in places:
                    m = len(tiles) // 2
                    for i in range(m):
                        s, g = tiles[(k // 4) * m + i]
                        value = ZG[k, off + i].astype(F32)
                        if s == t:
                            value = jnp.where(keep, value, 0.0)
                        out_mix[rows, g, s * 128 : (s + 1) * 128] = value
                    off += m

    vec_wait(VD, 3)
    out_vec[...] = VD[0:6]
    for g in range(GROUPS):
        for k in range(4):
            out_bias[g : g + 1, k * 128 : (k + 1) * 128] = VD[6 + g // 2, (g % 2) * 4 + k : (g % 2) * 4 + k + 1]


def writer(u, v, mix, vec, bias, out_u, out_v, out_mix, out_bias, out_gain, out_shift, sems):
    copies = [
        pltpu.make_async_copy(source, dest, sems.at[i])
        for i, (source, dest) in enumerate(
            (
                (u, out_u),
                (v, out_v),
                (mix, out_mix),
                (bias, out_bias),
                (vec.at[0:3], out_gain),
                (vec.at[3:6], out_shift),
            )
        )
    ]
    for copy in copies:
        copy.start()
    for copy in copies:
        copy.wait()


def per_device(gated, values_in, upstream, gain, shift, mix_w, mix_bias):
    vmem = pl.BlockSpec(memory_space=pltpu.VMEM)
    hbm = pl.BlockSpec(memory_space=pltpu.HBM)
    chunks = (CHUNKS, ROWS, CW)
    dma = pltpu.SemaphoreType.DMA
    results = pl.pallas_call(
        kernel,
        out_shape=(
            jax.ShapeDtypeStruct((1, ROWS, WIDTH), BF16),
            jax.ShapeDtypeStruct((1, ROWS, WIDTH), BF16),
            jax.ShapeDtypeStruct((64, GROUPS, 512), F32),
            jax.ShapeDtypeStruct((6, 8, 128), F32),
            jax.ShapeDtypeStruct((GROUPS, 512), F32),
        ),
        in_specs=[hbm] * 3 + [vmem] * 4,
        out_specs=[vmem] * 5,
        scratch_shapes=[
            pltpu.VMEM((ROWS, WIDTH), BF16),
            pltpu.VMEM((ROWS, WIDTH), BF16),
            pltpu.VMEM((ROWS, WIDTH), BF16),
            pltpu.VMEM((CHUNKS, 2 * ROWS, CW), BF16),
            pltpu.VMEM((CHUNKS // 2, ROWS, CW), BF16),
            pltpu.VMEM((CHUNKS, 3 * ROWS, CW), BF16),
            pltpu.VMEM(chunks, F32),
            pltpu.VMEM((ROWS, 128), F32),
            pltpu.VMEM((ROWS, 128), F32),
            pltpu.VMEM((2, *chunks), BF16),
            pltpu.VMEM(chunks, F32),
            pltpu.VMEM(chunks, BF16),
            pltpu.VMEM(chunks, BF16),
            pltpu.VMEM(chunks, BF16),
            pltpu.VMEM(chunks, BF16),
            pltpu.VMEM(chunks, BF16),
            pltpu.VMEM((2, ROWS, 128), F32),
            pltpu.VMEM((4, GROUPS, 128, 512), BF16),
            pltpu.VMEM((GROUPS, 384, 256), BF16),
            pltpu.VMEM((GROUPS, 256, 384), BF16),
            pltpu.VMEM((GROUPS, 128, 128), F32),
            pltpu.VMEM((GROUPS, 384, 256), F32),
            pltpu.VMEM((4, 2, 8, 64, 128), BF16),
            pltpu.VMEM((8, 8, 64, 128), BF16),
            pltpu.VMEM((4, 8, 16, 128), BF16),
            pltpu.VMEM((8, 4, 16, 128), BF16),
            pltpu.VMEM((4, 16, 128), BF16),
            pltpu.VMEM((8, 4, 16, 128), BF16),
            pltpu.VMEM((8, 16, 128), BF16),
            pltpu.VMEM((8, 8, 16, 128), BF16),
            pltpu.VMEM((8, 8, 128), F32),
            pltpu.VMEM((8, 8, 128), F32),
            pltpu.VMEM((8, 128), F32),
            pltpu.VMEM((8, 8, 128), F32),
            pltpu.VMEM((8, 128), F32),
            pltpu.VMEM((8, 8, 128), F32),
            pltpu.VMEM((8, 128), F32),
            pltpu.VMEM((8, 8, 128), F32),
            dma((6,)), dma((1,)), dma((4,)), dma((4, 4)), dma((4,)), dma((2,)), dma((8,)), dma((4,)), dma((4,)),
            dma((2, 4)), dma((2,)), dma((1,)), dma((1,)), dma((1,)), dma((4,)), dma((1,)), dma((1,)),
            dma((4,)), dma((4,)),
        ],
        compiler_params=pltpu.CompilerParams(
            collective_id=0, has_side_effects=True, vmem_limit_bytes=67043328 - 13312 * 1024
        ),
        name="span",
    )(
        gated,
        values_in,
        upstream,
        gain.reshape(1, WIDTH),
        shift.reshape(1, WIDTH),
        mix_w.transpose(1, 0, 2),
        mix_bias,
    )
    out_u, out_v, out_mix, out_bias, out_gain, out_shift = pl.pallas_call(
        writer,
        out_shape=(
            jax.ShapeDtypeStruct((1, ROWS, WIDTH), BF16),
            jax.ShapeDtypeStruct((1, ROWS, WIDTH), BF16),
            jax.ShapeDtypeStruct((64, GROUPS, 512), F32),
            jax.ShapeDtypeStruct((GROUPS, 512), F32),
            jax.ShapeDtypeStruct((3, 8, 128), F32),
            jax.ShapeDtypeStruct((3, 8, 128), F32),
        ),
        in_specs=[vmem] * 5,
        out_specs=[hbm] * 6,
        scratch_shapes=[dma((6,))],
        compiler_params=pltpu.CompilerParams(vmem_limit_bytes=1024 * 1024),
        name="writer",
    )(*results)
    return (out_u, out_v, out_mix, out_bias, out_gain.reshape(WIDTH), out_shift.reshape(WIDTH))


def solution(mesh):
    torus = Mesh(mesh.devices.reshape(8, 8, 4, 2), AXES)
    return jax.shard_map(
        per_device,
        mesh=torus,
        in_specs=(
            P(DP, SP, None),
            P(DP, SP, None),
            P(DP, SP, None),
            P(),
            P(),
            P(DP, None, None),
            P(),
        ),
        out_specs=(P(DP, SP, None), P(DP, SP, None), P(DP, None, None), P(), P(), P()),
        check_vma=False,
    )
```

```python
import jax
import jax.numpy as jnp
from jax import lax
from jax.experimental import pallas as pl
from jax.experimental.pallas import tpu as pltpu
from jax.sharding import Mesh
from jax.sharding import PartitionSpec as P

AXES = ("z", "y", "x", "core")
DP = ("x", "core")
SP = ("z", "y")
MESH = pl.DeviceIdType.MESH
F32 = jnp.float32
BF16 = jnp.bfloat16
EPS = 1e-05

GROUPS = 4
ROWS = 128
WIDTH = 3072
CHUNKS = 8
CW = WIDTH // CHUNKS

TILES = {
    (0, 0): [(0, g) for g in range(4)],
    (1, 1): [(0, 0), (0, 1), (1, 0), (1, 1), (0, 2), (1, 2), (0, 3), (1, 3)],
    (1, 2): [(0, 2), (1, 2), (0, 3), (1, 3)],
    (1, 3): [(0, 2), (1, 2), (0, 3), (1, 3)],
    (2, 2): [(2, 2), (2, 3), (2, 0), (0, 0), (1, 0), (2, 1), (0, 1), (1, 1)],
    (2, 3): [(2, 2), (2, 3), (2, 0), (0, 0), (1, 0), (2, 1), (0, 1), (1, 1)],
    (3, 3): [(3, g) for g in range(4)],
}
ENDS = {
    (0, 0): (0, 4, 4, 4),
    (1, 1): (0, 4, 6, 8),
    (1, 2): (0, 0, 2, 4),
    (1, 3): (0, 0, 2, 4),
    (2, 2): (0, 2, 5, 8),
    (2, 3): (0, 2, 5, 8),
    (3, 3): (0, 4, 4, 4),
}
ORDER = {0: (0, 1, 2, 3), 1: (0, 1, 2, 3), 2: (2, 3, 0, 1), 3: (2, 3, 0, 1)}
COLUMNS = {
    (0, 0): {g: (0, 128) for g in range(4)},
    (1, 1): {g: (0, 256) for g in range(4)},
    (1, 2): {2: (0, 256), 3: (0, 256)},
    (1, 3): {2: (0, 256), 3: (0, 256)},
    (2, 2): {0: (0, 384), 1: (0, 384), 2: (256, 384), 3: (256, 384)},
    (2, 3): {0: (0, 384), 1: (0, 384), 2: (256, 384), 3: (256, 384)},
    (3, 3): {g: (384, 512) for g in range(4)},
}


def remote(src, dst, send, recv, device):
    return pltpu.make_async_remote_copy(
        src_ref=src, dst_ref=dst, send_sem=send, recv_sem=recv, device_id=device, device_id_type=MESH
    )


def dot(a, b):
    return jnp.dot(a, b, preferred_element_type=F32)


def dot_t(a, b):
    return lax.dot_general(a, b, (((1,), (1,)), ((), ())), preferred_element_type=F32)


def loop(lo, hi, body, name="loop"):
    with jax.named_scope(name):
        lax.fori_loop(lo, hi, lambda i, _: (body(i), None)[1], None)


def kernel(
    gated_hbm, values_hbm, upstream_hbm, gain, shift, WT, bias,
    out_u, out_v, out_mix, out_vec, out_bias,
    gated, values, upstream,
    XC, XF, XR, YC, UN, MEAN, INV, RES, YP, PS1, PS2, PSQ, PR, PQ, ACC,
    WBUF, WX, WXT, BIASC, GX, GS, GR, GZ, ZR, YS, YR, ZS, ZG,
    VS, VA, VT, VB, VU, VC, VW, VD,
    in_s, w_s, f_s, w_r, w_r2, m_s, m_r, y_r, p_r, r1_s, r1_r, r2_s, r2_r, r3_s, r3_r, r4_s, r4_r,
    v_s, v_r,
):
    z, y = lax.axis_index("z"), lax.axis_index("y")
    x, core = lax.axis_index("x"), lax.axis_index("core")
    d = x * 2 + core
    half = y // 4
    j = y % 4
    up = j // 2
    inner = (j == 1) | (j == 2)
    outer = jnp.logical_not(inner)
    lower = up == 0
    upper = up == 1
    base = half * 4
    own_outer = (z, base + 3 * up, x, core)
    own_inner = (z, base + 1 + up, x, core)
    opp_inner = (z, base + 2 - up, x, core)
    opp_outer = (z, base + 3 - 3 * up, x, core)
    partner = (z, y, x, 1 - core)
    kx, ky = up, 1 - up

    def dp_peer(o):
        e = (d + o) % 8
        return e, (z, y, e // 2, e % 2)

    def z_peer(o):
        e = (z + o) % 8
        return e, (e, y, x, core)

    def y_peer(o):
        e = (y + o) % 8
        return e, (z, e, x, core)

    def phys(q):
        return (q + 4 * up) % 8

    big = ((values_hbm, values), (upstream_hbm, upstream), (gated_hbm, gated))

    def fetch(k, part):
        rows = pl.ds(part * 32, 32)
        source, dest = big[k]
        return pltpu.make_async_copy(source.at[0, rows, :], dest.at[rows, :], in_s.at[part if k == 0 else 3 + k])

    barrier = pltpu.get_barrier_semaphore()

    def greet(o):
        for peer in (dp_peer, z_peer, y_peer):
            pl.semaphore_signal(barrier, inc=1, device_id=peer(o)[1], device_id_type=MESH)

    @pl.when(lower)
    def _():
        for part in range(4):
            fetch(0, part).start()

    @pl.when(upper)
    def _():
        for part in range(4):
            fetch(1, part).start()
            fetch(2, part).start()

    loop(1, 8, greet, "greet")

    @pl.when(lower)
    def _():
        for part in range(4):
            fetch(1, part).start()
            fetch(2, part).start()

    @pl.when(upper)
    def _():
        for part in range(4):
            fetch(0, part).start()

    def stats(i):
        r = pl.multiple_of(i * 32, 32)
        fetch(0, i).wait()
        v = values[pl.ds(r, 32), :].astype(F32)
        mean = jnp.sum(v, axis=1, keepdims=True) * (1.0 / WIDTH)
        d0 = v - mean
        inv = lax.rsqrt(jnp.sum(d0 * d0, axis=1, keepdims=True) * (1.0 / WIDTH) + EPS)
        MEAN[pl.ds(r, 32), :] = jnp.broadcast_to(mean, (32, 128))
        INV[pl.ds(r, 32), :] = jnp.broadcast_to(inv, (32, 128))

    def wide(v):
        return jnp.concatenate([v] * (CW // 128), axis=1)

    def columns(c):
        return pl.ds(pl.multiple_of(c * CW, 128), CW)

    def norm(c, dest, row0, far=False):
        cols = columns(c)
        u = (values[:, cols].astype(F32) - wide(MEAN[...])) * wide(INV[...])
        UN[c] = u
        if far:
            XF[c] = u.astype(BF16)
        dest[c, row0 : row0 + ROWS, :] = (u * gain[:, cols] + shift[:, cols]).astype(BF16)

    def mix_grad(c, dest, row0, far=False):
        cols = columns(c)
        m = (upstream[:, cols].astype(F32) * gated[:, cols].astype(F32)).astype(BF16)
        if far:
            XF[c] = m
        dest[c, row0 : row0 + ROWS, :] = m

    def fetched_pair():
        for k in (1, 2):
            source, dest = big[k]
            pltpu.make_async_copy(source.at[0], dest, in_s.at[3 + k]).wait()

    @pl.when(lower)
    def _():
        loop(0, 4, stats, "stats")

    @pl.when(upper)
    def _():
        fetched_pair()

    with jax.named_scope("barrier"):
        pl.semaphore_wait(barrier, 21)

    def x_near(c):
        return remote(XF.at[c], XR.at[c], m_s.at[1], m_r.at[c], own_inner)

    def x_opp(c):
        return remote(XF.at[c], YC.at[c, pl.ds(ROWS, ROWS), :], m_s.at[0], y_r.at[c % 4], opp_inner)

    def x_relay(c):
        return remote(XR.at[c], YC.at[c, pl.ds(2 * ROWS, ROWS), :], m_s.at[1], y_r.at[c % 4], opp_inner)

    def p_inner(c):
        return remote(PS1.at[c], PR.at[c], m_s.at[1], p_r.at[c % 4], opp_inner)

    def p_outer(c):
        return remote(PS2.at[c], PR.at[c], m_s.at[1], p_r.at[c % 4], opp_outer)

    def q_outer(c):
        return remote(PSQ.at[c], PQ.at[c], m_s.at[0], m_r.at[c], own_outer)

    def make_x(c):
        @pl.when(lower)
        def _():
            norm(c, XC, ROWS, True)

        @pl.when(upper)
        def _():
            mix_grad(c, XC, ROWS, True)

    @pl.when(inner)
    def _():
        def send(q):
            c = phys(q)
            make_x(c)
            x_opp(c).start()

        loop(0, 4, send, "make_x")

    @pl.when(outer)
    def _():
        def send(q):
            c = phys(q)
            make_x(c)
            x_near(c).start()

        loop(0, 8, send, "make_x")

    def w_rows(t, g, h):
        c0, c1 = COLUMNS[t][g]
        return WBUF.at[t[1], g, pl.ds(h * 64, 64), c0:c1]

    def w_send(key, g, o):
        c0, c1 = COLUMNS[key][g]
        to = partner if o == 0 else (z, y, (x + o) % 4, core)
        land = w_r2.at[g] if o == 0 else w_r.at[key[1], g]
        return remote(WT.at[g, :, c0:c1], w_rows(key, g, core), w_s.at[0], land, to)

    for key in COLUMNS:

        @pl.when((j == key[0]) & (x == key[1]))
        def _(key=key):
            for g in ORDER[key[0]]:
                if g in COLUMNS[key]:
                    for o in (2, 1, 3, 0):
                        w_send(key, g, o).start()

    WBUF[x, :, pl.ds(pl.multiple_of(core * 64, 64), 64), :] = WT[...]

    @pl.when(inner)
    def _():
        loop(4, 8, lambda q: make_x(phys(q)), "make_x")

    @pl.when(lower)
    def _():
        fetched_pair()
        loop(0, CHUNKS, lambda c: mix_grad(c, YC, 0), "mix_grad")

    @pl.when(upper)
    def _():
        loop(0, 4, stats, "stats")
        loop(0, CHUNKS, lambda c: norm(c, YC, 0), "norm")

    VS[...] = jnp.zeros_like(VS)
    GX[...] = jnp.zeros_like(GX)
    ACC[...] = jnp.zeros_like(ACC)
    ones = jnp.ones((8, CW), BF16)
    for g in range(GROUPS):
        rows = jnp.broadcast_to(bias[pl.ds(g, 1), pl.ds(pl.multiple_of(j * 128, 128), 128)], (128, 128))
        BIASC[g] = rows.T

    def sum_bias(source, row0):
        for g in range(GROUPS):
            s = dot_t(ones, source[2 * g, pl.ds(row0, ROWS), :]) + dot_t(ones, source[2 * g + 1, pl.ds(row0, ROWS), :])
            VS[6 + g // 2, pl.ds((g % 2) * 4 + j, 1), :] = s[0:1]

    @pl.when(lower)
    def _():
        sum_bias(YC, 0)

    @pl.when(upper)
    def _():
        sum_bias(XC, ROWS)

    seg_t = lax.broadcasted_iota(jnp.int32, (128, 128), 0) // 64
    seg_s = lax.broadcasted_iota(jnp.int32, (128, 128), 1) // 64
    allowed = seg_t >= seg_s

    def tile(t, s, g):
        w = WBUF[t, g, :, s * 128 : (s + 1) * 128]
        return jnp.where(allowed, w, jnp.zeros_like(w)) if t == s else w

    def place(g, dst, src, a, b):
        WX[g, dst * 128 : (dst + 1) * 128, src * 128 : (src + 1) * 128] = a
        WXT[g, src * 128 : (src + 1) * 128, dst * 128 : (dst + 1) * 128] = b

    def w_relay(key, g):
        rows = w_rows(key, g, core)
        return remote(rows, rows, f_s.at[key[1]], w_r2.at[g], partner)

    def w_ready(jj, g):
        keys = [key for key in COLUMNS if key[0] == jj and g in COLUMNS[key]]
        with jax.named_scope("w_wait"):
            for key in keys:

                @pl.when(x != key[1])
                def _(key=key):
                    rows = w_rows(key, g, core)
                    remote(rows, rows, w_s.at[0], w_r.at[key[1], g], partner).wait_recv()
                    w_relay(key, g).start()

            c0, c1 = COLUMNS[keys[0]][g]
            rows = WBUF.at[0 : len(keys), g, 0:64, c0:c1]
            remote(rows, rows, w_s.at[0], w_r2.at[g], partner).wait_recv()
        if jj == 0:
            w = tile(0, 0, g)
            place(g, 0, 0, w, w.T)
        elif jj == 3:
            w = tile(3, 3, g)
            place(g, 0, 0, w.T, w)
        elif jj == 1:
            for t in (1, 2, 3) if g >= 2 else (1,):
                for s in (0, 1):
                    w = tile(t, s, g)
                    place(g, t - 1, s, w, w.T)
        else:
            for s in (0, 1, 2) if g < 2 else (2,):
                for t in (2, 3):
                    w = tile(t, s, g)
                    place(g, 2 - s, 3 - t, w.T, w)

    def bias_of(g, on):
        b = jnp.where(on, BIASC[g], 0.0)
        return jnp.concatenate([b] * (CW // 128), axis=1)

    def row_sums(c, back):
        a = back * gain[:, columns(c)]
        b = a * UN[c]
        ACC[0] += a[:, 0:128] + a[:, 128:256] + a[:, 256:384]
        ACC[1] += b[:, 0:128] + b[:, 128:256] + b[:, 256:384]

    def column_sums(c, product, back):
        gt = jnp.sum(product, axis=0, keepdims=True)
        st = jnp.sum(back, axis=0, keepdims=True)
        for i in range(3):
            row = c * 3 + i
            VS[row // 8, pl.ds(row % 8, 1), :] += gt[:, i * 128 : (i + 1) * 128]
            VS[row // 8 + 3, pl.ds(row % 8, 1), :] += st[:, i * 128 : (i + 1) * 128]

    def put_x(c, g, value):
        value = (value + bias_of(g, lower)).astype(BF16)
        RES[kx, c] = value

        @pl.when(upper)
        def _():
            back = value.astype(F32)
            row_sums(c, back)
            column_sums(c, back * UN[c], back)

    def put_y(c, g, value, columns_too):
        value = (value + bias_of(g, upper)).astype(BF16)
        RES[ky, c] = value

        @pl.when(lower)
        def _():
            back = value.astype(F32)
            row_sums(c, back)
            if columns_too:
                column_sums(c, back * UN[c], back)

    def stage(part):
        for key, tiles in TILES.items():
            jj, t = key
            lo, hi = ENDS[key][part : part + 2]
            if lo == hi:
                continue

            @pl.when(j == jj)
            def _(jj=jj, t=t, tiles=tiles, lo=lo, hi=hi):
                for index in range(lo, hi):
                    s, g = tiles[index]
                    if jj == 0:
                        value = GX[g, 0:128, 0:128]
                    elif jj == 3:
                        value = GX[g, 0:128, 0:128].T
                    elif jj == 1:
                        value = GX[g, (t - 1) * 128 : t * 128, s * 128 : (s + 1) * 128]
                    else:
                        value = GX[g, (2 - s) * 128 : (3 - s) * 128, (3 - t) * 128 : (4 - t) * 128].T
                    value = value.astype(BF16)
                    GS[t, 0, index] = value[0:64]
                    GS[t, 1, index] = value[64:128]
                for h in range(2):
                    e = 2 * t + h

                    @pl.when(d != e)
                    def _():
                        remote(
                            GS.at[t, h, lo:hi], GR.at[d, lo:hi], r1_s.at[part, t], r1_r.at[part], (z, y, t, h)
                        ).start()

                    @pl.when(d == e)
                    def _():
                        GR[e, lo:hi] = GS[t, h, lo:hi]

    def sum_dp(key, tiles):
        n = len(tiles)
        with jax.named_scope("r1_wait"):
            for part in range(3):
                a, b = ENDS[key][part : part + 2]
                if a < b:
                    there = GR.at[0:7, a:b]
                    remote(there, there, r1_s.at[0, 0], r1_r.at[part], partner).wait_recv()

        def add(i):
            total = GR[0, i].astype(F32)
            for e in range(1, 8):
                total = total + GR[e, i].astype(F32)
            total = total.astype(BF16)
            for rs in range(4):
                GZ[rs, i] = total[rs * 16 : (rs + 1) * 16]

        loop(0, n, add, "dp_add")
        m = n // 2

        def send(o):
            e, peer = z_peer(o)
            remote(GZ.at[e % 4, pl.ds((e // 4) * m, m)], ZR.at[z, 0:m], r2_s.at[0], r2_r.at[0], peer).start()

        loop(1, 8, send, "r2_send")
        ZR[z, 0:m] = GZ[z % 4, pl.ds((z // 4) * m, m)]

    def sum_z(key, tiles):
        jj = key[0]
        m = len(tiles) // 2

        with jax.named_scope("r2_wait"):
            there = ZR.at[0:7, 0:m]
            remote(there, there, r2_s.at[0], r2_r.at[0], partner).wait_recv()
        total = ZR[0, 0:m].astype(F32)
        for e in range(1, 8):
            total = total + ZR[e, 0:m].astype(F32)
        YS[0:m] = total.astype(BF16)

        def send(o):
            e, peer = y_peer(o)
            remote(YS.at[0:m], YR.at[y, 0:m], r3_s.at[0], r3_r.at[jj], peer).start()

        loop(1, 8, send, "r3_send")
        YR[y, 0:m] = YS[0:m]

    @pl.when(inner)
    def _():
        def arrived(c):
            x_near(c).wait_recv()

        def take(c):
            @pl.when(lower)
            def _():
                n = XR[c].astype(F32) * gain[:, columns(c)] + shift[:, columns(c)]
                XC[c, pl.ds(0, ROWS), :] = n.astype(BF16)

            @pl.when(upper)
            def _():
                XC[c, pl.ds(0, ROWS), :] = XR[c]

        def outer_sums(c):
            back = PSQ[c].astype(F32)
            column_sums(c, back * XR[c].astype(F32), back)

        def first(c):
            g = c // 2
            s = dot(WXT[g, :, 0:ROWS], YC[c, 0:ROWS, :])
            PSQ[c] = s[0:ROWS].astype(BF16)
            YP[c] = s[ROWS:]
            q_outer(c).start()

            @pl.when(lower)
            def _():
                column_sums(c, s[ROWS:] * UN[c], s[ROWS:])

            with jax.named_scope("wait_x"):
                arrived(c)
            x_relay(c).start()
            take(c)
            put_x(c, g, dot(WX[g, 0:ROWS, :], XC[c]))
            GX[g, 0:ROWS, :] += dot_t(YC[c, 0:ROWS, :], XC[c])

            @pl.when(lower)
            def _():
                outer_sums(c)

        def second(c):
            g = c // 2
            with jax.named_scope("wait_x"):
                arrived(c)
            take(c)
            r = dot(WX[g], XC[c])
            PS1[c] = r[ROWS : 2 * ROWS].astype(BF16)
            PS2[c] = r[2 * ROWS :].astype(BF16)
            p_outer(c).start()
            p_inner(c).start()
            put_x(c, g, r[0:ROWS])
            with jax.named_scope("wait_y"):
                both_y = YC.at[c, pl.ds(ROWS, 2 * ROWS), :]
                remote(both_y, both_y, m_s.at[0], y_r.at[c % 4], opp_inner).wait_recv()

            @pl.when(upper)
            def _():
                u = YC[c, pl.ds(ROWS, 2 * ROWS), :].astype(F32)
                near, far = PS1[c].astype(F32), PS2[c].astype(F32)
                column_sums(c, near * u[0:ROWS] + far * u[ROWS:], near + far)
                YC[c, pl.ds(ROWS, 2 * ROWS), :] = (u * gain[:, columns(c)] + shift[:, columns(c)]).astype(BF16)

            s = dot(WXT[g], YC[c])
            PSQ[c] = s[0:ROWS].astype(BF16)
            put_y(c, g, s[ROWS:], True)
            q_outer(c).start()
            GX[g] += dot_t(YC[c], XC[c])

            @pl.when(lower)
            def _():
                outer_sums(c)

        for i in range(4):
            for jj in (1, 2):

                @pl.when(j == jj)
                def _(jj=jj, i=i):
                    w_ready(jj, ORDER[jj][i])

            if i < 2:
                loop(2 * i, 2 * i + 2, lambda q: first(phys(q)), "first")
            else:
                loop(2 * i, 2 * i + 2, lambda q: second(phys(q)), "second")
            if i > 0:
                with jax.named_scope("stage"):
                    stage(i - 1)

    @pl.when(outer)
    def _():
        for jj in (0, 3):

            @pl.when(j == jj)
            def _(jj=jj):
                for g in ORDER[jj]:
                    w_ready(jj, g)

        def local(c):
            g = c // 2
            own_x = XC[c, pl.ds(ROWS, ROWS), :]
            own_y = YC[c, pl.ds(0, ROWS), :]
            put_x(c, g, dot(WX[g, 0:ROWS, 0:ROWS], own_x))
            part = dot(WXT[g, 0:ROWS, 0:ROWS], own_y)
            YP[c] = part

            @pl.when(lower)
            def _():
                column_sums(c, part * UN[c], part)

            GX[g, 0:ROWS, 0:ROWS] += dot_t(own_y, own_x)

        loop(0, 8, local, "local")
        stage(0)

    def late(q):
        c = phys(q)
        p_inner(c).wait_recv()
        put_y(c, c // 2, YP[c] + PR[c].astype(F32), False)

    def near_part(q):
        c = phys(q)
        q_outer(c).wait_recv()
        YP[c] += PQ[c].astype(F32)

    def near_whole(q):
        c = phys(q)
        q_outer(c).wait_recv()
        put_y(c, c // 2, YP[c] + PQ[c].astype(F32), False)

    def owned(places, body):
        for key, tiles in TILES.items():
            if key[0] in places:

                @pl.when((j == key[0]) & (x == key[1]))
                def _(key=key, tiles=tiles):
                    body(key, tiles)

    def vec_send(source, land, me, k, peer):
        for o in range(1, 8):
            e, to = peer(o)
            remote(source(e), land.at[me], v_s.at[k], v_r.at[k], to).start()

    def vec_wait(land, k):
        with jax.named_scope("v_wait"):
            remote(land.at[0:7], land.at[0:7], v_s.at[k], v_r.at[k], partner).wait()

    def vec_sum(land):
        total = land[0]
        for e in range(1, 8):
            total = total + land[e]
        return total

    def vec_dp():
        vec_send(lambda e: VS.at[e], VA, d, 0, dp_peer)
        VA[d] = VS[d]

    def vec_z():
        vec_wait(VA, 0)
        VT[...] = vec_sum(VA)
        vec_send(lambda e: VT, VB, z, 1, z_peer)
        VB[z] = VT[...]

    def vec_y():
        vec_wait(VB, 1)
        VU[...] = vec_sum(VB)
        vec_send(lambda e: VU, VC, y, 2, y_peer)
        VC[y] = VU[...]

    @pl.when(inner)
    def _():
        vec_dp()
        late(0)
        vec_z()
        late(1)
        owned((1, 2), sum_dp)
        vec_y()
        late(2)
        owned((1, 2), sum_z)

    @pl.when(outer)
    def _():
        vec_dp()
        owned((0, 3), sum_dp)
        loop(0, 4, near_part, "near_part")
        owned((0, 3), sum_z)
        vec_z()
        loop(4, 6, near_whole, "near_whole")
        vec_y()
        loop(6, 8, near_whole, "near_whole")
        loop(0, 3, late, "late")

    vec_wait(VC, 2)
    VW[...] = vec_sum(VC)
    vec_send(lambda e: VW, VD, d, 3, dp_peer)
    VD[d] = VW[...]
    with jax.named_scope("late"):
        late(3)

    mean_a = jnp.sum(ACC[0], axis=1, keepdims=True) * (1.0 / WIDTH)
    mean_b = jnp.sum(ACC[1], axis=1, keepdims=True) * (1.0 / WIDTH)
    ACC[0] = jnp.broadcast_to(mean_a, (ROWS, 128))
    ACC[1] = jnp.broadcast_to(mean_b, (ROWS, 128))

    def outputs(c):
        cols = columns(c)
        scaled = RES[1, c].astype(F32) * gain[:, cols]
        out_v[0, :, cols] = (wide(INV[...]) * (scaled - wide(ACC[0]) - UN[c] * wide(ACC[1]))).astype(BF16)
        out_u[0, :, cols] = (upstream[:, cols].astype(F32) * RES[0, c].astype(F32)).astype(BF16)

    loop(0, CHUNKS, outputs, "outputs")

    for t in range(4):
        places = [(jj, tiles) for (jj, tt), tiles in TILES.items() if tt == t]
        total_tiles = sum(len(tiles) // 2 for _, tiles in places)

        @pl.when(x == t)
        def _(t=t, places=places, total_tiles=total_tiles):
            off = 0
            for jj, tiles in places:
                m = len(tiles) // 2
                for count in (1, 2):

                    @pl.when((j == jj) if count == 1 else (j != jj))
                    @jax.named_scope("r3_wait")
                    def _():
                        there = YR.at[0:count, 0:m]
                        remote(there, there, r3_s.at[0], r3_r.at[jj], partner).wait_recv()

                for i in range(m):
                    ZS[off + i] = (YR[jj, i].astype(F32) + YR[jj + 4, i].astype(F32)).astype(BF16)
                off += m

            def send(o):
                e, peer = z_peer(o)
                remote(ZS.at[0:total_tiles], ZG.at[z, 0:total_tiles], r4_s.at[0], r4_r.at[0], peer).start()

            loop(1, 8, send, "r4_send")
            ZG[z, 0:total_tiles] = ZS[0:total_tiles]

    for key in COLUMNS:

        total = sum(c1 - c0 for c0, c1 in COLUMNS[key].values())
        groups = 2 if total % 512 == 0 and key != (1, 1) and key[0] != 0 and key[0] != 3 else 4
        cols = total // groups

        @pl.when((j == key[0]) & (x == key[1]))
        def _(groups=groups, cols=cols):
            rows = WBUF.at[0:4, 0:groups, 0:64, 0:cols]
            remote(rows, rows, w_s.at[0], w_r2.at[0], partner).wait_send()

        @pl.when((j == key[0]) & (x != key[1]))
        def _(key=key, groups=groups, cols=cols):
            rows = WBUF.at[0, 0:groups, 0:64, 0:cols]
            remote(rows, rows, f_s.at[key[1]], w_r2.at[0], partner).wait_send()

    def chunks_left(source, sem):
        remote(source, source, m_s.at[sem], m_r.at[0], own_inner).wait_send()

    @pl.when(inner)
    def _():
        chunks_left(YC.at[0:4], 0)
        chunks_left(YC.at[0:4], 1)

    @pl.when(outer)
    def _():
        chunks_left(PS1, 1)

    for key, tiles in TILES.items():
        jj, t = key
        for part in range(3):
            lo, hi = ENDS[key][part : part + 2]
            for count in (1, 2):
                if lo < hi:

                    @pl.when((j == jj) & ((x == t) if count == 1 else (x != t)))
                    def _(t=t, count=count, lo=lo, hi=hi, part=part):
                        there = GS.at[0, 0:count, lo:hi]
                        remote(there, there, r1_s.at[part, t], r1_r.at[part], partner).wait_send()

    def sent(key, tiles):
        m = len(tiles) // 2

        there = ZR.at[0:7, 0:m]
        remote(there, there, r2_s.at[0], r2_r.at[0], partner).wait_send()
        remote(there, there, r3_s.at[0], r3_r.at[0], partner).wait_send()

    owned((0, 1, 2, 3), sent)

    out_mix[...] = jnp.zeros_like(out_mix)
    keep = lax.broadcasted_iota(jnp.int32, (16, 128), 1) // 64 <= core
    for t in range(4):
        places = [(jj, tiles) for (jj, tt), tiles in TILES.items() if tt == t]
        total_tiles = sum(len(tiles) // 2 for _, tiles in places)

        @pl.when(x == t)
        def _(t=t, places=places, total_tiles=total_tiles):
            with jax.named_scope("r4_wait"):
                there = ZG.at[0:7, 0:total_tiles]
                remote(there, there, r4_s.at[0], r4_r.at[0], partner).wait()
            for k in range(8):
                rows = slice(16 * (k % 4), 16 * (k % 4) + 16)
                off = 0
                for jj, tiles in places:
                    m = len(tiles) // 2
                    for i in range(m):
                        s, g = tiles[(k // 4) * m + i]
                        value = ZG[k, off + i].astype(F32)
                        if s == t:
                            value = jnp.where(keep, value, 0.0)
                        out_mix[rows, g, s * 128 : (s + 1) * 128] = value
                    off += m

    vec_wait(VD, 3)
    out_vec[...] = VD[0:6]
    for g in range(GROUPS):
        for k in range(4):
            out_bias[g : g + 1, k * 128 : (k + 1) * 128] = VD[6 + g // 2, (g % 2) * 4 + k : (g % 2) * 4 + k + 1]


def writer(u, v, mix, vec, bias, out_u, out_v, out_mix, out_bias, out_gain, out_shift, sems):
    copies = [
        pltpu.make_async_copy(source, dest, sems.at[i])
        for i, (source, dest) in enumerate(
            (
                (u, out_u),
                (v, out_v),
                (mix, out_mix),
                (bias, out_bias),
                (vec.at[0:3], out_gain),
                (vec.at[3:6], out_shift),
            )
        )
    ]
    for copy in copies:
        copy.start()
    for copy in copies:
        copy.wait()


def per_device(gated, values_in, upstream, gain, shift, mix_w, mix_bias):
    vmem = pl.BlockSpec(memory_space=pltpu.VMEM)
    hbm = pl.BlockSpec(memory_space=pltpu.HBM)
    chunks = (CHUNKS, ROWS, CW)
    dma = pltpu.SemaphoreType.DMA
    results = pl.pallas_call(
        kernel,
        out_shape=(
            jax.ShapeDtypeStruct((1, ROWS, WIDTH), BF16),
            jax.ShapeDtypeStruct((1, ROWS, WIDTH), BF16),
            jax.ShapeDtypeStruct((64, GROUPS, 512), F32),
            jax.ShapeDtypeStruct((6, 8, 128), F32),
            jax.ShapeDtypeStruct((GROUPS, 512), F32),
        ),
        in_specs=[hbm] * 3 + [vmem] * 4,
        out_specs=[vmem] * 5,
        scratch_shapes=[
            pltpu.VMEM((ROWS, WIDTH), BF16),
            pltpu.VMEM((ROWS, WIDTH), BF16),
            pltpu.VMEM((ROWS, WIDTH), BF16),
            pltpu.VMEM((CHUNKS, 2 * ROWS, CW), BF16),
            pltpu.VMEM(chunks, BF16),
            pltpu.VMEM(chunks, BF16),
            pltpu.VMEM((CHUNKS, 3 * ROWS, CW), BF16),
            pltpu.VMEM(chunks, F32),
            pltpu.VMEM((ROWS, 128), F32),
            pltpu.VMEM((ROWS, 128), F32),
            pltpu.VMEM((2, *chunks), BF16),
            pltpu.VMEM(chunks, F32),
            pltpu.VMEM(chunks, BF16),
            pltpu.VMEM(chunks, BF16),
            pltpu.VMEM(chunks, BF16),
            pltpu.VMEM(chunks, BF16),
            pltpu.VMEM(chunks, BF16),
            pltpu.VMEM((2, ROWS, 128), F32),
            pltpu.VMEM((4, GROUPS, 128, 512), BF16),
            pltpu.VMEM((GROUPS, 384, 256), BF16),
            pltpu.VMEM((GROUPS, 256, 384), BF16),
            pltpu.VMEM((GROUPS, 128, 128), F32),
            pltpu.VMEM((GROUPS, 384, 256), F32),
            pltpu.VMEM((4, 2, 8, 64, 128), BF16),
            pltpu.VMEM((8, 8, 64, 128), BF16),
            pltpu.VMEM((4, 8, 16, 128), BF16),
            pltpu.VMEM((8, 4, 16, 128), BF16),
            pltpu.VMEM((4, 16, 128), BF16),
            pltpu.VMEM((8, 4, 16, 128), BF16),
            pltpu.VMEM((8, 16, 128), BF16),
            pltpu.VMEM((8, 8, 16, 128), BF16),
            pltpu.VMEM((8, 8, 128), F32),
            pltpu.VMEM((8, 8, 128), F32),
            pltpu.VMEM((8, 128), F32),
            pltpu.VMEM((8, 8, 128), F32),
            pltpu.VMEM((8, 128), F32),
            pltpu.VMEM((8, 8, 128), F32),
            pltpu.VMEM((8, 128), F32),
            pltpu.VMEM((8, 8, 128), F32),
            dma((6,)), dma((1,)), dma((4,)), dma((4, 4)), dma((4,)), dma((2,)), dma((8,)), dma((4,)), dma((4,)),
            dma((3, 4)), dma((3,)), dma((1,)), dma((1,)), dma((1,)), dma((4,)), dma((1,)), dma((1,)),
            dma((4,)), dma((4,)),
        ],
        compiler_params=pltpu.CompilerParams(
            collective_id=0, has_side_effects=True, vmem_limit_bytes=67043328 - 13312 * 1024
        ),
        name="span",
    )(
        gated,
        values_in,
        upstream,
        gain.reshape(1, WIDTH),
        shift.reshape(1, WIDTH),
        mix_w.transpose(1, 0, 2),
        mix_bias,
    )
    out_u, out_v, out_mix, out_bias, out_gain, out_shift = pl.pallas_call(
        writer,
        out_shape=(
            jax.ShapeDtypeStruct((1, ROWS, WIDTH), BF16),
            jax.ShapeDtypeStruct((1, ROWS, WIDTH), BF16),
            jax.ShapeDtypeStruct((64, GROUPS, 512), F32),
            jax.ShapeDtypeStruct((GROUPS, 512), F32),
            jax.ShapeDtypeStruct((3, 8, 128), F32),
            jax.ShapeDtypeStruct((3, 8, 128), F32),
        ),
        in_specs=[vmem] * 5,
        out_specs=[hbm] * 6,
        scratch_shapes=[dma((6,))],
        compiler_params=pltpu.CompilerParams(vmem_limit_bytes=1024 * 1024),
        name="writer",
    )(*results)
    return (out_u, out_v, out_mix, out_bias, out_gain.reshape(WIDTH), out_shift.reshape(WIDTH))


def solution(mesh):
    torus = Mesh(mesh.devices.reshape(8, 8, 4, 2), AXES)
    return jax.shard_map(
        per_device,
        mesh=torus,
        in_specs=(
            P(DP, SP, None),
            P(DP, SP, None),
            P(DP, SP, None),
            P(),
            P(),
            P(DP, None, None),
            P(),
        ),
        out_specs=(P(DP, SP, None), P(DP, SP, None), P(DP, None, None), P(), P(), P()),
        check_vma=False,
    )
```

```python
import jax
import jax.numpy as jnp
from jax import lax
from jax.experimental import pallas as pl
from jax.experimental.pallas import tpu as pltpu
from jax.sharding import Mesh
from jax.sharding import PartitionSpec as P

AXES = ("z", "y", "x", "core")
DP = ("x", "core")
SP = ("z", "y")
MESH = pl.DeviceIdType.MESH
F32 = jnp.float32
BF16 = jnp.bfloat16
EPS = 1e-05

GROUPS = 4
ROWS = 128
WIDTH = 3072
CHUNKS = 8
CW = WIDTH // CHUNKS

TILES = {
    (0, 0): [(0, g) for g in range(4)],
    (1, 1): [(0, 0), (0, 1), (1, 0), (1, 1), (0, 2), (1, 2), (0, 3), (1, 3)],
    (1, 2): [(0, 2), (1, 2), (0, 3), (1, 3)],
    (1, 3): [(0, 2), (1, 2), (0, 3), (1, 3)],
    (2, 2): [(2, 2), (2, 3), (2, 0), (0, 0), (1, 0), (2, 1), (0, 1), (1, 1)],
    (2, 3): [(2, 2), (2, 3), (2, 0), (0, 0), (1, 0), (2, 1), (0, 1), (1, 1)],
    (3, 3): [(3, g) for g in range(4)],
}
ENDS = {
    (0, 0): (0, 4, 4, 4),
    (1, 1): (0, 4, 6, 8),
    (1, 2): (0, 0, 2, 4),
    (1, 3): (0, 0, 2, 4),
    (2, 2): (0, 2, 4, 8),
    (2, 3): (0, 2, 4, 8),
    (3, 3): (0, 4, 4, 4),
}


def chain(key, k):
    ends = ENDS[key]
    return ((ends[0], ends[2]), (ends[2], ends[3]))[k]


def places_of(t, k):
    off = sum(ENDS[key][2] // 2 for key in TILES if key[1] == t) if k else 0
    out = []
    for key in TILES:
        a, b = chain(key, k)
        if key[1] == t and a < b:
            out.append((key, (b - a) // 2, off))
            off += (b - a) // 2
    return out


ORDER = {0: (0, 1, 2, 3), 1: (0, 1, 2, 3), 2: (2, 3, 0, 1), 3: (2, 3, 0, 1)}
COLUMNS = {
    (0, 0): {g: (0, 128) for g in range(4)},
    (1, 1): {g: (0, 256) for g in range(4)},
    (1, 2): {2: (0, 256), 3: (0, 256)},
    (1, 3): {2: (0, 256), 3: (0, 256)},
    (2, 2): {0: (0, 384), 1: (0, 384), 2: (256, 384), 3: (256, 384)},
    (2, 3): {0: (0, 384), 1: (0, 384), 2: (256, 384), 3: (256, 384)},
    (3, 3): {g: (384, 512) for g in range(4)},
}


def remote(src, dst, send, recv, device):
    return pltpu.make_async_remote_copy(
        src_ref=src, dst_ref=dst, send_sem=send, recv_sem=recv, device_id=device, device_id_type=MESH
    )


def dot(a, b):
    return jnp.dot(a, b, preferred_element_type=F32)


def dot_t(a, b):
    return lax.dot_general(a, b, (((1,), (1,)), ((), ())), preferred_element_type=F32)


def loop(lo, hi, body, name="loop"):
    with jax.named_scope(name):
        lax.fori_loop(lo, hi, lambda i, _: (body(i), None)[1], None)


def kernel(
    gated_hbm, values_hbm, upstream_hbm, gain, shift, WT, bias,
    out_u, out_v, out_mix, out_vec, out_bias,
    gated, values, upstream,
    XC, XF, XR, UR, YC, UN, MEAN, INV, RES, YP, PS1, PS2, PSQ, PR, PQ, ACC,
    WBUF, WX, WXT, BIASC, GX, GS, GR, GZ, ZR, YS, YR, ZS, ZG,
    VS, VA, VT, VB, VU, VC, VW, VD,
    in_s, w_s, f_s, w_r, w_r2, m_s, m_r, y_r, p_r, r1_s, r1_r, r2_s, r2_r, r3_s, r3_r, r4_s, r4_r,
    v_s, v_r,
):
    z, y = lax.axis_index("z"), lax.axis_index("y")
    x, core = lax.axis_index("x"), lax.axis_index("core")
    d = x * 2 + core
    half = y // 4
    j = y % 4
    up = j // 2
    inner = (j == 1) | (j == 2)
    outer = jnp.logical_not(inner)
    lower = up == 0
    upper = up == 1
    base = half * 4
    own_outer = (z, base + 3 * up, x, core)
    own_inner = (z, base + 1 + up, x, core)
    opp_inner = (z, base + 2 - up, x, core)
    opp_outer = (z, base + 3 - 3 * up, x, core)
    partner = (z, y, x, 1 - core)
    kx, ky = up, 1 - up

    def dp_peer(o):
        e = (d + o) % 8
        return e, (z, y, e // 2, e % 2)

    def z_peer(o):
        e = (z + o) % 8
        return e, (e, y, x, core)

    def y_peer(o):
        e = (y + o) % 8
        return e, (z, e, x, core)

    def phys(q):
        return (q + 4 * up) % 8

    big = ((values_hbm, values), (upstream_hbm, upstream), (gated_hbm, gated))

    def fetch(k, part):
        rows = pl.ds(part * 32, 32)
        source, dest = big[k]
        return pltpu.make_async_copy(source.at[0, rows, :], dest.at[rows, :], in_s.at[part if k == 0 else 3 + k])

    barrier = pltpu.get_barrier_semaphore()

    def greet(o):
        for peer in (dp_peer, z_peer, y_peer):
            pl.semaphore_signal(barrier, inc=1, device_id=peer(o)[1], device_id_type=MESH)

    @pl.when(lower)
    def _():
        for part in range(4):
            fetch(0, part).start()

    @pl.when(upper)
    def _():
        for part in range(4):
            fetch(1, part).start()
            fetch(2, part).start()

    loop(1, 8, greet, "greet")

    @pl.when(lower)
    def _():
        for part in range(4):
            fetch(1, part).start()
            fetch(2, part).start()

    @pl.when(upper)
    def _():
        for part in range(4):
            fetch(0, part).start()

    def stats(i):
        r = pl.multiple_of(i * 32, 32)
        fetch(0, i).wait()
        v = values[pl.ds(r, 32), :].astype(F32)
        mean = jnp.sum(v, axis=1, keepdims=True) * (1.0 / WIDTH)
        d0 = v - mean
        inv = lax.rsqrt(jnp.sum(d0 * d0, axis=1, keepdims=True) * (1.0 / WIDTH) + EPS)
        MEAN[pl.ds(r, 32), :] = jnp.broadcast_to(mean, (32, 128))
        INV[pl.ds(r, 32), :] = jnp.broadcast_to(inv, (32, 128))

    def wide(v):
        return jnp.concatenate([v] * (CW // 128), axis=1)

    def columns(c):
        return pl.ds(pl.multiple_of(c * CW, 128), CW)

    def norm(c, dest, row0, far=False):
        cols = columns(c)
        u = (values[:, cols].astype(F32) - wide(MEAN[...])) * wide(INV[...])
        UN[c] = u
        if far:
            XF[c] = u.astype(BF16)
        dest[c, row0 : row0 + ROWS, :] = (u * gain[:, cols] + shift[:, cols]).astype(BF16)

    def mix_grad(c, dest, row0, far=False):
        cols = columns(c)
        m = (upstream[:, cols].astype(F32) * gated[:, cols].astype(F32)).astype(BF16)
        if far:
            XF[c] = m
        dest[c, row0 : row0 + ROWS, :] = m

    def fetched_pair():
        for k in (1, 2):
            source, dest = big[k]
            pltpu.make_async_copy(source.at[0], dest, in_s.at[3 + k]).wait()

    @pl.when(lower)
    def _():
        loop(0, 4, stats, "stats")

    @pl.when(upper)
    def _():
        fetched_pair()

    with jax.named_scope("barrier"):
        pl.semaphore_wait(barrier, 21)

    def x_near(c):
        return remote(XF.at[c], XR.at[c], m_s.at[1], m_r.at[c], own_inner)

    def x_opp(c):
        return remote(XF.at[c], YC.at[c, pl.ds(ROWS, ROWS), :], m_s.at[0], y_r.at[c % 4], opp_inner)

    def x_relay(c):
        return remote(XR.at[c], YC.at[c, pl.ds(2 * ROWS, ROWS), :], m_s.at[1], y_r.at[c % 4], opp_inner)

    def p_inner(c):
        return remote(PS1.at[c], PR.at[c], m_s.at[1], p_r.at[c % 4], opp_inner)

    def p_outer(c):
        return remote(PS2.at[c], PR.at[c], m_s.at[1], p_r.at[c % 4], opp_outer)

    def q_outer(c):
        return remote(PSQ.at[c], PQ.at[c], m_s.at[0], m_r.at[c], own_outer)

    def make_x(c):
        @pl.when(lower)
        def _():
            norm(c, XC, ROWS, True)

        @pl.when(upper)
        def _():
            mix_grad(c, XC, ROWS, True)

    @pl.when(inner)
    def _():
        def send(q):
            c = phys(q)
            make_x(c)
            x_opp(c).start()

        loop(0, 4, send, "make_x")

    @pl.when(outer)
    def _():
        def send(q):
            c = phys(q)
            make_x(c)
            x_near(c).start()

        loop(0, 8, send, "make_x")

    def w_rows(t, g, h):
        c0, c1 = COLUMNS[t][g]
        return WBUF.at[t[1], g, pl.ds(h * 64, 64), c0:c1]

    def w_send(key, g, o):
        c0, c1 = COLUMNS[key][g]
        to = partner if o == 0 else (z, y, (x + o) % 4, core)
        land = w_r2.at[g] if o == 0 else w_r.at[key[1], g]
        return remote(WT.at[g, :, c0:c1], w_rows(key, g, core), w_s.at[0], land, to)

    for key in COLUMNS:

        @pl.when((j == key[0]) & (x == key[1]))
        def _(key=key):
            for g in ORDER[key[0]]:
                if g in COLUMNS[key]:
                    for o in (2, 1, 3, 0):
                        w_send(key, g, o).start()

    WBUF[x, :, pl.ds(pl.multiple_of(core * 64, 64), 64), :] = WT[...]

    @pl.when(inner)
    def _():
        loop(4, 8, lambda q: make_x(phys(q)), "make_x")

    @pl.when(lower)
    def _():
        fetched_pair()
        loop(0, CHUNKS, lambda c: mix_grad(c, YC, 0), "mix_grad")

    @pl.when(upper)
    def _():
        loop(0, 4, stats, "stats")
        loop(0, CHUNKS, lambda c: norm(c, YC, 0), "norm")

    VS[...] = jnp.zeros_like(VS)
    out_mix[...] = jnp.zeros_like(out_mix)
    GX[...] = jnp.zeros_like(GX)
    ACC[...] = jnp.zeros_like(ACC)
    ones = jnp.ones((8, CW), BF16)
    for g in range(GROUPS):
        rows = jnp.broadcast_to(bias[pl.ds(g, 1), pl.ds(pl.multiple_of(j * 128, 128), 128)], (128, 128))
        BIASC[g] = rows.T

    def sum_bias(source, row0):
        for g in range(GROUPS):
            s = dot_t(ones, source[2 * g, pl.ds(row0, ROWS), :]) + dot_t(ones, source[2 * g + 1, pl.ds(row0, ROWS), :])
            VS[6 + g // 2, pl.ds((g % 2) * 4 + j, 1), :] = s[0:1]

    @pl.when(lower)
    def _():
        sum_bias(YC, 0)

    @pl.when(upper)
    def _():
        sum_bias(XC, ROWS)

    seg_t = lax.broadcasted_iota(jnp.int32, (128, 128), 0) // 64
    seg_s = lax.broadcasted_iota(jnp.int32, (128, 128), 1) // 64
    allowed = seg_t >= seg_s

    def tile(t, s, g):
        w = WBUF[t, g, :, s * 128 : (s + 1) * 128]
        return jnp.where(allowed, w, jnp.zeros_like(w)) if t == s else w

    def place(g, dst, src, a, b):
        WX[g, dst * 128 : (dst + 1) * 128, src * 128 : (src + 1) * 128] = a
        WXT[g, src * 128 : (src + 1) * 128, dst * 128 : (dst + 1) * 128] = b

    def w_relay(key, g):
        rows = w_rows(key, g, core)
        return remote(rows, rows, f_s.at[key[1]], w_r2.at[g], partner)

    def w_ready(jj, g):
        keys = [key for key in COLUMNS if key[0] == jj and g in COLUMNS[key]]
        with jax.named_scope("w_wait"):
            for key in keys:

                @pl.when(x != key[1])
                def _(key=key):
                    rows = w_rows(key, g, core)
                    remote(rows, rows, w_s.at[0], w_r.at[key[1], g], partner).wait_recv()
                    w_relay(key, g).start()

            c0, c1 = COLUMNS[keys[0]][g]
            rows = WBUF.at[0 : len(keys), g, 0:64, c0:c1]
            remote(rows, rows, w_s.at[0], w_r2.at[g], partner).wait_recv()
        if jj == 0:
            w = tile(0, 0, g)
            place(g, 0, 0, w, w.T)
        elif jj == 3:
            w = tile(3, 3, g)
            place(g, 0, 0, w.T, w)
        elif jj == 1:
            for t in (1, 2, 3) if g >= 2 else (1,):
                for s in (0, 1):
                    w = tile(t, s, g)
                    place(g, t - 1, s, w, w.T)
        else:
            for s in (0, 1, 2) if g < 2 else (2,):
                for t in (2, 3):
                    w = tile(t, s, g)
                    place(g, 2 - s, 3 - t, w.T, w)

    def bias_of(g, on):
        b = jnp.where(on, BIASC[g], 0.0)
        return jnp.concatenate([b] * (CW // 128), axis=1)

    def row_sums(c, back):
        a = back * gain[:, columns(c)]
        b = a * UN[c]
        ACC[0] += a[:, 0:128] + a[:, 128:256] + a[:, 256:384]
        ACC[1] += b[:, 0:128] + b[:, 128:256] + b[:, 256:384]

    def column_sums(c, product, back):
        gt = jnp.sum(product, axis=0, keepdims=True)
        st = jnp.sum(back, axis=0, keepdims=True)
        for i in range(3):
            row = c * 3 + i
            VS[row // 8, pl.ds(row % 8, 1), :] += gt[:, i * 128 : (i + 1) * 128]
            VS[row // 8 + 3, pl.ds(row % 8, 1), :] += st[:, i * 128 : (i + 1) * 128]

    def put_x(c, g, value):
        value = (value + bias_of(g, lower)).astype(BF16)
        RES[kx, c] = value

        @pl.when(upper)
        def _():
            back = value.astype(F32)
            row_sums(c, back)
            column_sums(c, back * UN[c], back)

    def put_y(c, g, value, columns_too):
        value = (value + bias_of(g, upper)).astype(BF16)
        RES[ky, c] = value

        @pl.when(lower)
        def _():
            back = value.astype(F32)
            row_sums(c, back)
            if columns_too:
                column_sums(c, back * UN[c], back)

    def stage(part):
        for key, tiles in TILES.items():
            jj, t = key
            lo, hi = ENDS[key][part : part + 2]
            if lo == hi:
                continue

            @pl.when(j == jj)
            def _(jj=jj, t=t, tiles=tiles, lo=lo, hi=hi):
                for index in range(lo, hi):
                    s, g = tiles[index]
                    if jj == 0:
                        value = GX[g, 0:128, 0:128]
                    elif jj == 3:
                        value = GX[g, 0:128, 0:128].T
                    elif jj == 1:
                        value = GX[g, (t - 1) * 128 : t * 128, s * 128 : (s + 1) * 128]
                    else:
                        value = GX[g, (2 - s) * 128 : (3 - s) * 128, (3 - t) * 128 : (4 - t) * 128].T
                    value = value.astype(BF16)
                    GS[t, 0, index] = value[0:64]
                    GS[t, 1, index] = value[64:128]
                for h in range(2):
                    e = 2 * t + h

                    @pl.when(d != e)
                    def _():
                        remote(
                            GS.at[t, h, lo:hi], GR.at[d, lo:hi], r1_s.at[part, t], r1_r.at[part], (z, y, t, h)
                        ).start()

                    @pl.when(d == e)
                    def _():
                        GR[e, lo:hi] = GS[t, h, lo:hi]

    def sum_dp(k):
        def body(key):
            a, b = chain(key, k)
            with jax.named_scope("r1_wait"):
                for part in (0, 1) if k == 0 else (2,):
                    lo, hi = ENDS[key][part : part + 2]
                    if lo < hi:
                        there = GR.at[0:7, lo:hi]
                        remote(there, there, r1_s.at[0, 0], r1_r.at[part], partner).wait_recv()

            def add(i):
                total = GR[0, i].astype(F32)
                for e in range(1, 8):
                    total = total + GR[e, i].astype(F32)
                total = total.astype(BF16)
                for rs in range(4):
                    GZ[rs, i] = total[rs * 16 : (rs + 1) * 16]

            loop(a, b, add, "dp_add")
            m = (b - a) // 2
            at = a // 2

            def piece(e):
                return pl.ds(a + (e // 4) * m, m)

            def send(o):
                e, peer = z_peer(o)
                remote(GZ.at[e % 4, piece(e)], ZR.at[z, at : at + m], r2_s.at[k], r2_r.at[k], peer).start()

            loop(1, 8, send, "r2_send")
            ZR[z, at : at + m] = GZ[z % 4, piece(z)]

        return body

    def sum_z(k):
        def body(key):
            a, b = chain(key, k)
            m = (b - a) // 2
            here = slice(a // 2, a // 2 + m)
            with jax.named_scope("r2_wait"):
                there = ZR.at[0:7, here]
                remote(there, there, r2_s.at[k], r2_r.at[k], partner).wait_recv()
            total = ZR[0, here].astype(F32)
            for e in range(1, 8):
                total = total + ZR[e, here].astype(F32)
            YS[here] = total.astype(BF16)

            def send(o):
                e, peer = y_peer(o)
                remote(YS.at[here], YR.at[y, here], r3_s.at[k], r3_r.at[k, key[0]], peer).start()

            loop(1, 8, send, "r3_send")
            YR[y, here] = YS[here]

        return body

    def join(k):
        for t in range(4):
            places = places_of(t, k)
            if not places:
                continue

            @pl.when(x == t)
            def _(places=places):
                for key, m, off in places:
                    jj = key[0]
                    at = chain(key, k)[0] // 2
                    for count in (1, 2):

                        @pl.when((j == jj) if count == 1 else (j != jj))
                        @jax.named_scope("r3_wait")
                        def _():
                            there = YR.at[0:count, at : at + m]
                            remote(there, there, r3_s.at[k], r3_r.at[k, jj], partner).wait_recv()

                    for i in range(m):
                        ZS[off + i] = (YR[jj, at + i].astype(F32) + YR[jj + 4, at + i].astype(F32)).astype(BF16)
                here = slice(places[0][2], places[-1][2] + places[-1][1])

                def send(o):
                    e, peer = z_peer(o)
                    remote(ZS.at[here], ZG.at[z, here], r4_s.at[k], r4_r.at[k], peer).start()

                loop(1, 8, send, "r4_send")
                ZG[z, here] = ZS[here]

    def put_mix(k):
        keep = lax.broadcasted_iota(jnp.int32, (16, 128), 1) // 64 <= core
        for t in range(4):
            places = places_of(t, k)
            if not places:
                continue

            @pl.when(x == t)
            def _(t=t, places=places):
                there = ZG.at[0:7, places[0][2] : places[-1][2] + places[-1][1]]
                with jax.named_scope("r4_wait"):
                    remote(there, there, r4_s.at[k], r4_r.at[k], partner).wait()
                for part in range(8):
                    rows = slice(16 * (part % 4), 16 * (part % 4) + 16)
                    for key, m, off in places:
                        for i in range(m):
                            s, g = TILES[key][chain(key, k)[0] + (part // 4) * m + i]
                            value = ZG[part, off + i].astype(F32)
                            if s == t:
                                value = jnp.where(keep, value, 0.0)
                            out_mix[rows, g, s * 128 : (s + 1) * 128] = value

    def vec_send(source, land, me, k, peer):
        for o in range(1, 8):
            e, to = peer(o)
            remote(source(e), land.at[me], v_s.at[k], v_r.at[k], to).start()

    def vec_wait(land, k):
        with jax.named_scope("v_wait"):
            remote(land.at[0:7], land.at[0:7], v_s.at[k], v_r.at[k], partner).wait()

    def vec_sum(land):
        total = land[0]
        for e in range(1, 8):
            total = total + land[e]
        return total

    def vec_dp():
        vec_send(lambda e: VS.at[e], VA, d, 0, dp_peer)
        VA[d] = VS[d]

    @pl.when(inner)
    def _():
        def arrived(c):
            x_near(c).wait_recv()

        def take(c):
            @pl.when(lower)
            def _():
                n = XR[c].astype(F32) * gain[:, columns(c)] + shift[:, columns(c)]
                XC[c, pl.ds(0, ROWS), :] = n.astype(BF16)

            @pl.when(upper)
            def _():
                XC[c, pl.ds(0, ROWS), :] = XR[c]

        def outer_sums(c):
            back = PSQ[c].astype(F32)
            column_sums(c, back * XR[c].astype(F32), back)

        def first(c):
            g = c // 2
            s = dot(WXT[g, :, 0:ROWS], YC[c, 0:ROWS, :])
            PSQ[c] = s[0:ROWS].astype(BF16)
            YP[c] = s[ROWS:]
            q_outer(c).start()

            @pl.when(lower)
            def _():
                column_sums(c, s[ROWS:] * UN[c], s[ROWS:])

            with jax.named_scope("wait_x"):
                arrived(c)
            x_relay(c).start()
            take(c)
            put_x(c, g, dot(WX[g, 0:ROWS, :], XC[c]))
            GX[g, 0:ROWS, :] += dot_t(YC[c, 0:ROWS, :], XC[c])

            @pl.when(lower)
            def _():
                outer_sums(c)

        def meet(c):
            g = c // 2
            with jax.named_scope("wait_x"):
                arrived(c)
            take(c)
            with jax.named_scope("wait_y"):
                both_y = YC.at[c, pl.ds(ROWS, 2 * ROWS), :]
                remote(both_y, both_y, m_s.at[0], y_r.at[c % 4], opp_inner).wait_recv()

            @pl.when(upper)
            def _():
                raw = YC[c, pl.ds(ROWS, 2 * ROWS), :]
                UR[c % 4] = raw
                n = raw.astype(F32) * gain[:, columns(c)] + shift[:, columns(c)]
                YC[c, pl.ds(ROWS, 2 * ROWS), :] = n.astype(BF16)

            GX[g] += dot_t(YC[c], XC[c])

        def multiply(c, now):
            g = c // 2
            r = dot(WX[g], XC[c])
            PS1[c] = r[ROWS : 2 * ROWS].astype(BF16)
            PS2[c] = r[2 * ROWS :].astype(BF16)
            if now:
                p_outer(c).start()
                p_inner(c).start()
            put_x(c, g, r[0:ROWS])
            s = dot(WXT[g], YC[c])
            PSQ[c] = s[0:ROWS].astype(BF16)
            put_y(c, g, s[ROWS:], True)
            q_outer(c).start()

            @pl.when(lower)
            def _():
                outer_sums(c)

            @pl.when(upper)
            def _():
                u = UR[c % 4].astype(F32)
                near, far = PS1[c].astype(F32), PS2[c].astype(F32)
                column_sums(c, near * u[0:ROWS] + far * u[ROWS:], near + far)

        def second(c):
            meet(c)
            multiply(c, True)

        for i in range(4):
            for jj in (1, 2):

                @pl.when(j == jj)
                def _(jj=jj, i=i):
                    w_ready(jj, ORDER[jj][i])

            if i < 2:
                loop(2 * i, 2 * i + 2, lambda q: first(phys(q)), "first")
            elif i == 2:
                loop(2 * i, 2 * i + 2, lambda q: second(phys(q)), "second")
            else:
                loop(2 * i, 2 * i + 2, lambda q: meet(phys(q)), "meet")
            if i > 0:
                with jax.named_scope("stage"):
                    stage(i - 1)
        with jax.named_scope("multiply"):
            multiply(phys(6), True)
            multiply(phys(7), False)
        vec_dp()

    @pl.when(outer)
    def _():
        for jj in (0, 3):

            @pl.when(j == jj)
            def _(jj=jj):
                for g in ORDER[jj]:
                    w_ready(jj, g)

        def local(c):
            g = c // 2
            own_x = XC[c, pl.ds(ROWS, ROWS), :]
            own_y = YC[c, pl.ds(0, ROWS), :]
            put_x(c, g, dot(WX[g, 0:ROWS, 0:ROWS], own_x))
            part = dot(WXT[g, 0:ROWS, 0:ROWS], own_y)
            YP[c] = part

            @pl.when(lower)
            def _():
                column_sums(c, part * UN[c], part)

            GX[g, 0:ROWS, 0:ROWS] += dot_t(own_y, own_x)

        loop(0, 8, local, "local")
        stage(0)

    def late(q):
        c = phys(q)
        p_inner(c).wait_recv()
        put_y(c, c // 2, YP[c] + PR[c].astype(F32), False)

    def near_part(q):
        c = phys(q)
        q_outer(c).wait_recv()
        YP[c] += PQ[c].astype(F32)

    def near_whole(q):
        c = phys(q)
        q_outer(c).wait_recv()
        put_y(c, c // 2, YP[c] + PQ[c].astype(F32), False)

    def owned(places, body):
        for key in TILES:
            if key[0] in places:

                @pl.when((j == key[0]) & (x == key[1]))
                def _(key=key):
                    body(key)

    def vec_z():
        vec_wait(VA, 0)
        VT[...] = vec_sum(VA)
        vec_send(lambda e: VT, VB, z, 1, z_peer)
        VB[z] = VT[...]

    def vec_y():
        vec_wait(VB, 1)
        VU[...] = vec_sum(VB)
        vec_send(lambda e: VU, VC, y, 2, y_peer)
        VC[y] = VU[...]

    @pl.when(inner)
    def _():
        owned((1, 2), sum_dp(0))
        vec_z()
        owned((1, 2), sum_dp(1))
        loop(0, 2, late, "late")
        owned((1, 2), sum_z(0))
        p_outer(phys(7)).start()
        p_inner(phys(7)).start()
        vec_y()
        owned((1, 2), sum_z(1))

    @pl.when(outer)
    def _():
        vec_dp()
        owned((0, 3), sum_dp(0))
        loop(0, 4, near_part, "near_part")
        owned((0, 3), sum_z(0))
        vec_z()
        loop(4, 6, near_whole, "near_whole")
        vec_y()
        loop(6, 8, near_whole, "near_whole")
        loop(0, 2, late, "late")

    join(0)
    with jax.named_scope("late"):
        late(2)
    with jax.named_scope("late"):
        late(3)
    vec_wait(VC, 2)
    VW[...] = vec_sum(VC)
    vec_send(lambda e: VW, VD, d, 3, dp_peer)
    VD[d] = VW[...]
    join(1)

    mean_a = jnp.sum(ACC[0], axis=1, keepdims=True) * (1.0 / WIDTH)
    mean_b = jnp.sum(ACC[1], axis=1, keepdims=True) * (1.0 / WIDTH)
    ACC[0] = jnp.broadcast_to(mean_a, (ROWS, 128))
    ACC[1] = jnp.broadcast_to(mean_b, (ROWS, 128))

    def outputs(c):
        cols = columns(c)
        scaled = RES[1, c].astype(F32) * gain[:, cols]
        out_v[0, :, cols] = (wide(INV[...]) * (scaled - wide(ACC[0]) - UN[c] * wide(ACC[1]))).astype(BF16)
        out_u[0, :, cols] = (upstream[:, cols].astype(F32) * RES[0, c].astype(F32)).astype(BF16)

    loop(0, CHUNKS, outputs, "outputs")

    for key in COLUMNS:

        total = sum(c1 - c0 for c0, c1 in COLUMNS[key].values())
        groups = 2 if total % 512 == 0 and key != (1, 1) and key[0] != 0 and key[0] != 3 else 4
        cols = total // groups

        @pl.when((j == key[0]) & (x == key[1]))
        def _(groups=groups, cols=cols):
            rows = WBUF.at[0:4, 0:groups, 0:64, 0:cols]
            remote(rows, rows, w_s.at[0], w_r2.at[0], partner).wait_send()

        @pl.when((j == key[0]) & (x != key[1]))
        def _(key=key, groups=groups, cols=cols):
            rows = WBUF.at[0, 0:groups, 0:64, 0:cols]
            remote(rows, rows, f_s.at[key[1]], w_r2.at[0], partner).wait_send()

    def chunks_left(source, sem):
        remote(source, source, m_s.at[sem], m_r.at[0], own_inner).wait_send()

    @pl.when(inner)
    def _():
        chunks_left(YC.at[0:4], 0)
        chunks_left(YC.at[0:4], 1)

    @pl.when(outer)
    def _():
        chunks_left(PS1, 1)

    for key, tiles in TILES.items():
        jj, t = key
        for part in range(3):
            lo, hi = ENDS[key][part : part + 2]
            for count in (1, 2):
                if lo < hi:

                    @pl.when((j == jj) & ((x == t) if count == 1 else (x != t)))
                    def _(t=t, count=count, lo=lo, hi=hi, part=part):
                        there = GS.at[0, 0:count, lo:hi]
                        remote(there, there, r1_s.at[part, t], r1_r.at[part], partner).wait_send()

    def sent(key):
        for k in range(2):
            a, b = chain(key, k)
            if a < b:
                there = ZR.at[0:7, 0 : (b - a) // 2]
                remote(there, there, r2_s.at[k], r2_r.at[k], partner).wait_send()
                remote(there, there, r3_s.at[k], r3_r.at[k, 0], partner).wait_send()

    owned((0, 1, 2, 3), sent)
    put_mix(0)
    put_mix(1)
    vec_wait(VD, 3)
    out_vec[...] = VD[0:6]
    for g in range(GROUPS):
        for k in range(4):
            out_bias[g : g + 1, k * 128 : (k + 1) * 128] = VD[6 + g // 2, (g % 2) * 4 + k : (g % 2) * 4 + k + 1]


def writer(u, v, mix, vec, bias, out_u, out_v, out_mix, out_bias, out_gain, out_shift, sems):
    copies = [
        pltpu.make_async_copy(source, dest, sems.at[i])
        for i, (source, dest) in enumerate(
            (
                (u, out_u),
                (v, out_v),
                (mix, out_mix),
                (bias, out_bias),
                (vec.at[0:3], out_gain),
                (vec.at[3:6], out_shift),
            )
        )
    ]
    for copy in copies:
        copy.start()
    for copy in copies:
        copy.wait()


def per_device(gated, values_in, upstream, gain, shift, mix_w, mix_bias):
    vmem = pl.BlockSpec(memory_space=pltpu.VMEM)
    hbm = pl.BlockSpec(memory_space=pltpu.HBM)
    chunks = (CHUNKS, ROWS, CW)
    dma = pltpu.SemaphoreType.DMA
    results = pl.pallas_call(
        kernel,
        out_shape=(
            jax.ShapeDtypeStruct((1, ROWS, WIDTH), BF16),
            jax.ShapeDtypeStruct((1, ROWS, WIDTH), BF16),
            jax.ShapeDtypeStruct((64, GROUPS, 512), F32),
            jax.ShapeDtypeStruct((6, 8, 128), F32),
            jax.ShapeDtypeStruct((GROUPS, 512), F32),
        ),
        in_specs=[hbm] * 3 + [vmem] * 4,
        out_specs=[vmem] * 5,
        scratch_shapes=[
            pltpu.VMEM((ROWS, WIDTH), BF16),
            pltpu.VMEM((ROWS, WIDTH), BF16),
            pltpu.VMEM((ROWS, WIDTH), BF16),
            pltpu.VMEM((CHUNKS, 2 * ROWS, CW), BF16),
            pltpu.VMEM(chunks, BF16),
            pltpu.VMEM(chunks, BF16),
            pltpu.VMEM((CHUNKS // 2, 2 * ROWS, CW), BF16),
            pltpu.VMEM((CHUNKS, 3 * ROWS, CW), BF16),
            pltpu.VMEM(chunks, F32),
            pltpu.VMEM((ROWS, 128), F32),
            pltpu.VMEM((ROWS, 128), F32),
            pltpu.VMEM((2, *chunks), BF16),
            pltpu.VMEM(chunks, F32),
            pltpu.VMEM(chunks, BF16),
            pltpu.VMEM(chunks, BF16),
            pltpu.VMEM(chunks, BF16),
            pltpu.VMEM(chunks, BF16),
            pltpu.VMEM(chunks, BF16),
            pltpu.VMEM((2, ROWS, 128), F32),
            pltpu.VMEM((4, GROUPS, 128, 512), BF16),
            pltpu.VMEM((GROUPS, 384, 256), BF16),
            pltpu.VMEM((GROUPS, 256, 384), BF16),
            pltpu.VMEM((GROUPS, 128, 128), F32),
            pltpu.VMEM((GROUPS, 384, 256), F32),
            pltpu.VMEM((4, 2, 8, 64, 128), BF16),
            pltpu.VMEM((8, 8, 64, 128), BF16),
            pltpu.VMEM((4, 8, 16, 128), BF16),
            pltpu.VMEM((8, 4, 16, 128), BF16),
            pltpu.VMEM((4, 16, 128), BF16),
            pltpu.VMEM((8, 4, 16, 128), BF16),
            pltpu.VMEM((8, 16, 128), BF16),
            pltpu.VMEM((8, 8, 16, 128), BF16),
            pltpu.VMEM((8, 8, 128), F32),
            pltpu.VMEM((8, 8, 128), F32),
            pltpu.VMEM((8, 128), F32),
            pltpu.VMEM((8, 8, 128), F32),
            pltpu.VMEM((8, 128), F32),
            pltpu.VMEM((8, 8, 128), F32),
            pltpu.VMEM((8, 128), F32),
            pltpu.VMEM((8, 8, 128), F32),
            dma((6,)), dma((1,)), dma((4,)), dma((4, 4)), dma((4,)), dma((2,)), dma((8,)), dma((4,)), dma((4,)),
            dma((3, 4)), dma((3,)), dma((2,)), dma((2,)), dma((2,)), dma((2, 4)), dma((2,)), dma((2,)),
            dma((4,)), dma((4,)),
        ],
        compiler_params=pltpu.CompilerParams(
            collective_id=0, has_side_effects=True, vmem_limit_bytes=67043328 - 13312 * 1024
        ),
        name="span",
    )(
        gated,
        values_in,
        upstream,
        gain.reshape(1, WIDTH),
        shift.reshape(1, WIDTH),
        mix_w.transpose(1, 0, 2),
        mix_bias,
    )
    out_u, out_v, out_mix, out_bias, out_gain, out_shift = pl.pallas_call(
        writer,
        out_shape=(
            jax.ShapeDtypeStruct((1, ROWS, WIDTH), BF16),
            jax.ShapeDtypeStruct((1, ROWS, WIDTH), BF16),
            jax.ShapeDtypeStruct((64, GROUPS, 512), F32),
            jax.ShapeDtypeStruct((GROUPS, 512), F32),
            jax.ShapeDtypeStruct((3, 8, 128), F32),
            jax.ShapeDtypeStruct((3, 8, 128), F32),
        ),
        in_specs=[vmem] * 5,
        out_specs=[hbm] * 6,
        scratch_shapes=[dma((6,))],
        compiler_params=pltpu.CompilerParams(vmem_limit_bytes=1024 * 1024),
        name="writer",
    )(*results)
    return (out_u, out_v, out_mix, out_bias, out_gain.reshape(WIDTH), out_shift.reshape(WIDTH))


def solution(mesh):
    torus = Mesh(mesh.devices.reshape(8, 8, 4, 2), AXES)
    return jax.shard_map(
        per_device,
        mesh=torus,
        in_specs=(
            P(DP, SP, None),
            P(DP, SP, None),
            P(DP, SP, None),
            P(),
            P(),
            P(DP, None, None),
            P(),
        ),
        out_specs=(P(DP, SP, None), P(DP, SP, None), P(DP, None, None), P(), P(), P()),
        check_vma=False,
    )
```

```python
import jax
import jax.numpy as jnp
from jax import lax
from jax.experimental import pallas as pl
from jax.experimental.pallas import tpu as pltpu
from jax.sharding import Mesh
from jax.sharding import PartitionSpec as P

AXES = ("z", "y", "x", "core")
DP = ("x", "core")
SP = ("z", "y")
MESH = pl.DeviceIdType.MESH
F32 = jnp.float32
BF16 = jnp.bfloat16
EPS = 1e-05

GROUPS = 4
ROWS = 128
WIDTH = 3072
CHUNKS = 8
CW = WIDTH // CHUNKS

TILES = {
    (0, 0): [(0, g) for g in range(4)],
    (1, 1): [(0, 0), (0, 1), (1, 0), (1, 1), (0, 2), (1, 2), (0, 3), (1, 3)],
    (1, 2): [(0, 2), (1, 2), (0, 3), (1, 3)],
    (1, 3): [(0, 2), (1, 2), (0, 3), (1, 3)],
    (2, 2): [(2, 2), (2, 3), (2, 0), (0, 0), (1, 0), (2, 1), (0, 1), (1, 1)],
    (2, 3): [(2, 2), (2, 3), (2, 0), (0, 0), (1, 0), (2, 1), (0, 1), (1, 1)],
    (3, 3): [(3, g) for g in range(4)],
}
ENDS = {
    (0, 0): (0, 4, 4, 4),
    (1, 1): (0, 4, 6, 8),
    (1, 2): (0, 0, 2, 4),
    (1, 3): (0, 0, 2, 4),
    (2, 2): (0, 2, 4, 8),
    (2, 3): (0, 2, 4, 8),
    (3, 3): (0, 4, 4, 4),
}


def chain(key, k):
    ends = ENDS[key]
    return ((ends[0], ends[2]), (ends[2], ends[3]))[k]


def places_of(t, k):
    off = sum(ENDS[key][2] // 2 for key in TILES if key[1] == t) if k else 0
    out = []
    for key in TILES:
        a, b = chain(key, k)
        if key[1] == t and a < b:
            out.append((key, (b - a) // 2, off))
            off += (b - a) // 2
    return out


ORDER = {0: (0, 1, 2, 3), 1: (0, 1, 2, 3), 2: (2, 3, 0, 1), 3: (2, 3, 0, 1)}
COLUMNS = {
    (0, 0): {g: (0, 128) for g in range(4)},
    (1, 1): {g: (0, 256) for g in range(4)},
    (1, 2): {2: (0, 256), 3: (0, 256)},
    (1, 3): {2: (0, 256), 3: (0, 256)},
    (2, 2): {0: (0, 384), 1: (0, 384), 2: (256, 384), 3: (256, 384)},
    (2, 3): {0: (0, 384), 1: (0, 384), 2: (256, 384), 3: (256, 384)},
    (3, 3): {g: (384, 512) for g in range(4)},
}


def remote(src, dst, send, recv, device):
    return pltpu.make_async_remote_copy(
        src_ref=src, dst_ref=dst, send_sem=send, recv_sem=recv, device_id=device, device_id_type=MESH
    )


def dot(a, b):
    return jnp.dot(a, b, preferred_element_type=F32)


def dot_t(a, b):
    return lax.dot_general(a, b, (((1,), (1,)), ((), ())), preferred_element_type=F32)


def loop(lo, hi, body, name="loop"):
    with jax.named_scope(name):
        lax.fori_loop(lo, hi, lambda i, _: (body(i), None)[1], None)


FAR_FIRST = (4, 3, 5, 2, 6, 1, 7)


def far_first(body):
    for o in FAR_FIRST:
        body(o)


def kernel(
    gated_hbm, values_hbm, upstream_hbm, gain, shift, WT, bias,
    out_u, out_v, out_mix, out_vec, out_bias,
    gated, values, upstream,
    XC, XF, XR, UR, YC, UN, MEAN, INV, RES, YP, PS1, PS2, PSQ, PR, PQ, ACC,
    WBUF, WX, WXT, BIASC, GX, GS, GR, GZ, ZR, YS, YR, ZS, ZG,
    VS, VA, VT, VB, VU, VC, VW, VD,
    in_s, w_s, f_s, w_r, w_r2, m_s, m_r, y_r, p_r, r1_s, r1_r, r2_s, r2_r, r3_s, r3_r, r4_s, r4_r,
    v_s, v_r,
):
    z, y = lax.axis_index("z"), lax.axis_index("y")
    x, core = lax.axis_index("x"), lax.axis_index("core")
    d = x * 2 + core
    half = y // 4
    j = y % 4
    up = j // 2
    inner = (j == 1) | (j == 2)
    outer = jnp.logical_not(inner)
    lower = up == 0
    upper = up == 1
    base = half * 4
    own_outer = (z, base + 3 * up, x, core)
    own_inner = (z, base + 1 + up, x, core)
    opp_inner = (z, base + 2 - up, x, core)
    opp_outer = (z, base + 3 - 3 * up, x, core)
    partner = (z, y, x, 1 - core)
    kx, ky = up, 1 - up

    def dp_peer(o):
        e = (d + o) % 8
        return e, (z, y, e // 2, e % 2)

    def z_peer(o):
        e = (z + o) % 8
        return e, (e, y, x, core)

    def y_peer(o):
        e = (y + o) % 8
        return e, (z, e, x, core)

    def phys(q):
        return (q + 4 * up) % 8

    big = ((values_hbm, values), (upstream_hbm, upstream), (gated_hbm, gated))

    def fetch(k, part):
        rows = pl.ds(part * 32, 32)
        source, dest = big[k]
        return pltpu.make_async_copy(source.at[0, rows, :], dest.at[rows, :], in_s.at[part if k == 0 else 3 + k])

    barrier = pltpu.get_barrier_semaphore()

    def greet(o):
        for peer in (dp_peer, z_peer, y_peer):
            pl.semaphore_signal(barrier, inc=1, device_id=peer(o)[1], device_id_type=MESH)

    @pl.when(lower)
    def _():
        for part in range(4):
            fetch(0, part).start()

    @pl.when(upper)
    def _():
        for part in range(4):
            fetch(1, part).start()
            fetch(2, part).start()

    loop(1, 8, greet, "greet")

    @pl.when(lower)
    def _():
        for part in range(4):
            fetch(1, part).start()
            fetch(2, part).start()

    @pl.when(upper)
    def _():
        for part in range(4):
            fetch(0, part).start()

    def stats(i):
        r = pl.multiple_of(i * 32, 32)
        fetch(0, i).wait()
        v = values[pl.ds(r, 32), :].astype(F32)
        mean = jnp.sum(v, axis=1, keepdims=True) * (1.0 / WIDTH)
        d0 = v - mean
        inv = lax.rsqrt(jnp.sum(d0 * d0, axis=1, keepdims=True) * (1.0 / WIDTH) + EPS)
        MEAN[pl.ds(r, 32), :] = jnp.broadcast_to(mean, (32, 128))
        INV[pl.ds(r, 32), :] = jnp.broadcast_to(inv, (32, 128))

    def wide(v):
        return jnp.concatenate([v] * (CW // 128), axis=1)

    def columns(c):
        return pl.ds(pl.multiple_of(c * CW, 128), CW)

    def norm(c, dest, row0, far=False):
        cols = columns(c)
        u = (values[:, cols].astype(F32) - wide(MEAN[...])) * wide(INV[...])
        UN[c] = u
        if far:
            XF[c] = u.astype(BF16)
        dest[c, row0 : row0 + ROWS, :] = (u * gain[:, cols] + shift[:, cols]).astype(BF16)

    def mix_grad(c, dest, row0, far=False):
        cols = columns(c)
        m = (upstream[:, cols].astype(F32) * gated[:, cols].astype(F32)).astype(BF16)
        if far:
            XF[c] = m
        dest[c, row0 : row0 + ROWS, :] = m

    def fetched_pair():
        for k in (1, 2):
            source, dest = big[k]
            pltpu.make_async_copy(source.at[0], dest, in_s.at[3 + k]).wait()

    @pl.when(lower)
    def _():
        loop(0, 4, stats, "stats")

    @pl.when(upper)
    def _():
        fetched_pair()

    with jax.named_scope("barrier"):
        pl.semaphore_wait(barrier, 21)

    def x_near(c):
        return remote(XF.at[c], XR.at[c], m_s.at[1], m_r.at[c], own_inner)

    def x_opp(c):
        return remote(XF.at[c], YC.at[c, pl.ds(ROWS, ROWS), :], m_s.at[0], y_r.at[c % 4], opp_inner)

    def x_relay(c):
        return remote(XR.at[c], YC.at[c, pl.ds(2 * ROWS, ROWS), :], m_s.at[1], y_r.at[c % 4], opp_inner)

    def p_inner(c):
        return remote(PS1.at[c], PR.at[c], m_s.at[1], p_r.at[c % 4], opp_inner)

    def p_outer(c):
        return remote(PS2.at[c], PR.at[c], m_s.at[1], p_r.at[c % 4], opp_outer)

    def q_outer(c):
        return remote(PSQ.at[c], PQ.at[c], m_s.at[0], m_r.at[c], own_outer)

    def make_x(c):
        @pl.when(lower)
        def _():
            norm(c, XC, ROWS, True)

        @pl.when(upper)
        def _():
            mix_grad(c, XC, ROWS, True)

    @pl.when(inner)
    def _():
        def send(q):
            c = phys(q)
            make_x(c)
            x_opp(c).start()

        loop(0, 4, send, "make_x")

    @pl.when(outer)
    def _():
        def send(q):
            c = phys(q)
            make_x(c)
            x_near(c).start()

        loop(0, 8, send, "make_x")

    def w_rows(t, g, h):
        c0, c1 = COLUMNS[t][g]
        return WBUF.at[t[1], g, pl.ds(h * 64, 64), c0:c1]

    def w_send(key, g, o):
        c0, c1 = COLUMNS[key][g]
        to = partner if o == 0 else (z, y, (x + o) % 4, core)
        land = w_r2.at[g] if o == 0 else w_r.at[key[1], g]
        return remote(WT.at[g, :, c0:c1], w_rows(key, g, core), w_s.at[0], land, to)

    for key in COLUMNS:

        @pl.when((j == key[0]) & (x == key[1]))
        def _(key=key):
            for g in ORDER[key[0]]:
                if g in COLUMNS[key]:
                    for o in (2, 1, 3, 0):
                        w_send(key, g, o).start()

    WBUF[x, :, pl.ds(pl.multiple_of(core * 64, 64), 64), :] = WT[...]

    @pl.when(inner)
    def _():
        loop(4, 8, lambda q: make_x(phys(q)), "make_x")

    @pl.when(lower)
    def _():
        fetched_pair()
        loop(0, CHUNKS, lambda c: mix_grad(c, YC, 0), "mix_grad")

    @pl.when(upper)
    def _():
        loop(0, 4, stats, "stats")
        loop(0, CHUNKS, lambda c: norm(c, YC, 0), "norm")

    VS[...] = jnp.zeros_like(VS)
    out_mix[...] = jnp.zeros_like(out_mix)
    GX[...] = jnp.zeros_like(GX)
    ACC[...] = jnp.zeros_like(ACC)
    ones = jnp.ones((8, CW), BF16)
    for g in range(GROUPS):
        rows = jnp.broadcast_to(bias[pl.ds(g, 1), pl.ds(pl.multiple_of(j * 128, 128), 128)], (128, 128))
        BIASC[g] = rows.T

    def sum_bias(source, row0):
        for g in range(GROUPS):
            s = dot_t(ones, source[2 * g, pl.ds(row0, ROWS), :]) + dot_t(ones, source[2 * g + 1, pl.ds(row0, ROWS), :])
            VS[6 + g // 2, pl.ds((g % 2) * 4 + j, 1), :] = s[0:1]

    @pl.when(lower)
    def _():
        sum_bias(YC, 0)

    @pl.when(upper)
    def _():
        sum_bias(XC, ROWS)

    seg_t = lax.broadcasted_iota(jnp.int32, (128, 128), 0) // 64
    seg_s = lax.broadcasted_iota(jnp.int32, (128, 128), 1) // 64
    allowed = seg_t >= seg_s

    def tile(t, s, g):
        w = WBUF[t, g, :, s * 128 : (s + 1) * 128]
        return jnp.where(allowed, w, jnp.zeros_like(w)) if t == s else w

    def place(g, dst, src, a, b):
        WX[g, dst * 128 : (dst + 1) * 128, src * 128 : (src + 1) * 128] = a
        WXT[g, src * 128 : (src + 1) * 128, dst * 128 : (dst + 1) * 128] = b

    def w_relay(key, g):
        rows = w_rows(key, g, core)
        return remote(rows, rows, f_s.at[key[1]], w_r2.at[g], partner)

    def w_ready(jj, g):
        keys = [key for key in COLUMNS if key[0] == jj and g in COLUMNS[key]]
        with jax.named_scope("w_wait"):
            for key in keys:

                @pl.when(x != key[1])
                def _(key=key):
                    rows = w_rows(key, g, core)
                    remote(rows, rows, w_s.at[0], w_r.at[key[1], g], partner).wait_recv()
                    w_relay(key, g).start()

            c0, c1 = COLUMNS[keys[0]][g]
            rows = WBUF.at[0 : len(keys), g, 0:64, c0:c1]
            remote(rows, rows, w_s.at[0], w_r2.at[g], partner).wait_recv()
        if jj == 0:
            w = tile(0, 0, g)
            place(g, 0, 0, w, w.T)
        elif jj == 3:
            w = tile(3, 3, g)
            place(g, 0, 0, w.T, w)
        elif jj == 1:
            for t in (1, 2, 3) if g >= 2 else (1,):
                for s in (0, 1):
                    w = tile(t, s, g)
                    place(g, t - 1, s, w, w.T)
        else:
            for s in (0, 1, 2) if g < 2 else (2,):
                for t in (2, 3):
                    w = tile(t, s, g)
                    place(g, 2 - s, 3 - t, w.T, w)

    def bias_of(g, on):
        b = jnp.where(on, BIASC[g], 0.0)
        return jnp.concatenate([b] * (CW // 128), axis=1)

    def row_sums(c, back):
        a = back * gain[:, columns(c)]
        b = a * UN[c]
        ACC[0] += a[:, 0:128] + a[:, 128:256] + a[:, 256:384]
        ACC[1] += b[:, 0:128] + b[:, 128:256] + b[:, 256:384]

    def column_sums(c, product, back):
        gt = jnp.sum(product, axis=0, keepdims=True)
        st = jnp.sum(back, axis=0, keepdims=True)
        for i in range(3):
            row = c * 3 + i
            VS[row // 8, pl.ds(row % 8, 1), :] += gt[:, i * 128 : (i + 1) * 128]
            VS[row // 8 + 3, pl.ds(row % 8, 1), :] += st[:, i * 128 : (i + 1) * 128]

    def put_x(c, g, value):
        value = (value + bias_of(g, lower)).astype(BF16)
        RES[kx, c] = value

        @pl.when(upper)
        def _():
            back = value.astype(F32)
            row_sums(c, back)
            column_sums(c, back * UN[c], back)

    def put_y(c, g, value, columns_too):
        value = (value + bias_of(g, upper)).astype(BF16)
        RES[ky, c] = value

        @pl.when(lower)
        def _():
            back = value.astype(F32)
            row_sums(c, back)
            if columns_too:
                column_sums(c, back * UN[c], back)

    def stage(part):
        for key, tiles in TILES.items():
            jj, t = key
            lo, hi = ENDS[key][part : part + 2]
            if lo == hi:
                continue

            @pl.when(j == jj)
            def _(jj=jj, t=t, tiles=tiles, lo=lo, hi=hi):
                for index in range(lo, hi):
                    s, g = tiles[index]
                    if jj == 0:
                        value = GX[g, 0:128, 0:128]
                    elif jj == 3:
                        value = GX[g, 0:128, 0:128].T
                    elif jj == 1:
                        value = GX[g, (t - 1) * 128 : t * 128, s * 128 : (s + 1) * 128]
                    else:
                        value = GX[g, (2 - s) * 128 : (3 - s) * 128, (3 - t) * 128 : (4 - t) * 128].T
                    value = value.astype(BF16)
                    GS[t, 0, index] = value[0:64]
                    GS[t, 1, index] = value[64:128]
                for h in range(2):
                    e = 2 * t + h

                    @pl.when(d != e)
                    def _():
                        remote(
                            GS.at[t, h, lo:hi], GR.at[d, lo:hi], r1_s.at[part, t], r1_r.at[part], (z, y, t, h)
                        ).start()

                    @pl.when(d == e)
                    def _():
                        GR[e, lo:hi] = GS[t, h, lo:hi]

    def sum_dp(k):
        def body(key):
            a, b = chain(key, k)
            with jax.named_scope("r1_wait"):
                for part in (0, 1) if k == 0 else (2,):
                    lo, hi = ENDS[key][part : part + 2]
                    if lo < hi:
                        there = GR.at[0:7, lo:hi]
                        remote(there, there, r1_s.at[0, 0], r1_r.at[part], partner).wait_recv()

            def add(i):
                total = GR[0, i].astype(F32)
                for e in range(1, 8):
                    total = total + GR[e, i].astype(F32)
                total = total.astype(BF16)
                for rs in range(4):
                    GZ[rs, i] = total[rs * 16 : (rs + 1) * 16]

            loop(a, b, add, "dp_add")
            m = (b - a) // 2
            at = a // 2

            def piece(e):
                return pl.ds(a + (e // 4) * m, m)

            def send(o):
                e, peer = z_peer(o)
                remote(GZ.at[e % 4, piece(e)], ZR.at[z, at : at + m], r2_s.at[k], r2_r.at[k], peer).start()

            far_first(send)
            ZR[z, at : at + m] = GZ[z % 4, piece(z)]

        return body

    def sum_z(k):
        def body(key):
            a, b = chain(key, k)
            m = (b - a) // 2
            here = slice(a // 2, a // 2 + m)
            with jax.named_scope("r2_wait"):
                there = ZR.at[0:7, here]
                remote(there, there, r2_s.at[k], r2_r.at[k], partner).wait_recv()
            total = ZR[0, here].astype(F32)
            for e in range(1, 8):
                total = total + ZR[e, here].astype(F32)
            YS[here] = total.astype(BF16)

            def send(o):
                e, peer = y_peer(o)
                remote(YS.at[here], YR.at[y, here], r3_s.at[k], r3_r.at[k, key[0]], peer).start()

            far_first(send)
            YR[y, here] = YS[here]

        return body

    def join(k):
        for t in range(4):
            places = places_of(t, k)
            if not places:
                continue

            @pl.when(x == t)
            def _(places=places):
                for key, m, off in places:
                    jj = key[0]
                    at = chain(key, k)[0] // 2
                    for count in (1, 2):

                        @pl.when((j == jj) if count == 1 else (j != jj))
                        @jax.named_scope("r3_wait")
                        def _():
                            there = YR.at[0:count, at : at + m]
                            remote(there, there, r3_s.at[k], r3_r.at[k, jj], partner).wait_recv()

                    for i in range(m):
                        ZS[off + i] = (YR[jj, at + i].astype(F32) + YR[jj + 4, at + i].astype(F32)).astype(BF16)
                here = slice(places[0][2], places[-1][2] + places[-1][1])

                def send(o):
                    e, peer = z_peer(o)
                    remote(ZS.at[here], ZG.at[z, here], r4_s.at[k], r4_r.at[k], peer).start()

                far_first(send)
                ZG[z, here] = ZS[here]

    def put_mix(k):
        keep = lax.broadcasted_iota(jnp.int32, (16, 128), 1) // 64 <= core
        for t in range(4):
            places = places_of(t, k)
            if not places:
                continue

            @pl.when(x == t)
            def _(t=t, places=places):
                there = ZG.at[0:7, places[0][2] : places[-1][2] + places[-1][1]]
                with jax.named_scope("r4_wait"):
                    remote(there, there, r4_s.at[k], r4_r.at[k], partner).wait()
                for part in range(8):
                    rows = slice(16 * (part % 4), 16 * (part % 4) + 16)
                    for key, m, off in places:
                        for i in range(m):
                            s, g = TILES[key][chain(key, k)[0] + (part // 4) * m + i]
                            value = ZG[part, off + i].astype(F32)
                            if s == t:
                                value = jnp.where(keep, value, 0.0)
                            out_mix[rows, g, s * 128 : (s + 1) * 128] = value

    def vec_send(source, land, me, k, peer):
        for o in FAR_FIRST:
            e, to = peer(o)
            remote(source(e), land.at[me], v_s.at[k], v_r.at[k], to).start()

    def vec_wait(land, k):
        with jax.named_scope("v_wait"):
            remote(land.at[0:7], land.at[0:7], v_s.at[k], v_r.at[k], partner).wait()

    def vec_sum(land):
        total = land[0]
        for e in range(1, 8):
            total = total + land[e]
        return total

    def vec_dp():
        vec_send(lambda e: VS.at[e], VA, d, 0, dp_peer)
        VA[d] = VS[d]

    @pl.when(inner)
    def _():
        def arrived(c):
            x_near(c).wait_recv()

        def take(c):
            @pl.when(lower)
            def _():
                n = XR[c].astype(F32) * gain[:, columns(c)] + shift[:, columns(c)]
                XC[c, pl.ds(0, ROWS), :] = n.astype(BF16)

            @pl.when(upper)
            def _():
                XC[c, pl.ds(0, ROWS), :] = XR[c]

        def outer_sums(c):
            back = PSQ[c].astype(F32)
            column_sums(c, back * XR[c].astype(F32), back)

        def first(c):
            g = c // 2
            s = dot(WXT[g, :, 0:ROWS], YC[c, 0:ROWS, :])
            PSQ[c] = s[0:ROWS].astype(BF16)
            YP[c] = s[ROWS:]
            q_outer(c).start()

            @pl.when(lower)
            def _():
                column_sums(c, s[ROWS:] * UN[c], s[ROWS:])

            with jax.named_scope("wait_x"):
                arrived(c)
            x_relay(c).start()
            take(c)
            put_x(c, g, dot(WX[g, 0:ROWS, :], XC[c]))
            GX[g, 0:ROWS, :] += dot_t(YC[c, 0:ROWS, :], XC[c])

            @pl.when(lower)
            def _():
                outer_sums(c)

        def meet(c):
            g = c // 2
            with jax.named_scope("wait_x"):
                arrived(c)
            take(c)
            with jax.named_scope("wait_y"):
                both_y = YC.at[c, pl.ds(ROWS, 2 * ROWS), :]
                remote(both_y, both_y, m_s.at[0], y_r.at[c % 4], opp_inner).wait_recv()

            @pl.when(upper)
            def _():
                raw = YC[c, pl.ds(ROWS, 2 * ROWS), :]
                UR[c % 4] = raw
                n = raw.astype(F32) * gain[:, columns(c)] + shift[:, columns(c)]
                YC[c, pl.ds(ROWS, 2 * ROWS), :] = n.astype(BF16)

            GX[g] += dot_t(YC[c], XC[c])

        def multiply(c, now):
            g = c // 2
            r = dot(WX[g], XC[c])
            PS1[c] = r[ROWS : 2 * ROWS].astype(BF16)
            PS2[c] = r[2 * ROWS :].astype(BF16)
            if now:
                p_outer(c).start()
                p_inner(c).start()
            put_x(c, g, r[0:ROWS])
            s = dot(WXT[g], YC[c])
            PSQ[c] = s[0:ROWS].astype(BF16)
            put_y(c, g, s[ROWS:], True)
            q_outer(c).start()

            @pl.when(lower)
            def _():
                outer_sums(c)

            @pl.when(upper)
            def _():
                u = UR[c % 4].astype(F32)
                near, far = PS1[c].astype(F32), PS2[c].astype(F32)
                column_sums(c, near * u[0:ROWS] + far * u[ROWS:], near + far)

        def second(c):
            meet(c)
            multiply(c, True)

        for i in range(4):
            for jj in (1, 2):

                @pl.when(j == jj)
                def _(jj=jj, i=i):
                    w_ready(jj, ORDER[jj][i])

            if i < 2:
                loop(2 * i, 2 * i + 2, lambda q: first(phys(q)), "first")
            elif i == 2:
                loop(2 * i, 2 * i + 2, lambda q: second(phys(q)), "second")
            else:
                loop(2 * i, 2 * i + 2, lambda q: meet(phys(q)), "meet")
            if i > 0:
                with jax.named_scope("stage"):
                    stage(i - 1)
        with jax.named_scope("multiply"):
            multiply(phys(6), True)
            multiply(phys(7), False)
        vec_dp()

    @pl.when(outer)
    def _():
        for jj in (0, 3):

            @pl.when(j == jj)
            def _(jj=jj):
                for g in ORDER[jj]:
                    w_ready(jj, g)

        def local(c):
            g = c // 2
            own_x = XC[c, pl.ds(ROWS, ROWS), :]
            own_y = YC[c, pl.ds(0, ROWS), :]
            put_x(c, g, dot(WX[g, 0:ROWS, 0:ROWS], own_x))
            part = dot(WXT[g, 0:ROWS, 0:ROWS], own_y)
            YP[c] = part

            @pl.when(lower)
            def _():
                column_sums(c, part * UN[c], part)

            GX[g, 0:ROWS, 0:ROWS] += dot_t(own_y, own_x)

        loop(0, 8, local, "local")
        stage(0)

    def late(q):
        c = phys(q)
        p_inner(c).wait_recv()
        put_y(c, c // 2, YP[c] + PR[c].astype(F32), False)

    def near_part(q):
        c = phys(q)
        q_outer(c).wait_recv()
        YP[c] += PQ[c].astype(F32)

    def near_whole(q):
        c = phys(q)
        q_outer(c).wait_recv()
        put_y(c, c // 2, YP[c] + PQ[c].astype(F32), False)

    def owned(places, body):
        for key in TILES:
            if key[0] in places:

                @pl.when((j == key[0]) & (x == key[1]))
                def _(key=key):
                    body(key)

    def vec_z():
        vec_wait(VA, 0)
        VT[...] = vec_sum(VA)
        vec_send(lambda e: VT, VB, z, 1, z_peer)
        VB[z] = VT[...]

    def vec_y():
        vec_wait(VB, 1)
        VU[...] = vec_sum(VB)
        vec_send(lambda e: VU, VC, y, 2, y_peer)
        VC[y] = VU[...]

    @pl.when(inner)
    def _():
        owned((1, 2), sum_dp(0))
        owned((1, 2), sum_dp(1))
        vec_z()
        loop(0, 2, late, "late")
        owned((1, 2), sum_z(0))
        p_outer(phys(7)).start()
        p_inner(phys(7)).start()
        vec_y()
        owned((1, 2), sum_z(1))

    @pl.when(outer)
    def _():
        vec_dp()
        owned((0, 3), sum_dp(0))
        loop(0, 4, near_part, "near_part")
        owned((0, 3), sum_z(0))
        vec_z()
        loop(4, 6, near_whole, "near_whole")
        vec_y()
        loop(6, 8, near_whole, "near_whole")
        loop(0, 2, late, "late")

    join(0)
    with jax.named_scope("late"):
        late(2)
    with jax.named_scope("late"):
        late(3)
    vec_wait(VC, 2)
    VW[...] = vec_sum(VC)
    vec_send(lambda e: VW, VD, d, 3, dp_peer)
    VD[d] = VW[...]
    join(1)

    mean_a = jnp.sum(ACC[0], axis=1, keepdims=True) * (1.0 / WIDTH)
    mean_b = jnp.sum(ACC[1], axis=1, keepdims=True) * (1.0 / WIDTH)
    ACC[0] = jnp.broadcast_to(mean_a, (ROWS, 128))
    ACC[1] = jnp.broadcast_to(mean_b, (ROWS, 128))

    def outputs(c):
        cols = columns(c)
        scaled = RES[1, c].astype(F32) * gain[:, cols]
        out_v[0, :, cols] = (wide(INV[...]) * (scaled - wide(ACC[0]) - UN[c] * wide(ACC[1]))).astype(BF16)
        out_u[0, :, cols] = (upstream[:, cols].astype(F32) * RES[0, c].astype(F32)).astype(BF16)

    loop(0, CHUNKS, outputs, "outputs")

    for key in COLUMNS:

        total = sum(c1 - c0 for c0, c1 in COLUMNS[key].values())
        groups = 2 if total % 512 == 0 and key != (1, 1) and key[0] != 0 and key[0] != 3 else 4
        cols = total // groups

        @pl.when((j == key[0]) & (x == key[1]))
        def _(groups=groups, cols=cols):
            rows = WBUF.at[0:4, 0:groups, 0:64, 0:cols]
            remote(rows, rows, w_s.at[0], w_r2.at[0], partner).wait_send()

        @pl.when((j == key[0]) & (x != key[1]))
        def _(key=key, groups=groups, cols=cols):
            rows = WBUF.at[0, 0:groups, 0:64, 0:cols]
            remote(rows, rows, f_s.at[key[1]], w_r2.at[0], partner).wait_send()

    def chunks_left(source, sem):
        remote(source, source, m_s.at[sem], m_r.at[0], own_inner).wait_send()

    @pl.when(inner)
    def _():
        chunks_left(YC.at[0:4], 0)
        chunks_left(YC.at[0:4], 1)

    @pl.when(outer)
    def _():
        chunks_left(PS1, 1)

    for key, tiles in TILES.items():
        jj, t = key
        for part in range(3):
            lo, hi = ENDS[key][part : part + 2]
            for count in (1, 2):
                if lo < hi:

                    @pl.when((j == jj) & ((x == t) if count == 1 else (x != t)))
                    def _(t=t, count=count, lo=lo, hi=hi, part=part):
                        there = GS.at[0, 0:count, lo:hi]
                        remote(there, there, r1_s.at[part, t], r1_r.at[part], partner).wait_send()

    def sent(key):
        for k in range(2):
            a, b = chain(key, k)
            if a < b:
                there = ZR.at[0:7, 0 : (b - a) // 2]
                remote(there, there, r2_s.at[k], r2_r.at[k], partner).wait_send()
                remote(there, there, r3_s.at[k], r3_r.at[k, 0], partner).wait_send()

    owned((0, 1, 2, 3), sent)
    put_mix(0)
    vec_wait(VD, 3)
    out_vec[...] = VD[0:6]
    for g in range(GROUPS):
        for k in range(4):
            out_bias[g : g + 1, k * 128 : (k + 1) * 128] = VD[6 + g // 2, (g % 2) * 4 + k : (g % 2) * 4 + k + 1]
    put_mix(1)


def writer(u, v, mix, vec, bias, out_u, out_v, out_mix, out_bias, out_gain, out_shift, sems):
    copies = [
        pltpu.make_async_copy(source, dest, sems.at[i])
        for i, (source, dest) in enumerate(
            (
                (u, out_u),
                (v, out_v),
                (mix, out_mix),
                (bias, out_bias),
                (vec.at[0:3], out_gain),
                (vec.at[3:6], out_shift),
            )
        )
    ]
    for copy in copies:
        copy.start()
    for copy in copies:
        copy.wait()


def per_device(gated, values_in, upstream, gain, shift, mix_w, mix_bias):
    vmem = pl.BlockSpec(memory_space=pltpu.VMEM)
    hbm = pl.BlockSpec(memory_space=pltpu.HBM)
    chunks = (CHUNKS, ROWS, CW)
    dma = pltpu.SemaphoreType.DMA
    results = pl.pallas_call(
        kernel,
        out_shape=(
            jax.ShapeDtypeStruct((1, ROWS, WIDTH), BF16),
            jax.ShapeDtypeStruct((1, ROWS, WIDTH), BF16),
            jax.ShapeDtypeStruct((64, GROUPS, 512), F32),
            jax.ShapeDtypeStruct((6, 8, 128), F32),
            jax.ShapeDtypeStruct((GROUPS, 512), F32),
        ),
        in_specs=[hbm] * 3 + [vmem] * 4,
        out_specs=[vmem] * 5,
        scratch_shapes=[
            pltpu.VMEM((ROWS, WIDTH), BF16),
            pltpu.VMEM((ROWS, WIDTH), BF16),
            pltpu.VMEM((ROWS, WIDTH), BF16),
            pltpu.VMEM((CHUNKS, 2 * ROWS, CW), BF16),
            pltpu.VMEM(chunks, BF16),
            pltpu.VMEM(chunks, BF16),
            pltpu.VMEM((CHUNKS // 2, 2 * ROWS, CW), BF16),
            pltpu.VMEM((CHUNKS, 3 * ROWS, CW), BF16),
            pltpu.VMEM(chunks, F32),
            pltpu.VMEM((ROWS, 128), F32),
            pltpu.VMEM((ROWS, 128), F32),
            pltpu.VMEM((2, *chunks), BF16),
            pltpu.VMEM(chunks, F32),
            pltpu.VMEM(chunks, BF16),
            pltpu.VMEM(chunks, BF16),
            pltpu.VMEM(chunks, BF16),
            pltpu.VMEM(chunks, BF16),
            pltpu.VMEM(chunks, BF16),
            pltpu.VMEM((2, ROWS, 128), F32),
            pltpu.VMEM((4, GROUPS, 128, 512), BF16),
            pltpu.VMEM((GROUPS, 384, 256), BF16),
            pltpu.VMEM((GROUPS, 256, 384), BF16),
            pltpu.VMEM((GROUPS, 128, 128), F32),
            pltpu.VMEM((GROUPS, 384, 256), F32),
            pltpu.VMEM((4, 2, 8, 64, 128), BF16),
            pltpu.VMEM((8, 8, 64, 128), BF16),
            pltpu.VMEM((4, 8, 16, 128), BF16),
            pltpu.VMEM((8, 4, 16, 128), BF16),
            pltpu.VMEM((4, 16, 128), BF16),
            pltpu.VMEM((8, 4, 16, 128), BF16),
            pltpu.VMEM((8, 16, 128), BF16),
            pltpu.VMEM((8, 8, 16, 128), BF16),
            pltpu.VMEM((8, 8, 128), F32),
            pltpu.VMEM((8, 8, 128), F32),
            pltpu.VMEM((8, 128), F32),
            pltpu.VMEM((8, 8, 128), F32),
            pltpu.VMEM((8, 128), F32),
            pltpu.VMEM((8, 8, 128), F32),
            pltpu.VMEM((8, 128), F32),
            pltpu.VMEM((8, 8, 128), F32),
            dma((6,)), dma((1,)), dma((4,)), dma((4, 4)), dma((4,)), dma((2,)), dma((8,)), dma((4,)), dma((4,)),
            dma((3, 4)), dma((3,)), dma((2,)), dma((2,)), dma((2,)), dma((2, 4)), dma((2,)), dma((2,)),
            dma((4,)), dma((4,)),
        ],
        compiler_params=pltpu.CompilerParams(
            collective_id=0, has_side_effects=True, vmem_limit_bytes=67043328 - 13312 * 1024
        ),
        name="span",
    )(
        gated,
        values_in,
        upstream,
        gain.reshape(1, WIDTH),
        shift.reshape(1, WIDTH),
        mix_w.transpose(1, 0, 2),
        mix_bias,
    )
    out_u, out_v, out_mix, out_bias, out_gain, out_shift = pl.pallas_call(
        writer,
        out_shape=(
            jax.ShapeDtypeStruct((1, ROWS, WIDTH), BF16),
            jax.ShapeDtypeStruct((1, ROWS, WIDTH), BF16),
            jax.ShapeDtypeStruct((64, GROUPS, 512), F32),
            jax.ShapeDtypeStruct((GROUPS, 512), F32),
            jax.ShapeDtypeStruct((3, 8, 128), F32),
            jax.ShapeDtypeStruct((3, 8, 128), F32),
        ),
        in_specs=[vmem] * 5,
        out_specs=[hbm] * 6,
        scratch_shapes=[dma((6,))],
        compiler_params=pltpu.CompilerParams(vmem_limit_bytes=1024 * 1024),
        name="writer",
    )(*results)
    return (out_u, out_v, out_mix, out_bias, out_gain.reshape(WIDTH), out_shift.reshape(WIDTH))


def solution(mesh):
    torus = Mesh(mesh.devices.reshape(8, 8, 4, 2), AXES)
    return jax.shard_map(
        per_device,
        mesh=torus,
        in_specs=(
            P(DP, SP, None),
            P(DP, SP, None),
            P(DP, SP, None),
            P(),
            P(),
            P(DP, None, None),
            P(),
        ),
        out_specs=(P(DP, SP, None), P(DP, SP, None), P(DP, None, None), P(), P(), P()),
        check_vma=False,
    )
```
